32 devices in a mesh: grp: 2 (over y), sp: 4 (over z), tp: 4 (over x, core).
Axes of the slice: x: 2, y: 2, z: 4, core: 2. Of those that a mesh axis runs over, the one named last changes fastest.
Arguments:
- query_rows: bfloat16 [1024, 1024], P(('grp', 'sp'), 'tp'), parts along dimension 0, may hold values from -6 to 6
- key_rows: bfloat16 [1024, 1024], P(('grp', 'sp'), 'tp'), parts along dimension 0, may hold values from -6 to 6
- value_rows: bfloat16 [1024, 1024], P(('grp', 'sp'), 'tp'), parts along dimension 0, may hold values from -6 to 6
- gate_rows: bfloat16 [1024, 1024], P(('grp', 'sp'), 'tp'), parts along dimension 0, may hold values from -6 to 6
- log_decay: float32 [2, 8, 1024], P(None, 'tp', ('grp', 'sp')), parts along dimension 2, may hold values from -2 to 0, as said below
- head_gain: float32 [2, 1024], P(None, 'tp'), may hold values from 0.1 to 1.9
- out_weight: bfloat16 [1024, 2048], P('tp'), may hold values from -0.1875 to 0.1875
- residual: bfloat16 [1024, 2048], P(('grp', 'sp')), parts along dimension 0, may hold values from -6 to 6
- norm_gain: bfloat16 [2048], replicated, may hold values from 0.099609375 to 1.8984375
- gate_weight: bfloat16 [2048, 5632], P('sp', 'tp'), may hold values from -0.125 to 0.125
- up_weight: bfloat16 [2048, 5632], P('sp', 'tp'), may hold values from -0.125 to 0.125
- down_weight: bfloat16 [2048, 5632], P('sp', 'tp'), may hold values from -0.078125 to 0.078125
- gate_taps: bfloat16 [3, 5632], P(None, 'tp'), may hold values from -3.5 to 3.5
- up_taps: bfloat16 [3, 5632], P(None, 'tp'), may hold values from -3.5 to 3.5
Outputs:
- block_out: bfloat16 [1024, 2048], P(('grp', 'sp', 'tp')), parts along dimension 0
The draws below stay inside these ranges and needn't reach their ends.
There are 2 independent parts, one for each index of `grp`. The reference program is written for one: setup_inputs(seed, part) draws one part's arguments, and reference() takes and returns one part's arrays. A program takes and returns all parts, laid end to end along the dimension named above; an argument that names none is the same for every part. Nothing has to cross between parts.
Inputs may be any that keep to these rules, and one draw needn't show every extreme that they name: `log_decay`: every entry is negative.
All inputs are finite; a program needn't handle non-finite values.
Results may differ from the reference program's by a relative error of at most 0.017.
Values may be sent and summed in bfloat16 or wider, within the bound.
A program may use at most 64 MiB of HBM per device.

```python
import math
import jax
import jax.numpy as jnp
from jax import lax

D = 2048
RETENTION_HEADS = 8
HEAD = 128
FF = 5632
TOK_DEV = 128
VALUE = 1024
TOKENS = 512


def spread_log(subkey, shape, low_end, high_end):
    return jnp.exp(jax.random.uniform(subkey, shape, jnp.float32, jnp.log(low_end), jnp.log(high_end)))


def draw_log_decay(key, part):
    random_subkeys = jax.random.split(jax.random.fold_in(key, 17), 7)
    blocks = TOKENS // TOK_DEV
    slow_share = 0.5
    totals = spread_log(random_subkeys[1], (2, RETENTION_HEADS, 1), 0.2, 0.7)
    is_slow = jax.random.bernoulli(random_subkeys[0], slow_share, (2, RETENTION_HEADS, 1))
    reach_len = spread_log(random_subkeys[2], (2, RETENTION_HEADS, 1), 30.0, 100.0)
    baseline_decay_rate = jnp.where(is_slow, -totals / TOKENS, -1.0 / reach_len)
    multiplier = spread_log(random_subkeys[3], (2, RETENTION_HEADS, blocks, 1), 0.5, 1.5)
    multiplier = jnp.broadcast_to(multiplier, (2, RETENTION_HEADS, blocks, TOK_DEV)).reshape(2, RETENTION_HEADS, TOKENS)
    approximate_multiplier = jax.random.uniform(random_subkeys[4], (2, RETENTION_HEADS, TOKENS), jnp.float32, 0.6, 1.4)
    target_locations = jax.random.randint(random_subkeys[5], (2, RETENTION_HEADS, 2, 1), 0, TOKENS)
    spike_depth = jnp.log(jax.random.uniform(random_subkeys[6], (2, RETENTION_HEADS, 2, 1), jnp.float32, 0.55, 0.8))
    token_positions = jnp.arange(TOKENS)[None, None, None, :]
    spike_events = jnp.sum(jnp.where(token_positions == target_locations, spike_depth, 0.0), axis=2)
    return (baseline_decay_rate * multiplier * approximate_multiplier + spike_events).astype(jnp.float32)


def block_levels(key, shape, pieces, low, high):
    level, own = 1.0, jax.random.fold_in(key, 6)
    for position, blocks in pieces:
        draws = jnp.exp(jax.random.uniform(jax.random.fold_in(own, position), (blocks,), jnp.float32, low / len(pieces), high / len(pieces)))
        level = level * jnp.repeat(draws, shape[position] // blocks).reshape([-1 if axis == position else 1 for axis in range(len(shape))])
    return level


def normal_values(key, extent, scale, bound, cuts=(), dtype=jnp.bfloat16):
    entries = jax.random.normal(key, extent, jnp.float32) * scale
    if len(cuts) > 0:
        entries = block_levels(key, extent, cuts, -0.22, 0.18) * entries
    return jnp.clip(entries, min=-bound, max=bound).astype(dtype)


def setup_inputs(seed: int = 0, part: int = 0) -> dict:
    splits = jax.random.split(jax.random.key(seed), 15)
    part_keys = jax.random.split(jax.random.fold_in(splits[14], part), 15)
    query_rows = normal_values(part_keys[0], (TOKENS, VALUE), 1.0, 6.0, ((0, 4), (1, 4)))
    key_rows = normal_values(part_keys[1], (TOKENS, VALUE), 1.0, 6.0, ((0, 4), (1, 4)))
    value_rows = normal_values(part_keys[2], (TOKENS, VALUE), 1.0, 6.0, ((0, 4), (1, 4)))
    gate_rows = normal_values(part_keys[3], (TOKENS, VALUE), 1.0, 6.0, ((0, 4), (1, 4)))
    log_decay = draw_log_decay(jax.random.fold_in(jax.random.fold_in(splits[14], part), 71), part)
    head_gain = jnp.clip(1.0 + 0.18 * jax.random.normal(splits[5], (2, VALUE), jnp.float32), 0.1, 1.9)
    out_weight = normal_values(splits[6], (VALUE, D), VALUE ** -0.5, 0.1875, ((0, 4),))
    residual = normal_values(part_keys[7], (TOKENS, D), 1.0, 6.0, ((0, 4),))
    norm_gain = jnp.clip(1.0 + 0.18 * jax.random.normal(splits[8], (D,), jnp.float32), 0.099609375, 1.8984375).astype(jnp.bfloat16)
    gate_weight = normal_values(splits[9], (D, FF), D ** -0.5, 0.125, ((0, 4), (1, 4)))
    up_weight = normal_values(splits[10], (D, FF), D ** -0.5, 0.125, ((0, 4), (1, 4)))
    down_weight = normal_values(splits[11], (D, FF), FF ** -0.5, 0.078125, ((0, 4), (1, 4)))
    gate_taps = normal_values(splits[12], (3, FF), 3 ** -0.5, 3.5, ((1, 4),))
    up_taps = normal_values(splits[13], (3, FF), 3 ** -0.5, 3.5, ((1, 4),))
    return {"query_rows": query_rows, "key_rows": key_rows, "value_rows": value_rows, "gate_rows": gate_rows, "log_decay": log_decay, "head_gain": head_gain, "out_weight": out_weight, "residual": residual, "norm_gain": norm_gain, "gate_weight": gate_weight, "up_weight": up_weight, "down_weight": down_weight, "gate_taps": gate_taps, "up_taps": up_taps}


FULL_PRECISION = lax.Precision.HIGHEST
GROUP_EPS = 1e-05
NORM_EPS = 1e-06

def scan_retention(query_all, key_all, value_all, log_rates):
    length, head_count, head_width = query_all.shape
    block_len = math.gcd(length, 512)
    block_count = length // block_len
    query_blocks = query_all.reshape(block_count, block_len, head_count, head_width)
    key_blocks = key_all.reshape(block_count, block_len, head_count, head_width)
    value_blocks = value_all.reshape(block_count, block_len, head_count, head_width)
    rate_blocks = log_rates.T.reshape(block_count, block_len, head_count)
    lower_mask = jnp.arange(block_len)[:, None] >= jnp.arange(block_len)[None, :]

    def block_step(carry_state, inputs):
        query_blk, key_blk, value_blk, rate_blk = inputs
        cumul = jnp.cumsum(rate_blk, axis=0)
        gap_logs = cumul[:, None, :] - cumul[None, :, :]
        decay_mask = jnp.where(lower_mask[:, :, None], jnp.exp(jnp.minimum(gap_logs, 0.0)), 0.0)
        scores = jnp.einsum('thd,shd->tsh', query_blk, key_blk, precision=FULL_PRECISION) * decay_mask
        inner_part = jnp.einsum('tsh,she->the', scores, value_blk, precision=FULL_PRECISION)
        carried = jnp.einsum('thd,hde->the', query_blk * jnp.exp(cumul)[:, :, None], carry_state, precision=FULL_PRECISION)
        last_cumul = cumul[-1]
        key_decayed = key_blk * jnp.exp(last_cumul[None, :] - cumul)[:, :, None]
        new_state = carry_state * jnp.exp(last_cumul)[:, None, None] + jnp.einsum('shd,she->hde', key_decayed, value_blk, precision=FULL_PRECISION)
        return (new_state, inner_part + carried)
    zero_state = jnp.zeros((head_count, head_width, head_width), jnp.float32)
    ignored, block_outs = lax.scan(block_step, zero_state, (query_blocks, key_blocks, value_blocks, rate_blocks))
    return block_outs.reshape(length, head_count, head_width)

def group_norm(values):
    length, head_count, head_width = values.shape
    centre = values - lax.optimization_barrier(jnp.mean(values, axis=2, keepdims=True))
    spread = lax.optimization_barrier(jnp.mean(centre * centre, axis=2, keepdims=True))
    return (centre * lax.rsqrt(spread + GROUP_EPS)).reshape(length, head_count * head_width)

def rms_scale(middle, gain):
    values = middle.astype(jnp.float32)
    multiplier = lax.rsqrt(lax.optimization_barrier(jnp.mean(values * values, axis=1, keepdims=True)) + NORM_EPS)
    return (values * multiplier * gain.astype(jnp.float32)).astype(jnp.bfloat16)

def reference(query_rows, key_rows, value_rows, gate_rows, log_decay, head_gain, out_weight, residual, norm_gain, gate_weight, up_weight, down_weight, gate_taps, up_taps):
    key_scale = HEAD ** (-0.5)
    query_all = query_rows.astype(jnp.float32).reshape(TOKENS, RETENTION_HEADS, HEAD)
    key_all = key_rows.astype(jnp.float32).reshape(TOKENS, RETENTION_HEADS, HEAD) * key_scale
    value_all = value_rows.astype(jnp.float32).reshape(TOKENS, RETENTION_HEADS, HEAD)
    ahead_out = scan_retention(query_all, key_all, value_all, log_decay[0])
    behind_out = scan_retention(query_all[::-1], key_all[::-1], value_all[::-1], log_decay[1][:, ::-1])[::-1]
    combined = group_norm(ahead_out) * head_gain[0] + group_norm(behind_out) * head_gain[1]
    mixed_heads = (jax.nn.silu(gate_rows.astype(jnp.float32)) * combined).astype(jnp.bfloat16)
    attended = jnp.dot(mixed_heads, out_weight, preferred_element_type=jnp.float32)
    middle = lax.optimization_barrier((residual.astype(jnp.float32) + attended).astype(jnp.bfloat16))
    normed = rms_scale(middle, norm_gain)
    model_width = normed.shape[1]
    zero_row = jnp.zeros((1, model_width), jnp.bfloat16)
    padded = jnp.concatenate([zero_row, normed, zero_row], axis=0)
    block_len = math.gcd(TOKENS, 512)
    taps_gate = gate_taps.astype(jnp.float32)
    taps_up = up_taps.astype(jnp.float32)

    def one_block(block_index):
        first_row = (block_index * block_len).astype(jnp.int32)
        rows_with_rims = lax.dynamic_slice_in_dim(padded, first_row, block_len + 2, 0)
        pre_gate = lax.optimization_barrier(jnp.dot(rows_with_rims, gate_weight, preferred_element_type=jnp.float32).astype(jnp.bfloat16)).astype(jnp.float32)
        pre_up = lax.optimization_barrier(jnp.dot(rows_with_rims, up_weight, preferred_element_type=jnp.float32).astype(jnp.bfloat16)).astype(jnp.float32)
        conv_gate = taps_gate[0] * pre_gate[:-2] + taps_gate[1] * pre_gate[1:-1] + taps_gate[2] * pre_gate[2:]
        conv_up = taps_up[0] * pre_up[:-2] + taps_up[1] * pre_up[1:-1] + taps_up[2] * pre_up[2:]
        hidden = (jax.nn.silu(conv_gate) * conv_up).astype(jnp.bfloat16)
        ff_out = lax.dot_general(hidden, down_weight, (((1,), (1,)), ((), ())), preferred_element_type=jnp.float32)
        middle_rows = lax.dynamic_slice_in_dim(middle, first_row, block_len, 0).astype(jnp.float32)
        return (middle_rows + ff_out).astype(jnp.bfloat16)
    block_outs = lax.map(one_block, jnp.arange(TOKENS // block_len).astype(jnp.int32))
    return block_outs.reshape(TOKENS, model_width)
```

```python
import functools
import math

import jax
import jax.numpy as jnp
from jax import lax
from jax.experimental import pallas as pl
from jax.experimental.pallas import tpu as pltpu
from jax.sharding import PartitionSpec as P

HEAD = 128


FULL_PRECISION = lax.Precision.HIGHEST
GROUP_EPS = 1e-05
NORM_EPS = 1e-06


def prefix(value, axis, join, neutral, backward):
    count, mine = (lax.axis_size(axis), lax.axis_index(axis))
    pieces = jax.tree.map(lambda part: lax.all_gather(part, axis), value)
    if backward:
        pieces = jax.tree.map(lambda part: part[::-1], pieces)
        mine = count - 1 - mine
    running = jax.tree.map(
        lambda part, zero: jnp.full_like(part, 0) + jnp.asarray(zero, part.dtype), value, neutral
    )

    def lap(position, running):
        longer = join(running, jax.tree.map(lambda part: part[position], pieces))
        return jax.tree.map(lambda new, old: jnp.where(position < mine, new, old), longer, running)

    return lax.fori_loop(0, count - 1, lap, running)


def padded_2(shard, sides, width):
    for axis, dim in sides:
        size, length = (lax.axis_size(axis), shard.shape[dim])
        up = [(i, (i + 1) % size) for i in range(size - 1)]
        down = [(j, i) for i, j in up]
        last = lax.slice_in_dim(shard, length - width, length, axis=dim)
        initial = lax.slice_in_dim(shard, 0, width, axis=dim)
        before = lax.ppermute(last, axis, up)
        after = lax.ppermute(initial, axis, down)
        shard = jnp.concatenate([before, shard, after], axis=dim)
    return shard


def state_combine(earlier, later):
    return (earlier[0] * later[0], earlier[1] * later[0][:, None, None] + later[1])


def group_norm(values):
    length, head_count, head_width = values.shape
    centre = values - jnp.mean(values, axis=2, keepdims=True)
    spread = jnp.mean(centre * centre, axis=2, keepdims=True)
    return (centre * lax.rsqrt(spread + GROUP_EPS)).reshape(length, head_count * head_width)


def rms_scale(middle, gain):
    values = middle.astype(jnp.float32)
    multiplier = lax.rsqrt(jnp.mean(values * values, axis=1, keepdims=True) + NORM_EPS)
    return (values * multiplier * gain.astype(jnp.float32)).astype(jnp.bfloat16)


def local_retention(query_all, key_all, value_all, log_rates):
    length, head_count, head_width = query_all.shape
    block_len = math.gcd(length, 512)
    block_count = length // block_len
    cumul = jnp.cumsum(log_rates, axis=1).T
    query_block = query_all.reshape(block_count, block_len, head_count, head_width)
    key_block = key_all.reshape(block_count, block_len, head_count, head_width)
    value_block = value_all.reshape(block_count, block_len, head_count, head_width)
    cumul_block = cumul.reshape(block_count, block_len, head_count)
    before = jnp.concatenate(
        [jnp.zeros((1, head_count), jnp.float32), cumul_block[:-1, -1]], axis=0
    )
    local_cumul = cumul_block - before[:, None, :]
    gap_logs = local_cumul[:, :, None, :] - local_cumul[:, None, :, :]
    lower_mask = (jnp.arange(block_len)[:, None] >= jnp.arange(block_len)[None, :])[
        None, :, :, None
    ]
    decay_mask = jnp.where(lower_mask, jnp.exp(jnp.minimum(gap_logs, 0.0)), 0.0)
    scores = (
        jnp.einsum("bthd,bshd->btsh", query_block, key_block, precision=FULL_PRECISION) * decay_mask
    )
    inner_part = jnp.einsum("btsh,bshe->bthe", scores, value_block, precision=FULL_PRECISION)
    to_end = jnp.exp(local_cumul[:, -1:, :] - local_cumul)
    block_states = jnp.einsum(
        "bshd,bshe->bhde", key_block * to_end[..., None], value_block, precision=FULL_PRECISION
    )
    block_decay = jnp.exp(local_cumul[:, -1, :])

    def carry_step(carry_state, inputs):
        return (carry_state * inputs[0][:, None, None] + inputs[1], carry_state)

    zero_state = jnp.zeros((head_count, head_width, head_width), jnp.float32)
    end_state, entering = lax.scan(carry_step, zero_state, (block_decay, block_states))
    carried = jnp.einsum(
        "bthd,bhde->bthe",
        query_block * jnp.exp(local_cumul)[..., None],
        entering,
        precision=FULL_PRECISION,
    )
    output = (inner_part + carried).reshape(length, head_count, head_width)
    return (output, end_state, cumul, jnp.exp(cumul[-1]))


def with_incoming(output, query_all, cumul, incoming):
    return output + jnp.einsum(
        "thd,hde->the", query_all * jnp.exp(cumul)[:, :, None], incoming, precision=FULL_PRECISION
    )


def shards(
    query_rows,
    key_rows,
    value_rows,
    gate_rows,
    log_decay,
    head_gain,
    out_weight,
    residual,
    norm_gain,
    gate_weight,
    up_weight,
    down_weight,
    gate_taps,
    up_taps,
):
    pair_local = jnp.concatenate([gate_weight, up_weight], axis=1)
    row_count = query_rows.shape[0]
    head_count = query_rows.shape[1] // HEAD
    key_scale = HEAD ** (-0.5)
    query_all = query_rows.astype(jnp.float32).reshape(row_count, head_count, HEAD)
    key_all = key_rows.astype(jnp.float32).reshape(row_count, head_count, HEAD) * key_scale
    value_all = value_rows.astype(jnp.float32).reshape(row_count, head_count, HEAD)
    identity = (
        jnp.ones((head_count,), jnp.float32),
        jnp.zeros((head_count, HEAD, HEAD), jnp.float32),
    )
    ahead_local, ahead_state, ahead_cumul, ahead_decay = local_retention(
        query_all, key_all, value_all, log_decay[0]
    )
    query_back = query_all[::-1]
    behind_local, behind_state, behind_cumul, behind_decay = local_retention(
        query_back, key_all[::-1], value_all[::-1], log_decay[1][:, ::-1]
    )
    ahead_in = prefix((ahead_decay, ahead_state), "sp", state_combine, identity, False)[1]
    behind_in = prefix((behind_decay, behind_state), "sp", state_combine, identity, True)[1]
    ahead_out = with_incoming(ahead_local, query_all, ahead_cumul, ahead_in)
    behind_out = with_incoming(behind_local, query_back, behind_cumul, behind_in)[::-1]
    combined = group_norm(ahead_out) * head_gain[0] + group_norm(behind_out) * head_gain[1]
    mixed_heads = (jax.nn.silu(gate_rows.astype(jnp.float32)) * combined).astype(jnp.bfloat16)
    gathered = (
        lax.all_gather(pair_local, "sp", axis=0, tiled=True),
        lax.all_gather(down_weight, "sp", axis=0, tiled=True),
    )
    pair_full, down_full = gathered
    share_rows = row_count // lax.axis_size("tp")
    own_start = lax.axis_index("tp") * share_rows
    picked = mixed_heads
    attended = lax.psum_scatter(
        jnp.dot(picked, out_weight, preferred_element_type=jnp.float32).astype(jnp.bfloat16),
        "tp",
        scatter_dimension=0,
        tiled=True,
    ).astype(jnp.float32)
    residual_own = lax.dynamic_slice_in_dim(residual, own_start, share_rows, 0)
    middle_own = lax.optimization_barrier(
        (residual_own.astype(jnp.float32) + attended).astype(jnp.bfloat16)
    )
    normed = rms_scale(middle_own, norm_gain)
    pre_both = jnp.dot(
        lax.all_gather(normed, "tp", axis=0, tiled=True),
        pair_full,
        preferred_element_type=jnp.float32,
    ).astype(jnp.bfloat16)
    padded = padded_2(pre_both, (("sp", 0),), 1)
    half_width = gate_taps.shape[1]
    tap_table = jnp.concatenate([gate_taps, up_taps], axis=1).astype(jnp.float32)
    conv_out = (
        tap_table[0] * padded[:-2].astype(jnp.float32)
        + tap_table[1] * padded[1:-1].astype(jnp.float32)
        + tap_table[2] * padded[2:].astype(jnp.float32)
    )
    hidden = (jax.nn.silu(conv_out[:, :half_width]) * conv_out[:, half_width:]).astype(jnp.bfloat16)
    picked = hidden
    ff_out = lax.psum_scatter(
        lax.dot_general(
            picked, down_full, (((1,), (1,)), ((), ())), preferred_element_type=jnp.float32
        ).astype(jnp.bfloat16),
        "tp",
        scatter_dimension=0,
        tiled=True,
    ).astype(jnp.float32)
    return (middle_own.astype(jnp.float32) + ff_out).astype(jnp.bfloat16)


def tile_split(lanes, spans):
    least, rest = divmod(lanes, spans)
    return least, rest


def block_kernel(
    spans,
    shares,
    query_hbm,
    key_hbm,
    value_hbm,
    gate_hbm,
    rates_hbm,
    gains,
    residual_hbm,
    norm_gain,
    gate_taps,
    up_taps,
    out_hbm,
    fg_hbm,
    fu_hbm,
    down_hbm,
    result,
    query,
    key,
    value,
    gate,
    rates,
    residual,
    out_w,
    down_w,
    rate_all,
    state_send,
    state_recv,
    wide_a,
    wide_b,
    att_send,
    att_recv,
    middle_ref,
    norm_all,
    hid_all,
    tp_send,
    tp_recv,
    row_send,
    row_recv,
    local_sem,
    own_sem,
    state_sem,
    w_sem,
    relay_sem,
    att_sem,
    norm_sem,
    mate_sem,
    cross_sem,
    diag_sem,
    hid_sem,
    tp_sem,
    row_sem,
):
    side, me, lane = lax.axis_index("grp"), lax.axis_index("sp"), lax.axis_index("tp")
    rows, width = query.shape
    heads = width // HEAD
    share = rows // shares
    model = residual.shape[1]
    part_cols = model // spans
    half = part_cols // 2
    total = spans * rows
    lines = rates.shape[0]
    units = gate_taps.shape[1]
    least, rest = tile_split(units // 128, spans)
    f32, bf16 = jnp.float32, jnp.bfloat16
    mate = lane + 1 - 2 * lax.rem(lane, 2)
    cross = lax.rem(lane + shares // 2, shares)
    odd = lax.rem(lane, 2)
    sends = []

    def remote(src, dst, sems, **place):
        return pltpu.make_async_remote_copy(
            src_ref=src,
            dst_ref=dst,
            send_sem=sems.at[0],
            recv_sem=sems.at[1],
            device_id=place,
            device_id_type=pl.DeviceIdType.MESH,
        )

    def send(src, dst, sems, **place):
        copy = remote(src, dst, sems, **place)
        copy.start()
        sends.append(copy)
        return copy

    def span_at(step):
        return lax.rem(me + step, spans)

    def share_at(step):
        return lax.rem(lane + step, shares)

    def extra(span):
        return jnp.where(odd == 0, span < rest, span >= spans - rest)

    def first_col(span):
        before = jnp.where(
            odd == 0, jnp.minimum(span, rest), jnp.maximum(span - (spans - rest), 0)
        )
        return (span * least + before) * 128

    def cols_of(part, span):
        size = 128 if part else least * 128
        begin = jnp.minimum(first_col(span) + part * least * 128, units - size)
        return pl.ds(pl.multiple_of(begin, 128), size)

    barrier = pltpu.get_barrier_semaphore()
    peers = [{"grp": 1 - side}]
    peers += [{"sp": span_at(d)} for d in range(1, spans)]
    peers += [{"tp": share_at(d)} for d in range(1, shares)]
    for place in peers:
        pl.semaphore_signal(
            barrier, inc=1, device_id=place, device_id_type=pl.DeviceIdType.MESH
        )
    loads = [
        pltpu.make_async_copy(src, dst, local_sem.at[i])
        for i, (src, dst) in enumerate(
            (
                (rates_hbm, rates),
                (key_hbm, key),
                (value_hbm, value),
                (query_hbm, query),
                (gate_hbm, gate),
                (out_hbm, out_w),
                (residual_hbm, residual),
                (down_hbm, down_w),
            )
        )
    ]
    for load in loads:
        load.start()

    wides = (wide_a, wide_b)
    weights = (fg_hbm, fu_hbm)

    def own_copy(part, g):
        return pltpu.make_async_copy(
            weights[g].at[:, cols_of(part, me)],
            wides[part].at[g, pl.ds(pl.multiple_of(me * part_cols, part_cols), part_cols)],
            own_sem.at[part, g],
        )

    def half_rows(span):
        begin = span * part_cols + side * half
        return pl.ds(pl.multiple_of(begin, half), half)

    def weight_copy(part, d, g):
        to = span_at(d)
        return remote(
            weights[g].at[pl.ds(pl.multiple_of(side * half, half), half), cols_of(part, to)],
            wides[part].at[g, half_rows(me)],
            w_sem.at[part, d, g],
            sp=to,
        )

    def relay_copy(part, d, g):
        block = wides[part].at[g, half_rows(lax.rem(me + spans - d, spans))]
        return remote(block, block, relay_sem.at[part, d, g], grp=1 - side)

    def when_extra(part, span, step):
        if part:
            pl.when(extra(span))(step)
        else:
            step()

    def start_weights(part, d):
        def step():
            for g in range(2):
                weight_copy(part, d, g).start()

        when_extra(part, span_at(d), step)

    def relay_weights(part, d):
        def step():
            for g in range(2):
                weight_copy(part, d, g).wait_recv()
                relay_copy(part, d, g).start()

        when_extra(part, me, step)

    def own_weights(part, begin):
        def step():
            for g in range(2):
                if begin:
                    own_copy(part, g).start()
                else:
                    own_copy(part, g).wait()

        when_extra(part, me, step)

    for part in range(2):
        own_weights(part, True)

    with jax.named_scope("states"):
        loads[0].wait()
        low = lax.broadcasted_iota(jnp.int32, (rows, rows), 0)
        high = lax.broadcasted_iota(jnp.int32, (rows, rows), 1)
        rate = rates[...]

        def tall(table):
            return lax.dot_general(
                table.astype(f32),
                rate,
                (((1,), (1,)), ((), ())),
                precision=FULL_PRECISION,
                preferred_element_type=f32,
            )

        until = tall(low >= high)
        single = tall(low == high)
        after = tall(low < high)
        flat = jnp.dot(
            rate, (low <= high).astype(f32), precision=FULL_PRECISION, preferred_element_type=f32
        )
        loads[1].wait()
        loads[2].wait()

        def split(x):
            top = x.astype(bf16)
            return top, (x - top.astype(f32)).astype(bf16)

        for head in range(heads):
            cols = slice(head * HEAD, (head + 1) * HEAD)
            held = value[:, cols]
            for way in range(2):
                line = way * heads + head
                if way == 0:
                    weight = after[:, line : line + 1]
                else:
                    weight = until[:, line : line + 1] - single[:, line : line + 1]
                lifted = key[:, cols].astype(f32) * jnp.exp(jnp.minimum(weight, 0.0))
                state = jnp.zeros((HEAD, HEAD), f32)
                for piece in split(lifted):
                    state += lax.dot_general(
                        piece, held, (((0,), (0,)), ((), ())), preferred_element_type=f32
                    )
                state = state - jnp.mean(state, axis=1, keepdims=True)
                state_send[way, head] = state.astype(bf16)

    with jax.named_scope("barrier"):
        pl.semaphore_wait(barrier, len(peers))
    arrivals = []
    for d in range(1, spans):
        to = span_at(d)
        way = jnp.where(to > me, 0, 1)
        arrivals.append(send(rates, rate_all.at[me], state_sem.at[d, 0], sp=to))
        arrivals.append(
            send(state_send.at[way], state_recv.at[me], state_sem.at[d, 1], sp=to)
        )
    start_weights(0, 1)
    start_weights(0, 2)

    with jax.named_scope("inner"):
        loads[3].wait()
        inner = []
        for head in range(heads):
            cols = slice(head * HEAD, (head + 1) * HEAD)
            back = heads + head
            scores = lax.dot_general(
                query[:, cols],
                key[:, cols],
                (((1,), (1,)), ((), ())),
                preferred_element_type=f32,
            ) * (HEAD ** (-0.5))
            ahead_gap = until[:, head : head + 1] - flat[head : head + 1]
            behind_gap = (flat[back : back + 1] - rate[back : back + 1]) - (
                until[:, back : back + 1] - single[:, back : back + 1]
            )
            for gap, keep in ((ahead_gap, low >= high), (behind_gap, low <= high)):
                weighted = jnp.where(keep, jnp.exp(jnp.minimum(gap, 0.0)), 0.0) * scores
                out = jnp.zeros((rows, HEAD), f32)
                for piece in split(weighted):
                    out += jnp.dot(piece, value[:, cols], preferred_element_type=f32)
                inner.append(out)

    with jax.named_scope("state_wait"):
        for copy in arrivals:
            copy.wait_recv()
        loads[4].wait()
    with jax.named_scope("outer"):
        sums = [jnp.sum(rate_all[j], axis=1, keepdims=True) for j in range(spans)]
        mixed = []
        gaps = []
        for j in range(spans):
            ahead_far = jnp.zeros((lines, 1), f32)
            behind_far = jnp.zeros((lines, 1), f32)
            for i in range(spans):
                if i > j:
                    ahead_far += jnp.where(i < me, sums[i], 0.0)
                if i < j:
                    behind_far += jnp.where(i > me, sums[i], 0.0)
            gaps.append((ahead_far, behind_far))
        for head in range(heads):
            cols = slice(head * HEAD, (head + 1) * HEAD)
            back = heads + head
            ahead, behind = inner[2 * head], inner[2 * head + 1]
            for j in range(spans):
                product = jnp.dot(
                    query[:, cols], state_recv[j, head], preferred_element_type=f32
                ) * (HEAD ** (-0.5))
                near = until[:, head : head + 1] + gaps[j][0][head : head + 1]
                far = (
                    after[:, back : back + 1]
                    + single[:, back : back + 1]
                    + gaps[j][1][back : back + 1]
                )
                ahead += jnp.where(j < me, jnp.exp(jnp.minimum(near, 0.0)) * product, 0.0)
                behind += jnp.where(j > me, jnp.exp(jnp.minimum(far, 0.0)) * product, 0.0)
            sides = []
            for row, out in enumerate((ahead, behind)):
                centre = out - jnp.mean(out, axis=1, keepdims=True)
                spread = jnp.mean(centre * centre, axis=1, keepdims=True)
                sides.append(centre * lax.rsqrt(spread + GROUP_EPS) * gains[row : row + 1, cols])
            level = gate[:, cols].astype(f32)
            mixed.append(((level / (1.0 + jnp.exp(-level))) * (sides[0] + sides[1])).astype(bf16))
        mixed = jnp.concatenate(mixed, axis=1)

    def share_rows(index):
        return pl.ds(pl.multiple_of(index * share, share), share)

    with jax.named_scope("attend"):
        loads[5].wait()
        step_cols = math.gcd(model, 512)
        for at in range(0, model, step_cols):
            att_send[:, at : at + step_cols] = jnp.dot(
                mixed, out_w[:, at : at + step_cols], preferred_element_type=f32
            ).astype(bf16)
        arrivals = [
            send(
                att_send.at[share_rows(share_at(d))],
                att_recv.at[d],
                att_sem.at[d],
                tp=share_at(d),
            )
            for d in range(1, shares)
        ]
    with jax.named_scope("relay1"):
        relay_weights(0, 1)
    with jax.named_scope("attended_wait"):
        loads[6].wait()
        for copy in arrivals:
            copy.wait_recv()

    def token_rows(span, tp):
        return pl.ds(pl.multiple_of(span * rows + tp * share, share), share)

    with jax.named_scope("normed"):
        attended = att_send[share_rows(lane), :].astype(f32)
        for d in range(1, shares):
            attended = attended + att_recv[d].astype(f32)
        middle = (residual[share_rows(lane), :].astype(f32) + attended).astype(bf16)
        middle_ref[...] = middle
        middle = middle.astype(f32)
        factor = lax.rsqrt(jnp.mean(middle * middle, axis=1, keepdims=True) + NORM_EPS)
        normed = (middle * factor * norm_gain[...].astype(f32)).astype(bf16)
        norm_all[token_rows(me, lane), :] = normed

    steps = (1, -1)

    def origin(way, hop):
        return me - steps[way] * hop

    def inside(span):
        return (span >= 0) & (span < spans)

    def clamp(span):
        return jnp.clip(span, 0, spans - 1)

    def passes(way, hop):
        return inside(origin(way, hop)) & inside(me + steps[way])

    def norm_copy(way, hop):
        block = norm_all.at[token_rows(clamp(origin(way, hop)), lane)]
        return remote(
            block, block, norm_sem.at[way, hop], sp=clamp(me + steps[way])
        )

    def mate_copy(span):
        block = norm_all.at[token_rows(span, lane)]
        return remote(block, block, mate_sem.at[span], tp=mate)

    def cross_copy(span):
        block = norm_all.at[token_rows(span, lane)]
        return remote(block, block, cross_sem.at[span], tp=cross)

    def diag_copy(span):
        block = norm_all.at[token_rows(span, cross)]
        return remote(block, block, diag_sem.at[span], tp=mate)

    def spread_block(way, hop):
        if hop + 1 >= spans:
            return

        @pl.when(passes(way, hop))
        def _():
            norm_copy(way, hop).start()

    def norm_hop(hop):
        for way in range(2):

            @pl.when(inside(origin(way, hop)))
            def _():
                norm_copy(way, hop - 1).wait_recv()
                spread_block(way, hop)
                cross_copy(clamp(origin(way, hop))).start()
                mate_copy(clamp(origin(way, hop))).start()

    def cross_hop(hop):
        for way in range(2 if hop else 1):

            @pl.when(inside(origin(way, hop)))
            def _():
                cross_copy(clamp(origin(way, hop))).wait_recv()
                diag_copy(clamp(origin(way, hop))).start()

    with jax.named_scope("norm0"):
        for way in range(2):
            spread_block(way, 0)
        cross_copy(me).start()
        mate_copy(me).start()
        start_weights(0, 3)
    with jax.named_scope("relay2"):
        relay_weights(0, 2)
    for hop in range(1, spans):
        with jax.named_scope("norm_hop"):
            norm_hop(hop)
            start_weights(1, hop)
            cross_hop(hop - 1)
    with jax.named_scope("norm_last"):
        cross_hop(spans - 1)
        for span in range(spans):
            mate_copy(span).wait_recv()
            diag_copy(span).wait_recv()
    with jax.named_scope("relay3"):
        relay_weights(0, 3)
        own_weights(0, False)
        for d in range(1, spans):
            for g in range(2):
                relay_copy(0, d, g).wait_recv()

    row_at = lax.broadcasted_iota(jnp.int32, (total, 1), 0)

    def compute_hidden(part):
        cols = cols_of(part, me)
        convs = []
        for g, taps in enumerate((gate_taps, up_taps)):
            here = jnp.dot(norm_all[...], wides[part][g], preferred_element_type=f32)
            here = here.astype(bf16).astype(f32)
            earlier, later = pltpu.roll(here, 1, 0), pltpu.roll(here, total - 1, 0)
            earlier = jnp.where(row_at == 0, 0.0, earlier)
            later = jnp.where(row_at == total - 1, 0.0, later)
            weight = taps[:, cols].astype(f32)
            convs.append(weight[0:1] * earlier + weight[1:2] * here + weight[2:3] * later)
        hidden = ((convs[0] / (1.0 + jnp.exp(-convs[0]))) * convs[1]).astype(bf16)
        hid_all[:, cols] = hidden

    def hidden_copy(part, way, hop, b):
        block = hid_all.at[pl.ds(b * rows, rows), cols_of(part, clamp(origin(way, hop)))]
        return remote(
            block, block, hid_sem.at[part, way, hop, b], sp=clamp(me + steps[way])
        )

    def has(part, span):
        return inside(span) & extra(clamp(span)) if part else inside(span)

    def hidden_start(part, way, hop, b):
        if hop + 1 >= spans:
            return

        @pl.when(passes(way, hop) & has(part, origin(way, hop)))
        def _():
            hidden_copy(part, way, hop, b).start()

    def hidden_pass(part, hop, b):
        for way in range(2):

            @pl.when(has(part, origin(way, hop)))
            def _():
                hidden_copy(part, way, hop - 1, b).wait_recv()

            hidden_start(part, way, hop, b)

    with jax.named_scope("hidden_a"):
        compute_hidden(0)
        for b in range(spans):
            for way in range(2):
                hidden_start(0, way, 0, b)
    with jax.named_scope("relay4"):
        for d in range(1, spans):
            relay_weights(1, d)
    with jax.named_scope("relay5"):

        @pl.when(extra(me))
        def _():
            for d in range(1, spans):
                for g in range(2):
                    relay_copy(1, d, g).wait_recv()

        own_weights(1, False)
    with jax.named_scope("hidden_b"):

        @pl.when(extra(me))
        def _():
            compute_hidden(1)

        for b in range(spans):
            for way in range(2):
                hidden_start(1, way, 0, b)
    with jax.named_scope("pass_a"):
        for hop in range(1, spans):
            for b in range(spans):
                hidden_pass(0, hop, b)
    loads[7].wait()
    fans = {}
    for b in range(spans):
        with jax.named_scope("pass_b"):
            for hop in range(1, spans):
                hidden_pass(1, hop, b)
        with jax.named_scope("down"):
            tp_send[b] = lax.dot_general(
                hid_all[b * rows : (b + 1) * rows, :],
                down_w[...],
                (((1,), (1,)), ((), ())),
                preferred_element_type=f32,
            ).astype(bf16)
            for d in range(1, shares):
                fans[b, d] = send(
                    tp_send.at[b, share_rows(share_at(d))],
                    tp_recv.at[b, d],
                    tp_sem.at[b, d],
                    tp=share_at(d),
                )

    def row_out(b):
        d = lax.rem(b - me + spans, spans)
        return remote(row_send.at[b], row_recv.at[me], row_sem.at[d], sp=b)

    for b in range(spans):
        with jax.named_scope("rows"):
            summed = tp_send[b, share_rows(lane), :].astype(f32)
            for d in range(1, shares):
                fans[b, d].wait_recv()
                summed = summed + tp_recv[b, d].astype(f32)
            row_send[b] = summed.astype(bf16)

            @pl.when(b != me)
            def _():
                row_out(b).start()

            @pl.when(b == me)
            def _():
                row_recv[me] = row_send[b]

    with jax.named_scope("final"):
        for d in range(1, spans):
            row_out(span_at(d)).wait_recv()
        for j in range(spans):
            cols = slice(j * part_cols, (j + 1) * part_cols)
            result[:, cols] = (
                middle_ref[:, cols].astype(f32) + row_recv[j].astype(f32)
            ).astype(bf16)
    with jax.named_scope("drain"):
        for copy in sends:
            copy.wait_send()
        for part in range(2):
            for d in range(1, spans):

                def sent():
                    for g in range(2):
                        weight_copy(part, d, g).wait_send()

                def relayed():
                    for g in range(2):
                        relay_copy(part, d, g).wait_send()

                when_extra(part, span_at(d), sent)
                when_extra(part, me, relayed)
        for span in range(spans):
            cross_copy(span).wait_send()
            mate_copy(span).wait_send()
            diag_copy(span).wait_send()

            @pl.when(span != me)
            def _():
                row_out(span).wait_send()

        for way in range(2):
            for hop in range(spans - 1):

                @pl.when(passes(way, hop))
                def _():
                    norm_copy(way, hop).wait_send()

                for part in range(2):

                    @pl.when(passes(way, hop) & has(part, origin(way, hop)))
                    def _():
                        for b in range(spans):
                            hidden_copy(part, way, hop, b).wait_send()


def fused_block(
    query_rows,
    key_rows,
    value_rows,
    gate_rows,
    log_decay,
    head_gain,
    out_weight,
    residual,
    norm_gain,
    gate_weight,
    up_weight,
    down_weight,
    gate_taps,
    up_taps,
):
    spans, shares = (lax.axis_size("sp"), lax.axis_size("tp"))
    rows, width = query_rows.shape
    model = residual.shape[1]
    units = gate_weight.shape[1]
    part_cols, share = (model // spans, rows // shares)
    total = spans * rows
    least, rest = tile_split(units // 128, spans)
    lines = log_decay.shape[0] * log_decay.shape[1]
    heads = width // HEAD
    rates = log_decay.reshape(lines, rows)
    f32, bf16 = jnp.float32, jnp.bfloat16
    far = pl.BlockSpec(memory_space=pl.ANY)
    near = pl.BlockSpec(memory_space=pltpu.VMEM)
    dma = pltpu.SemaphoreType.DMA
    vmem = pltpu.VMEM
    return pl.pallas_call(
        functools.partial(block_kernel, spans, shares),
        out_shape=jax.ShapeDtypeStruct((share, model), bf16),
        in_specs=[far] * 5 + [near, far] + [near] * 3 + [far] * 4,
        out_specs=pl.BlockSpec(memory_space=pltpu.VMEM),
        scratch_shapes=[
            vmem((rows, width), bf16),
            vmem((rows, width), bf16),
            vmem((rows, width), bf16),
            vmem((rows, width), bf16),
            vmem((lines, rows), f32),
            vmem((rows, model), bf16),
            vmem(out_weight.shape, bf16),
            vmem(down_weight.shape, bf16),
            vmem((spans, lines, rows), f32),
            vmem((2, heads, HEAD, HEAD), bf16),
            vmem((spans, heads, HEAD, HEAD), bf16),
            vmem((2, model, least * 128), bf16),
            vmem((2, model, 128), bf16),
            vmem((rows, model), bf16),
            vmem((shares, share, model), bf16),
            vmem((share, model), bf16),
            vmem((total, model), bf16),
            vmem((total, units), bf16),
            vmem((spans, rows, part_cols), bf16),
            vmem((spans, shares, share, part_cols), bf16),
            vmem((spans, share, part_cols), bf16),
            vmem((spans, share, part_cols), bf16),
            dma((8,)),
            dma((2, 2)),
            dma((spans, 2, 2)),
            dma((2, spans, 2, 2)),
            dma((2, spans, 2, 2)),
            dma((shares, 2)),
            dma((2, spans, 2)),
            dma((spans, 2)),
            dma((spans, 2)),
            dma((spans, 2)),
            dma((2, 2, spans, spans, 2)),
            dma((spans, shares, 2)),
            dma((spans, 2)),
        ],
        compiler_params=pltpu.CompilerParams(collective_id=0, has_side_effects=True),
    )(
        query_rows,
        key_rows,
        value_rows,
        gate_rows,
        rates,
        head_gain,
        residual,
        norm_gain.reshape(1, model),
        gate_taps,
        up_taps,
        out_weight,
        gate_weight,
        up_weight,
        down_weight,
    )


def either(*args):
    spans, shares, twins = (lax.axis_size(name) for name in ("sp", "tp", "grp"))
    span_tokens = args[0].shape[0] * spans
    model_width = args[7].shape[1]
    lanes = args[9].shape[1] // 128
    if span_tokens < model_width and twins == 2 and shares == 4 and lanes >= spans:
        return fused_block(*args)
    return shards(*args)


def solution(mesh):
    in_specs = (
        P(("grp", "sp"), "tp"),
        P(("grp", "sp"), "tp"),
        P(("grp", "sp"), "tp"),
        P(("grp", "sp"), "tp"),
        P(None, "tp", ("grp", "sp")),
        P(None, "tp"),
        P("tp", None),
        P(("grp", "sp"), None),
        P(),
        P("sp", "tp"),
        P("sp", "tp"),
        P("sp", "tp"),
        P(None, "tp"),
        P(None, "tp"),
    )
    out_specs = P(("grp", "sp", "tp"), None)
    return jax.shard_map(either, mesh=mesh, in_specs=in_specs, out_specs=out_specs, check_vma=False)
```

```python
import functools
import math

import jax
import jax.numpy as jnp
from jax import lax
from jax.experimental import pallas as pl
from jax.experimental.pallas import tpu as pltpu
from jax.sharding import PartitionSpec as P

HEAD = 128


FULL_PRECISION = lax.Precision.HIGHEST
GROUP_EPS = 1e-05
NORM_EPS = 1e-06


def prefix(value, axis, join, neutral, backward):
    count, mine = (lax.axis_size(axis), lax.axis_index(axis))
    pieces = jax.tree.map(lambda part: lax.all_gather(part, axis), value)
    if backward:
        pieces = jax.tree.map(lambda part: part[::-1], pieces)
        mine = count - 1 - mine
    running = jax.tree.map(
        lambda part, zero: jnp.full_like(part, 0) + jnp.asarray(zero, part.dtype), value, neutral
    )

    def lap(position, running):
        longer = join(running, jax.tree.map(lambda part: part[position], pieces))
        return jax.tree.map(lambda new, old: jnp.where(position < mine, new, old), longer, running)

    return lax.fori_loop(0, count - 1, lap, running)


def padded_2(shard, sides, width):
    for axis, dim in sides:
        size, length = (lax.axis_size(axis), shard.shape[dim])
        up = [(i, (i + 1) % size) for i in range(size - 1)]
        down = [(j, i) for i, j in up]
        last = lax.slice_in_dim(shard, length - width, length, axis=dim)
        initial = lax.slice_in_dim(shard, 0, width, axis=dim)
        before = lax.ppermute(last, axis, up)
        after = lax.ppermute(initial, axis, down)
        shard = jnp.concatenate([before, shard, after], axis=dim)
    return shard


def state_combine(earlier, later):
    return (earlier[0] * later[0], earlier[1] * later[0][:, None, None] + later[1])


def group_norm(values):
    length, head_count, head_width = values.shape
    centre = values - jnp.mean(values, axis=2, keepdims=True)
    spread = jnp.mean(centre * centre, axis=2, keepdims=True)
    return (centre * lax.rsqrt(spread + GROUP_EPS)).reshape(length, head_count * head_width)


def rms_scale(middle, gain):
    values = middle.astype(jnp.float32)
    multiplier = lax.rsqrt(jnp.mean(values * values, axis=1, keepdims=True) + NORM_EPS)
    return (values * multiplier * gain.astype(jnp.float32)).astype(jnp.bfloat16)


def local_retention(query_all, key_all, value_all, log_rates):
    length, head_count, head_width = query_all.shape
    block_len = math.gcd(length, 512)
    block_count = length // block_len
    cumul = jnp.cumsum(log_rates, axis=1).T
    query_block = query_all.reshape(block_count, block_len, head_count, head_width)
    key_block = key_all.reshape(block_count, block_len, head_count, head_width)
    value_block = value_all.reshape(block_count, block_len, head_count, head_width)
    cumul_block = cumul.reshape(block_count, block_len, head_count)
    before = jnp.concatenate(
        [jnp.zeros((1, head_count), jnp.float32), cumul_block[:-1, -1]], axis=0
    )
    local_cumul = cumul_block - before[:, None, :]
    gap_logs = local_cumul[:, :, None, :] - local_cumul[:, None, :, :]
    lower_mask = (jnp.arange(block_len)[:, None] >= jnp.arange(block_len)[None, :])[
        None, :, :, None
    ]
    decay_mask = jnp.where(lower_mask, jnp.exp(jnp.minimum(gap_logs, 0.0)), 0.0)
    scores = (
        jnp.einsum("bthd,bshd->btsh", query_block, key_block, precision=FULL_PRECISION) * decay_mask
    )
    inner_part = jnp.einsum("btsh,bshe->bthe", scores, value_block, precision=FULL_PRECISION)
    to_end = jnp.exp(local_cumul[:, -1:, :] - local_cumul)
    block_states = jnp.einsum(
        "bshd,bshe->bhde", key_block * to_end[..., None], value_block, precision=FULL_PRECISION
    )
    block_decay = jnp.exp(local_cumul[:, -1, :])

    def carry_step(carry_state, inputs):
        return (carry_state * inputs[0][:, None, None] + inputs[1], carry_state)

    zero_state = jnp.zeros((head_count, head_width, head_width), jnp.float32)
    end_state, entering = lax.scan(carry_step, zero_state, (block_decay, block_states))
    carried = jnp.einsum(
        "bthd,bhde->bthe",
        query_block * jnp.exp(local_cumul)[..., None],
        entering,
        precision=FULL_PRECISION,
    )
    output = (inner_part + carried).reshape(length, head_count, head_width)
    return (output, end_state, cumul, jnp.exp(cumul[-1]))


def with_incoming(output, query_all, cumul, incoming):
    return output + jnp.einsum(
        "thd,hde->the", query_all * jnp.exp(cumul)[:, :, None], incoming, precision=FULL_PRECISION
    )


def shards(
    query_rows,
    key_rows,
    value_rows,
    gate_rows,
    log_decay,
    head_gain,
    out_weight,
    residual,
    norm_gain,
    gate_weight,
    up_weight,
    down_weight,
    gate_taps,
    up_taps,
):
    pair_local = jnp.concatenate([gate_weight, up_weight], axis=1)
    row_count = query_rows.shape[0]
    head_count = query_rows.shape[1] // HEAD
    key_scale = HEAD ** (-0.5)
    query_all = query_rows.astype(jnp.float32).reshape(row_count, head_count, HEAD)
    key_all = key_rows.astype(jnp.float32).reshape(row_count, head_count, HEAD) * key_scale
    value_all = value_rows.astype(jnp.float32).reshape(row_count, head_count, HEAD)
    identity = (
        jnp.ones((head_count,), jnp.float32),
        jnp.zeros((head_count, HEAD, HEAD), jnp.float32),
    )
    ahead_local, ahead_state, ahead_cumul, ahead_decay = local_retention(
        query_all, key_all, value_all, log_decay[0]
    )
    query_back = query_all[::-1]
    behind_local, behind_state, behind_cumul, behind_decay = local_retention(
        query_back, key_all[::-1], value_all[::-1], log_decay[1][:, ::-1]
    )
    ahead_in = prefix((ahead_decay, ahead_state), "sp", state_combine, identity, False)[1]
    behind_in = prefix((behind_decay, behind_state), "sp", state_combine, identity, True)[1]
    ahead_out = with_incoming(ahead_local, query_all, ahead_cumul, ahead_in)
    behind_out = with_incoming(behind_local, query_back, behind_cumul, behind_in)[::-1]
    combined = group_norm(ahead_out) * head_gain[0] + group_norm(behind_out) * head_gain[1]
    mixed_heads = (jax.nn.silu(gate_rows.astype(jnp.float32)) * combined).astype(jnp.bfloat16)
    gathered = (
        lax.all_gather(pair_local, "sp", axis=0, tiled=True),
        lax.all_gather(down_weight, "sp", axis=0, tiled=True),
    )
    pair_full, down_full = gathered
    share_rows = row_count // lax.axis_size("tp")
    own_start = lax.axis_index("tp") * share_rows
    picked = mixed_heads
    attended = lax.psum_scatter(
        jnp.dot(picked, out_weight, preferred_element_type=jnp.float32).astype(jnp.bfloat16),
        "tp",
        scatter_dimension=0,
        tiled=True,
    ).astype(jnp.float32)
    residual_own = lax.dynamic_slice_in_dim(residual, own_start, share_rows, 0)
    middle_own = lax.optimization_barrier(
        (residual_own.astype(jnp.float32) + attended).astype(jnp.bfloat16)
    )
    normed = rms_scale(middle_own, norm_gain)
    pre_both = jnp.dot(
        lax.all_gather(normed, "tp", axis=0, tiled=True),
        pair_full,
        preferred_element_type=jnp.float32,
    ).astype(jnp.bfloat16)
    padded = padded_2(pre_both, (("sp", 0),), 1)
    half_width = gate_taps.shape[1]
    tap_table = jnp.concatenate([gate_taps, up_taps], axis=1).astype(jnp.float32)
    conv_out = (
        tap_table[0] * padded[:-2].astype(jnp.float32)
        + tap_table[1] * padded[1:-1].astype(jnp.float32)
        + tap_table[2] * padded[2:].astype(jnp.float32)
    )
    hidden = (jax.nn.silu(conv_out[:, :half_width]) * conv_out[:, half_width:]).astype(jnp.bfloat16)
    picked = hidden
    ff_out = lax.psum_scatter(
        lax.dot_general(
            picked, down_full, (((1,), (1,)), ((), ())), preferred_element_type=jnp.float32
        ).astype(jnp.bfloat16),
        "tp",
        scatter_dimension=0,
        tiled=True,
    ).astype(jnp.float32)
    return (middle_own.astype(jnp.float32) + ff_out).astype(jnp.bfloat16)


def tile_split(lanes, spans):
    least, rest = divmod(lanes, spans)
    return least, rest


def block_kernel(
    spans,
    shares,
    query_hbm,
    key_hbm,
    value_hbm,
    gate_hbm,
    rates_hbm,
    gains,
    residual_hbm,
    norm_gain,
    gate_taps,
    up_taps,
    out_hbm,
    fg_hbm,
    fu_hbm,
    down_hbm,
    result,
    query,
    key,
    value,
    gate,
    rates,
    residual,
    out_w,
    down_w,
    rate_all,
    state_send,
    state_recv,
    wide,
    att_send,
    att_recv,
    middle_ref,
    norm_all,
    hid_all,
    tp_send,
    tp_recv,
    row_send,
    row_recv,
    local_sem,
    own_sem,
    state_sem,
    w_sem,
    relay_sem,
    att_sem,
    norm_sem,
    mate_sem,
    cross_sem,
    diag_sem,
    hid_sem,
    tp_sem,
    row_sem,
):
    side, me, lane = lax.axis_index("grp"), lax.axis_index("sp"), lax.axis_index("tp")
    rows, width = query.shape
    heads = width // HEAD
    share = rows // shares
    model = residual.shape[1]
    part_cols = model // spans
    half = part_cols // 2
    total = spans * rows
    lines = rates.shape[0]
    units = gate_taps.shape[1]
    least, rest = tile_split(units // 128, spans)
    parts = least + (rest > 0)
    f32, bf16 = jnp.float32, jnp.bfloat16
    mate = lane + 1 - 2 * lax.rem(lane, 2)
    cross = lax.rem(lane + shares // 2, shares)
    odd = lax.rem(lane, 2)
    sends = []

    def remote(src, dst, sems, **place):
        return pltpu.make_async_remote_copy(
            src_ref=src,
            dst_ref=dst,
            send_sem=sems.at[0],
            recv_sem=sems.at[1],
            device_id=place,
            device_id_type=pl.DeviceIdType.MESH,
        )

    def send(src, dst, sems, **place):
        copy = remote(src, dst, sems, **place)
        copy.start()
        sends.append(copy)
        return copy

    def span_at(step):
        return lax.rem(me + step, spans)

    def share_at(step):
        return lax.rem(lane + step, shares)

    def extra(span):
        return jnp.where(odd == 0, span < rest, span >= spans - rest)

    def first_col(span):
        before = jnp.where(
            odd == 0, jnp.minimum(span, rest), jnp.maximum(span - (spans - rest), 0)
        )
        return (span * least + before) * 128

    def cols_of(part, span):
        begin = jnp.minimum(first_col(span) + part * 128, units - 128)
        return pl.ds(pl.multiple_of(begin, 128), 128)

    barrier = pltpu.get_barrier_semaphore()
    peers = [{"grp": 1 - side}]
    peers += [{"sp": span_at(d)} for d in range(1, spans)]
    peers += [{"tp": share_at(d)} for d in range(1, shares)]
    for place in peers:
        pl.semaphore_signal(
            barrier, inc=1, device_id=place, device_id_type=pl.DeviceIdType.MESH
        )
    loads = [
        pltpu.make_async_copy(src, dst, local_sem.at[i])
        for i, (src, dst) in enumerate(
            (
                (rates_hbm, rates),
                (key_hbm, key),
                (value_hbm, value),
                (query_hbm, query),
                (gate_hbm, gate),
                (out_hbm, out_w),
                (residual_hbm, residual),
                (down_hbm, down_w),
            )
        )
    ]
    for load in loads:
        load.start()

    weights = (fg_hbm, fu_hbm)

    def lanes(g):
        return slice(g * 128, (g + 1) * 128)

    def own_copy(part, g):
        return pltpu.make_async_copy(
            weights[g].at[:, cols_of(part, me)],
            wide.at[part, pl.ds(pl.multiple_of(me * part_cols, part_cols), part_cols), lanes(g)],
            own_sem.at[part],
        )

    def own_wait(part):
        block = wide.at[part, pl.ds(pl.multiple_of(me * part_cols, part_cols), part_cols)]
        return pltpu.make_async_copy(block, block, own_sem.at[part])

    def half_rows(span):
        begin = span * part_cols + side * half
        return pl.ds(pl.multiple_of(begin, half), half)

    def weight_copy(part, d, g):
        to = span_at(d)
        return remote(
            weights[g].at[pl.ds(pl.multiple_of(side * half, half), half), cols_of(part, to)],
            wide.at[part, half_rows(me), lanes(g)],
            w_sem.at[part, d - 1],
            sp=to,
        )

    def relay_copy(part, d):
        block = wide.at[part, half_rows(lax.rem(me + spans - d, spans))]
        return remote(block, block, relay_sem.at[part, d - 1], grp=1 - side)

    def weight_wait(part, d):
        block = wide.at[part, half_rows(lax.rem(me + spans - d, spans))]
        return remote(block, block, w_sem.at[part, d - 1], sp=span_at(d))

    def when_extra(part, span, step):
        if part == least:
            pl.when(extra(span))(step)
        else:
            step()

    def start_weights(part, d):
        def step():
            for g in range(2):
                weight_copy(part, d, g).start()

        when_extra(part, span_at(d), step)

    def relay_weights(part, d):
        def step():
            weight_wait(part, d).wait_recv()
            relay_copy(part, d).start()

        when_extra(part, me, step)

    def own_weights(part):
        def step():
            for g in range(2):
                own_copy(part, g).start()

        when_extra(part, me, step)

    for part in range(parts):
        own_weights(part)

    with jax.named_scope("states"):
        loads[0].wait()
        low = lax.broadcasted_iota(jnp.int32, (rows, rows), 0)
        high = lax.broadcasted_iota(jnp.int32, (rows, rows), 1)
        rate = rates[...]

        def tall(table):
            return lax.dot_general(
                table.astype(f32),
                rate,
                (((1,), (1,)), ((), ())),
                precision=FULL_PRECISION,
                preferred_element_type=f32,
            )

        until = tall(low >= high)
        single = tall(low == high)
        after = tall(low < high)
        flat = jnp.dot(
            rate, (low <= high).astype(f32), precision=FULL_PRECISION, preferred_element_type=f32
        )
        loads[1].wait()
        loads[2].wait()

        def split(x):
            top = x.astype(bf16)
            return top, (x - top.astype(f32)).astype(bf16)

        for head in range(heads):
            cols = slice(head * HEAD, (head + 1) * HEAD)
            held = value[:, cols]
            for way in range(2):
                line = way * heads + head
                if way == 0:
                    weight = after[:, line : line + 1]
                else:
                    weight = until[:, line : line + 1] - single[:, line : line + 1]
                lifted = key[:, cols].astype(f32) * jnp.exp(jnp.minimum(weight, 0.0))
                state = jnp.zeros((HEAD, HEAD), f32)
                for piece in split(lifted):
                    state += lax.dot_general(
                        piece, held, (((0,), (0,)), ((), ())), preferred_element_type=f32
                    )
                state = state - jnp.mean(state, axis=1, keepdims=True)
                state_send[way, head] = state.astype(bf16)

    with jax.named_scope("barrier"):
        pl.semaphore_wait(barrier, len(peers))
    arrivals = []
    for d in range(1, spans):
        to = span_at(d)
        way = jnp.where(to > me, 0, 1)
        arrivals.append(send(rates, rate_all.at[me], state_sem.at[d - 1, 0], sp=to))
        arrivals.append(
            send(state_send.at[way], state_recv.at[me], state_sem.at[d - 1, 1], sp=to)
        )
    with jax.named_scope("inner"):
        loads[3].wait()
        inner = []
        for head in range(heads):
            cols = slice(head * HEAD, (head + 1) * HEAD)
            back = heads + head
            scores = lax.dot_general(
                query[:, cols],
                key[:, cols],
                (((1,), (1,)), ((), ())),
                preferred_element_type=f32,
            ) * (HEAD ** (-0.5))
            ahead_gap = until[:, head : head + 1] - flat[head : head + 1]
            behind_gap = (flat[back : back + 1] - rate[back : back + 1]) - (
                until[:, back : back + 1] - single[:, back : back + 1]
            )
            for gap, keep in ((ahead_gap, low >= high), (behind_gap, low <= high)):
                weighted = jnp.where(keep, jnp.exp(jnp.minimum(gap, 0.0)), 0.0) * scores
                out = jnp.zeros((rows, HEAD), f32)
                for piece in split(weighted):
                    out += jnp.dot(piece, value[:, cols], preferred_element_type=f32)
                inner.append(out)

    with jax.named_scope("state_wait"):
        for copy in arrivals:
            copy.wait_recv()
        loads[4].wait()
        start_weights(0, 1)
        start_weights(0, 2)
    with jax.named_scope("outer"):
        sums = [jnp.sum(rate_all[j], axis=1, keepdims=True) for j in range(spans)]
        mixed = []
        gaps = []
        for j in range(spans):
            ahead_far = jnp.zeros((lines, 1), f32)
            behind_far = jnp.zeros((lines, 1), f32)
            for i in range(spans):
                if i > j:
                    ahead_far += jnp.where(i < me, sums[i], 0.0)
                if i < j:
                    behind_far += jnp.where(i > me, sums[i], 0.0)
            gaps.append((ahead_far, behind_far))
        for head in range(heads):
            cols = slice(head * HEAD, (head + 1) * HEAD)
            back = heads + head
            ahead, behind = inner[2 * head], inner[2 * head + 1]
            for j in range(spans):
                product = jnp.dot(
                    query[:, cols], state_recv[j, head], preferred_element_type=f32
                ) * (HEAD ** (-0.5))
                near = until[:, head : head + 1] + gaps[j][0][head : head + 1]
                far = (
                    after[:, back : back + 1]
                    + single[:, back : back + 1]
                    + gaps[j][1][back : back + 1]
                )
                ahead += jnp.where(j < me, jnp.exp(jnp.minimum(near, 0.0)) * product, 0.0)
                behind += jnp.where(j > me, jnp.exp(jnp.minimum(far, 0.0)) * product, 0.0)
            sides = []
            for row, out in enumerate((ahead, behind)):
                centre = out - jnp.mean(out, axis=1, keepdims=True)
                spread = jnp.mean(centre * centre, axis=1, keepdims=True)
                sides.append(centre * lax.rsqrt(spread + GROUP_EPS) * gains[row : row + 1, cols])
            level = gate[:, cols].astype(f32)
            mixed.append(((level / (1.0 + jnp.exp(-level))) * (sides[0] + sides[1])).astype(bf16))
        mixed = jnp.concatenate(mixed, axis=1)

    def share_rows(index):
        return pl.ds(pl.multiple_of(index * share, share), share)

    with jax.named_scope("attend"):
        loads[5].wait()
        step_cols = math.gcd(model, 512)
        for at in range(0, model, step_cols):
            att_send[:, at : at + step_cols] = jnp.dot(
                mixed, out_w[:, at : at + step_cols], preferred_element_type=f32
            ).astype(bf16)
        arrivals = [
            send(
                att_send.at[share_rows(share_at(d))],
                att_recv.at[d],
                att_sem.at[d - 1],
                tp=share_at(d),
            )
            for d in range(1, shares)
        ]
    with jax.named_scope("attended_wait"):
        loads[6].wait()
        for copy in arrivals:
            copy.wait_recv()

    def token_rows(span, tp):
        return pl.ds(pl.multiple_of(span * rows + tp * share, share), share)

    with jax.named_scope("normed"):
        attended = att_send[share_rows(lane), :].astype(f32)
        for d in range(1, shares):
            attended = attended + att_recv[d].astype(f32)
        middle = (residual[share_rows(lane), :].astype(f32) + attended).astype(bf16)
        middle_ref[...] = middle
        middle = middle.astype(f32)
        factor = lax.rsqrt(jnp.mean(middle * middle, axis=1, keepdims=True) + NORM_EPS)
        for at in range(0, model, 128):
            gain = norm_gain[at // 128 : at // 128 + 1, :].astype(f32)
            norm_all[token_rows(me, lane), at : at + 128] = (
                middle[:, at : at + 128] * factor * gain
            ).astype(bf16)

    steps = (1, -1)

    def origin(way, hop):
        return me - steps[way] * hop

    def inside(span):
        return (span >= 0) & (span < spans)

    def clamp(span):
        return jnp.clip(span, 0, spans - 1)

    def passes(way, hop):
        return inside(origin(way, hop)) & inside(me + steps[way])

    slabs = 2
    slab = share // slabs

    def slab_rows(span, tp, c):
        begin = span * rows + tp * share + c * slab
        return pl.ds(pl.multiple_of(begin, slab), slab)

    def norm_copy(way, hop, c):
        block = norm_all.at[slab_rows(clamp(origin(way, hop)), lane, c)]
        return remote(block, block, norm_sem.at[way, hop, c], sp=clamp(me + steps[way]))

    def mate_copy(span):
        block = norm_all.at[token_rows(span, lane)]
        return remote(block, block, mate_sem.at[span], tp=mate)

    def cross_copy(span):
        block = norm_all.at[token_rows(span, lane)]
        return remote(block, block, cross_sem.at[span], tp=cross)

    def diag_copy(span):
        block = norm_all.at[token_rows(span, cross)]
        return remote(block, block, diag_sem.at[span], tp=mate)

    def spread_block(way, hop, c):
        if hop + 1 >= spans:
            return

        @pl.when(passes(way, hop))
        def _():
            norm_copy(way, hop, c).start()

    def norm_hop(hop):
        for c in range(slabs):
            for way in range(2):

                @pl.when(inside(origin(way, hop)))
                def _():
                    norm_copy(way, hop - 1, c).wait_recv()
                    spread_block(way, hop, c)
                    if c == slabs - 1:
                        cross_copy(clamp(origin(way, hop))).start()
                        mate_copy(clamp(origin(way, hop))).start()

    def cross_hop(hop):
        for way in range(2 if hop else 1):

            @pl.when(inside(origin(way, hop)))
            def _():
                cross_copy(clamp(origin(way, hop))).wait_recv()
                diag_copy(clamp(origin(way, hop))).start()

    with jax.named_scope("norm0"):
        for c in range(slabs):
            for way in range(2):
                spread_block(way, 0, c)
        cross_copy(me).start()
        mate_copy(me).start()
    with jax.named_scope("relay1"):
        relay_weights(0, 1)
    with jax.named_scope("norm_hop1"):
        norm_hop(1)
        start_weights(0, 3)
    with jax.named_scope("cross0"):
        cross_hop(0)
    with jax.named_scope("relay2"):
        relay_weights(0, 2)
    with jax.named_scope("norm_hop2"):
        norm_hop(2)
        start_weights(1, 1)
    with jax.named_scope("cross1"):
        cross_hop(1)
    with jax.named_scope("relay3"):
        relay_weights(0, 3)
    with jax.named_scope("norm_hop3"):
        for hop in range(3, spans):
            norm_hop(hop)
        start_weights(1, 2)
        start_weights(1, 3)
    with jax.named_scope("cross2"):
        cross_hop(2)
    with jax.named_scope("cross3"):
        for hop in range(3, spans):
            cross_hop(hop)
    with jax.named_scope("relay_early"):
        relay_weights(1, 1)
    with jax.named_scope("mate_wait"):
        for span in range(spans):
            mate_copy(span).wait_recv()
            diag_copy(span).wait_recv()

    row_at = lax.broadcasted_iota(jnp.int32, (total, 1), 0)

    def twin_wait(part):
        def step():
            own_wait(part).wait()
            for d in range(1, spans):
                relay_copy(part, d).wait_recv()

        when_extra(part, me, step)

    def compute_hidden(part):
        cols = cols_of(part, me)
        both = jnp.dot(norm_all[...], wide[part], preferred_element_type=f32)
        here = both.astype(bf16).astype(f32)
        earlier, later = pltpu.roll(here, 1, 0), pltpu.roll(here, total - 1, 0)
        earlier = jnp.where(row_at == 0, 0.0, earlier)
        later = jnp.where(row_at == total - 1, 0.0, later)
        weight = jnp.concatenate(
            [gate_taps[:, cols].astype(f32), up_taps[:, cols].astype(f32)], axis=1
        )
        conv = weight[0:1] * earlier + weight[1:2] * here + weight[2:3] * later
        level = conv[:, :128]
        hid_all[:, cols] = ((level / (1.0 + jnp.exp(-level))) * conv[:, 128:]).astype(bf16)

    groups = max(spans // 2, 1)
    depth = spans // groups

    def blocks(part):
        return groups

    def hidden_copy(part, way, hop, b):
        size = total // blocks(part)
        block = hid_all.at[pl.ds(b * size, size), cols_of(part, clamp(origin(way, hop)))]
        return remote(
            block, block, hid_sem.at[part, way, hop, b], sp=clamp(me + steps[way])
        )

    def has(part, span):
        return inside(span) & extra(clamp(span)) if part == least else inside(span)

    def hidden_start(part, way, hop, b):
        if hop + 1 >= spans:
            return

        @pl.when(passes(way, hop) & has(part, origin(way, hop)))
        def _():
            hidden_copy(part, way, hop, b).start()

    def hidden_pass(part, hop, b):
        for way in range(2):

            @pl.when(has(part, origin(way, hop)))
            def _():
                hidden_copy(part, way, hop - 1, b).wait_recv()

            hidden_start(part, way, hop, b)

    def hidden_hop(part, hop):
        with jax.named_scope(f"pass{part}_{hop}"):
            for b in range(blocks(part)):
                hidden_pass(part, hop, b)

    def make_hidden(part):
        with jax.named_scope(f"twin{part}"):
            twin_wait(part)
        with jax.named_scope(f"hidden{part}"):
            if part == least:

                @pl.when(extra(me))
                def _():
                    compute_hidden(part)

            else:
                compute_hidden(part)
            for b in range(blocks(part)):
                for way in range(2):
                    hidden_start(part, way, 0, b)

    make_hidden(0)
    for part in range(1, parts):
        with jax.named_scope(f"relay_p{part}"):
            if part + 1 < parts:
                for d in range(1, spans):
                    start_weights(part + 1, d)
            for d in range(1 + (part == 1), spans):
                relay_weights(part, d)
        if part > 1:
            for hop in range(2, spans):
                hidden_hop(part - 2, hop)
        hidden_hop(part - 1, 1)
        make_hidden(part)
    if parts > 1:
        for hop in range(2, spans):
            hidden_hop(parts - 2, hop)
    loads[7].wait()
    fans = {}
    for b in range(groups):
        with jax.named_scope("pass_b"):
            for hop in range(1, spans):
                hidden_pass(parts - 1, hop, b)
        with jax.named_scope("down"):
            few = slice(b * depth, (b + 1) * depth)
            tp_send[few] = (
                lax.dot_general(
                    hid_all[b * depth * rows : (b + 1) * depth * rows, :],
                    down_w[...],
                    (((1,), (1,)), ((), ())),
                    preferred_element_type=f32,
                )
                .astype(bf16)
                .reshape(depth, rows, part_cols)
            )
            for d in range(1, shares):
                fans[b, d] = send(
                    tp_send.at[pl.ds(b * depth, depth), share_rows(share_at(d))],
                    tp_recv.at[d, pl.ds(b * depth, depth)],
                    tp_sem.at[b, d - 1],
                    tp=share_at(d),
                )

    def row_out(b):
        d = lax.rem(b - me + spans, spans)
        return remote(row_send.at[b], row_recv.at[me], row_sem.at[jnp.maximum(d - 1, 0)], sp=b)

    for b in range(spans):
        with jax.named_scope("rows"):
            summed = tp_send[b, share_rows(lane), :].astype(f32)
            for d in range(1, shares):
                if b % depth == 0:
                    fans[b // depth, d].wait_recv()
                summed = summed + tp_recv[d, b].astype(f32)
            row_send[b] = summed.astype(bf16)

            @pl.when(b != me)
            def _():
                row_out(b).start()

            @pl.when(b == me)
            def _():
                row_recv[me] = row_send[b]

    with jax.named_scope("final"):
        for d in range(1, spans):
            row_out(span_at(d)).wait_recv()
        for j in range(spans):
            cols = slice(j * part_cols, (j + 1) * part_cols)
            result[:, cols] = (
                middle_ref[:, cols].astype(f32) + row_recv[j].astype(f32)
            ).astype(bf16)
    with jax.named_scope("drain"):
        for copy in sends:
            copy.wait_send()
        for part in range(parts):
            for d in range(1, spans):

                def sent():
                    weight_wait(part, d).wait_send()

                def relayed():
                    relay_copy(part, d).wait_send()

                when_extra(part, span_at(d), sent)
                when_extra(part, me, relayed)
        for span in range(spans):
            cross_copy(span).wait_send()
            mate_copy(span).wait_send()
            diag_copy(span).wait_send()

            @pl.when(span != me)
            def _():
                row_out(span).wait_send()

        for way in range(2):
            for hop in range(spans - 1):

                @pl.when(passes(way, hop))
                def _():
                    for c in range(slabs):
                        norm_copy(way, hop, c).wait_send()

                for part in range(parts):

                    @pl.when(passes(way, hop) & has(part, origin(way, hop)))
                    def _():
                        for b in range(blocks(part)):
                            hidden_copy(part, way, hop, b).wait_send()


def fused_block(
    query_rows,
    key_rows,
    value_rows,
    gate_rows,
    log_decay,
    head_gain,
    out_weight,
    residual,
    norm_gain,
    gate_weight,
    up_weight,
    down_weight,
    gate_taps,
    up_taps,
):
    spans, shares = (lax.axis_size("sp"), lax.axis_size("tp"))
    rows, width = query_rows.shape
    model = residual.shape[1]
    units = gate_weight.shape[1]
    part_cols, share = (model // spans, rows // shares)
    total = spans * rows
    least, rest = tile_split(units // 128, spans)
    parts = least + (rest > 0)
    lines = log_decay.shape[0] * log_decay.shape[1]
    heads = width // HEAD
    rates = log_decay.reshape(lines, rows)
    f32, bf16 = jnp.float32, jnp.bfloat16
    far = pl.BlockSpec(memory_space=pl.ANY)
    near = pl.BlockSpec(memory_space=pltpu.VMEM)
    dma = pltpu.SemaphoreType.DMA
    vmem = pltpu.VMEM
    return pl.pallas_call(
        functools.partial(block_kernel, spans, shares),
        out_shape=jax.ShapeDtypeStruct((share, model), bf16),
        in_specs=[far] * 5 + [near, far] + [near] * 3 + [far] * 4,
        out_specs=pl.BlockSpec(memory_space=pltpu.VMEM),
        scratch_shapes=[
            vmem((rows, width), bf16),
            vmem((rows, width), bf16),
            vmem((rows, width), bf16),
            vmem((rows, width), bf16),
            vmem((lines, rows), f32),
            vmem((rows, model), bf16),
            vmem(out_weight.shape, bf16),
            vmem(down_weight.shape, bf16),
            vmem((spans, lines, rows), f32),
            vmem((2, heads, HEAD, HEAD), bf16),
            vmem((spans, heads, HEAD, HEAD), bf16),
            vmem((parts, model, 256), bf16),
            vmem((rows, model), bf16),
            vmem((shares, share, model), bf16),
            vmem((share, model), bf16),
            vmem((total, model), bf16),
            vmem((total, units), bf16),
            vmem((spans, rows, part_cols), bf16),
            vmem((shares, spans, share, part_cols), bf16),
            vmem((spans, share, part_cols), bf16),
            vmem((spans, share, part_cols), bf16),
            dma((8,)),
            dma((parts,)),
            dma((spans - 1, 2, 2)),
            dma((parts, spans - 1, 2)),
            dma((parts, spans - 1, 2)),
            dma((shares - 1, 2)),
            dma((2, spans - 1, 2, 2)),
            dma((spans, 2)),
            dma((spans, 2)),
            dma((spans, 2)),
            dma((parts, 2, spans - 1, spans // 2, 2)),
            dma((spans // 2, shares - 1, 2)),
            dma((spans - 1, 2)),
        ],
        compiler_params=pltpu.CompilerParams(collective_id=0, has_side_effects=True),
    )(
        query_rows,
        key_rows,
        value_rows,
        gate_rows,
        rates,
        head_gain,
        residual,
        norm_gain.reshape(model // 128, 128),
        gate_taps,
        up_taps,
        out_weight,
        gate_weight,
        up_weight,
        down_weight,
    )


def either(*args):
    spans, shares, twins = (lax.axis_size(name) for name in ("sp", "tp", "grp"))
    span_tokens = args[0].shape[0] * spans
    model_width = args[7].shape[1]
    lanes = args[9].shape[1] // 128
    even = spans % 2 == 0 and lanes >= spans
    if even and span_tokens < model_width and twins == 2 and shares == 4:
        return fused_block(*args)
    return shards(*args)


def solution(mesh):
    in_specs = (
        P(("grp", "sp"), "tp"),
        P(("grp", "sp"), "tp"),
        P(("grp", "sp"), "tp"),
        P(("grp", "sp"), "tp"),
        P(None, "tp", ("grp", "sp")),
        P(None, "tp"),
        P("tp", None),
        P(("grp", "sp"), None),
        P(),
        P("sp", "tp"),
        P("sp", "tp"),
        P("sp", "tp"),
        P(None, "tp"),
        P(None, "tp"),
    )
    out_specs = P(("grp", "sp", "tp"), None)
    return jax.shard_map(either, mesh=mesh, in_specs=in_specs, out_specs=out_specs, check_vma=False)
```

```python
import functools
import math

import jax
import jax.numpy as jnp
from jax import lax
from jax.experimental import pallas as pl
from jax.experimental.pallas import tpu as pltpu
from jax.sharding import PartitionSpec as P

HEAD = 128
GRANT = 40 << 20
SLABS = 4
EARLY = ((0, 3), (0, 1), (0, 2))
SECOND = ()
ORDER = (('r', 0, 1), ('n', 1), ('x', 0), ('r', 0, 2), ('n', 2), ('w', 1, 1), ('x', 1), ('r', 0, 3), ('w', 1, 2), ('w', 1, 3), ('n', 3), ('x', 2), ('x', 3), ('r', 1, 1), ('m',), ('H', 0), ('w', 2, 1), ('w', 2, 2), ('w', 2, 3), ('r', 1, 2), ('r', 1, 3), ('h', 0, 1, 0), ('h', 0, 1, 1), ('H', 1), ('r', 2, 1), ('r', 2, 2), ('r', 2, 3), ('h', 0, 2, 0), ('h', 0, 2, 1), ('h', 0, 3, 0), ('h', 0, 3, 1), ('h', 1, 1, 0), ('h', 1, 1, 1), ('H', 2), ('h', 1, 2, 0), ('h', 1, 2, 1), ('h', 1, 3, 0), ('h', 1, 3, 1), ('h', 2, 1, 0), ('h', 2, 2, 0), ('h', 2, 3, 0), ('D', 0), ('h', 2, 1, 1), ('h', 2, 2, 1), ('h', 2, 3, 1), ('D', 1), ('P', 0), ('P', 1), ('R', 0), ('R', 1))


FULL_PRECISION = lax.Precision.HIGHEST
GROUP_EPS = 1e-05
NORM_EPS = 1e-06


def prefix(value, axis, join, neutral, backward):
    count, mine = (lax.axis_size(axis), lax.axis_index(axis))
    pieces = jax.tree.map(lambda part: lax.all_gather(part, axis), value)
    if backward:
        pieces = jax.tree.map(lambda part: part[::-1], pieces)
        mine = count - 1 - mine
    running = jax.tree.map(
        lambda part, zero: jnp.full_like(part, 0) + jnp.asarray(zero, part.dtype), value, neutral
    )

    def lap(position, running):
        longer = join(running, jax.tree.map(lambda part: part[position], pieces))
        return jax.tree.map(lambda new, old: jnp.where(position < mine, new, old), longer, running)

    return lax.fori_loop(0, count - 1, lap, running)


def padded_2(shard, sides, width):
    for axis, dim in sides:
        size, length = (lax.axis_size(axis), shard.shape[dim])
        up = [(i, (i + 1) % size) for i in range(size - 1)]
        down = [(j, i) for i, j in up]
        last = lax.slice_in_dim(shard, length - width, length, axis=dim)
        initial = lax.slice_in_dim(shard, 0, width, axis=dim)
        before = lax.ppermute(last, axis, up)
        after = lax.ppermute(initial, axis, down)
        shard = jnp.concatenate([before, shard, after], axis=dim)
    return shard


def state_combine(earlier, later):
    return (earlier[0] * later[0], earlier[1] * later[0][:, None, None] + later[1])


def group_norm(values):
    length, head_count, head_width = values.shape
    centre = values - jnp.mean(values, axis=2, keepdims=True)
    spread = jnp.mean(centre * centre, axis=2, keepdims=True)
    return (centre * lax.rsqrt(spread + GROUP_EPS)).reshape(length, head_count * head_width)


def rms_scale(middle, gain):
    values = middle.astype(jnp.float32)
    multiplier = lax.rsqrt(jnp.mean(values * values, axis=1, keepdims=True) + NORM_EPS)
    return (values * multiplier * gain.astype(jnp.float32)).astype(jnp.bfloat16)


def local_retention(query_all, key_all, value_all, log_rates):
    length, head_count, head_width = query_all.shape
    block_len = math.gcd(length, 512)
    block_count = length // block_len
    cumul = jnp.cumsum(log_rates, axis=1).T
    query_block = query_all.reshape(block_count, block_len, head_count, head_width)
    key_block = key_all.reshape(block_count, block_len, head_count, head_width)
    value_block = value_all.reshape(block_count, block_len, head_count, head_width)
    cumul_block = cumul.reshape(block_count, block_len, head_count)
    before = jnp.concatenate(
        [jnp.zeros((1, head_count), jnp.float32), cumul_block[:-1, -1]], axis=0
    )
    local_cumul = cumul_block - before[:, None, :]
    gap_logs = local_cumul[:, :, None, :] - local_cumul[:, None, :, :]
    lower_mask = (jnp.arange(block_len)[:, None] >= jnp.arange(block_len)[None, :])[
        None, :, :, None
    ]
    decay_mask = jnp.where(lower_mask, jnp.exp(jnp.minimum(gap_logs, 0.0)), 0.0)
    scores = (
        jnp.einsum("bthd,bshd->btsh", query_block, key_block, precision=FULL_PRECISION) * decay_mask
    )
    inner_part = jnp.einsum("btsh,bshe->bthe", scores, value_block, precision=FULL_PRECISION)
    to_end = jnp.exp(local_cumul[:, -1:, :] - local_cumul)
    block_states = jnp.einsum(
        "bshd,bshe->bhde", key_block * to_end[..., None], value_block, precision=FULL_PRECISION
    )
    block_decay = jnp.exp(local_cumul[:, -1, :])

    def carry_step(carry_state, inputs):
        return (carry_state * inputs[0][:, None, None] + inputs[1], carry_state)

    zero_state = jnp.zeros((head_count, head_width, head_width), jnp.float32)
    end_state, entering = lax.scan(carry_step, zero_state, (block_decay, block_states))
    carried = jnp.einsum(
        "bthd,bhde->bthe",
        query_block * jnp.exp(local_cumul)[..., None],
        entering,
        precision=FULL_PRECISION,
    )
    output = (inner_part + carried).reshape(length, head_count, head_width)
    return (output, end_state, cumul, jnp.exp(cumul[-1]))


def with_incoming(output, query_all, cumul, incoming):
    return output + jnp.einsum(
        "thd,hde->the", query_all * jnp.exp(cumul)[:, :, None], incoming, precision=FULL_PRECISION
    )


def shards(
    query_rows,
    key_rows,
    value_rows,
    gate_rows,
    log_decay,
    head_gain,
    out_weight,
    residual,
    norm_gain,
    gate_weight,
    up_weight,
    down_weight,
    gate_taps,
    up_taps,
):
    pair_local = jnp.concatenate([gate_weight, up_weight], axis=1)
    row_count = query_rows.shape[0]
    head_count = query_rows.shape[1] // HEAD
    key_scale = HEAD ** (-0.5)
    query_all = query_rows.astype(jnp.float32).reshape(row_count, head_count, HEAD)
    key_all = key_rows.astype(jnp.float32).reshape(row_count, head_count, HEAD) * key_scale
    value_all = value_rows.astype(jnp.float32).reshape(row_count, head_count, HEAD)
    identity = (
        jnp.ones((head_count,), jnp.float32),
        jnp.zeros((head_count, HEAD, HEAD), jnp.float32),
    )
    ahead_local, ahead_state, ahead_cumul, ahead_decay = local_retention(
        query_all, key_all, value_all, log_decay[0]
    )
    query_back = query_all[::-1]
    behind_local, behind_state, behind_cumul, behind_decay = local_retention(
        query_back, key_all[::-1], value_all[::-1], log_decay[1][:, ::-1]
    )
    ahead_in = prefix((ahead_decay, ahead_state), "sp", state_combine, identity, False)[1]
    behind_in = prefix((behind_decay, behind_state), "sp", state_combine, identity, True)[1]
    ahead_out = with_incoming(ahead_local, query_all, ahead_cumul, ahead_in)
    behind_out = with_incoming(behind_local, query_back, behind_cumul, behind_in)[::-1]
    combined = group_norm(ahead_out) * head_gain[0] + group_norm(behind_out) * head_gain[1]
    mixed_heads = (jax.nn.silu(gate_rows.astype(jnp.float32)) * combined).astype(jnp.bfloat16)
    gathered = (
        lax.all_gather(pair_local, "sp", axis=0, tiled=True),
        lax.all_gather(down_weight, "sp", axis=0, tiled=True),
    )
    pair_full, down_full = gathered
    share_rows = row_count // lax.axis_size("tp")
    own_start = lax.axis_index("tp") * share_rows
    picked = mixed_heads
    attended = lax.psum_scatter(
        jnp.dot(picked, out_weight, preferred_element_type=jnp.float32).astype(jnp.bfloat16),
        "tp",
        scatter_dimension=0,
        tiled=True,
    ).astype(jnp.float32)
    residual_own = lax.dynamic_slice_in_dim(residual, own_start, share_rows, 0)
    middle_own = lax.optimization_barrier(
        (residual_own.astype(jnp.float32) + attended).astype(jnp.bfloat16)
    )
    normed = rms_scale(middle_own, norm_gain)
    pre_both = jnp.dot(
        lax.all_gather(normed, "tp", axis=0, tiled=True),
        pair_full,
        preferred_element_type=jnp.float32,
    ).astype(jnp.bfloat16)
    padded = padded_2(pre_both, (("sp", 0),), 1)
    half_width = gate_taps.shape[1]
    tap_table = jnp.concatenate([gate_taps, up_taps], axis=1).astype(jnp.float32)
    conv_out = (
        tap_table[0] * padded[:-2].astype(jnp.float32)
        + tap_table[1] * padded[1:-1].astype(jnp.float32)
        + tap_table[2] * padded[2:].astype(jnp.float32)
    )
    hidden = (jax.nn.silu(conv_out[:, :half_width]) * conv_out[:, half_width:]).astype(jnp.bfloat16)
    picked = hidden
    ff_out = lax.psum_scatter(
        lax.dot_general(
            picked, down_full, (((1,), (1,)), ((), ())), preferred_element_type=jnp.float32
        ).astype(jnp.bfloat16),
        "tp",
        scatter_dimension=0,
        tiled=True,
    ).astype(jnp.float32)
    return (middle_own.astype(jnp.float32) + ff_out).astype(jnp.bfloat16)


def tile_split(lanes, spans):
    least, rest = divmod(lanes, spans)
    return least, rest


def block_kernel(
    spans,
    shares,
    query_hbm,
    key_hbm,
    value_hbm,
    gate_hbm,
    rates_hbm,
    gains_hbm,
    residual_hbm,
    norm_gain_hbm,
    gate_taps_hbm,
    up_taps_hbm,
    out_hbm,
    fg_hbm,
    fu_hbm,
    down_hbm,
    result,
    query,
    key,
    value,
    gate,
    rates,
    residual,
    out_w,
    down_w,
    gains,
    norm_gain,
    gate_taps,
    up_taps,
    rate_all,
    state_send,
    state_recv,
    wide,
    att_send,
    att_recv,
    att_mid,
    middle_ref,
    norm_all,
    hid_all,
    tp_send,
    tp_recv,
    tp_mid,
    row_send,
    row_recv,
    local_sem,
    own_sem,
    state_sem,
    state_leave,
    w_sem,
    relay_sem,
    w_leave,
    relay_leave,
    att_sem,
    norm_sem,
    norm_leave,
    cross_sem,
    gather_sem,
    leave_sem,
    hid_sem,
    hid_leave,
    tp_sem,
    tp_leave,
    row_sem,
    row_leave,
):
    side, me, lane = lax.axis_index("grp"), lax.axis_index("sp"), lax.axis_index("tp")
    rows, width = query.shape
    heads = width // HEAD
    share = rows // shares
    model = residual.shape[1]
    part_cols = model // spans
    half = part_cols // 2
    total = spans * rows
    lines = rates.shape[0]
    units = gate_taps.shape[1]
    least, rest = tile_split(units // 128, spans)
    parts = least + (rest > 0)
    f32, bf16 = jnp.float32, jnp.bfloat16
    mate = lane + 1 - 2 * lax.rem(lane, 2)
    cross = lax.rem(lane + shares // 2, shares)
    odd = lax.rem(lane, 2)
    diag = cross + 1 - 2 * odd
    sends = []

    def remote(src, dst, sems, leave=None, **place):
        return pltpu.make_async_remote_copy(
            src_ref=src,
            dst_ref=dst,
            send_sem=sems.at[0] if leave is None else leave,
            recv_sem=sems.at[1] if leave is None else sems,
            device_id=place,
            device_id_type=pl.DeviceIdType.MESH,
        )

    def send(src, dst, sems, **place):
        copy = remote(src, dst, sems, **place)
        copy.start()
        sends.append(copy)
        return copy

    def span_at(step):
        return lax.rem(me + step, spans)

    def share_at(step):
        return lax.rem(lane + step, shares)

    def extra(span):
        return jnp.where(odd == 0, span < rest, span >= spans - rest)

    def first_col(span):
        before = jnp.where(
            odd == 0, jnp.minimum(span, rest), jnp.maximum(span - (spans - rest), 0)
        )
        return (span * least + before) * 128

    def cols_of(part, span):
        begin = jnp.minimum(first_col(span) + part * 128, units - 128)
        return pl.ds(pl.multiple_of(begin, 128), 128)

    barrier = pltpu.get_barrier_semaphore()
    peers = [{"grp": 1 - side}]
    peers += [{"sp": span_at(d)} for d in range(1, spans)]
    peers += [{"tp": share_at(d)} for d in range(1, shares)]
    for place in peers:
        pl.semaphore_signal(
            barrier, inc=1, device_id=place, device_id_type=pl.DeviceIdType.MESH
        )
    loads = [
        pltpu.make_async_copy(src, dst, local_sem.at[i])
        for i, (src, dst) in enumerate(
            (
                (rates_hbm, rates),
                (key_hbm, key),
                (value_hbm, value),
                (query_hbm, query),
                (gate_hbm, gate),
                (out_hbm, out_w),
                (residual_hbm, residual),
                (down_hbm, down_w),
                (gains_hbm, gains),
                (norm_gain_hbm, norm_gain),
                (gate_taps_hbm, gate_taps),
                (up_taps_hbm, up_taps),
            )
        )
    ]
    for load in loads:
        load.start()

    weights = (fg_hbm, fu_hbm)

    def lanes(g):
        return slice(g * 128, (g + 1) * 128)

    def own_copy(part, g):
        return pltpu.make_async_copy(
            weights[g].at[:, cols_of(part, me)],
            wide.at[part, pl.ds(pl.multiple_of(me * part_cols, part_cols), part_cols), lanes(g)],
            own_sem.at[part],
        )

    def own_wait(part):
        block = wide.at[part, pl.ds(pl.multiple_of(me * part_cols, part_cols), part_cols)]
        return pltpu.make_async_copy(block, block, own_sem.at[part])

    def half_rows(span):
        begin = span * part_cols + side * half
        return pl.ds(pl.multiple_of(begin, half), half)

    def leave_at(part, d):
        return part if part < least else least + d - 1

    def weight_copy(part, d, g):
        to = span_at(d)
        return remote(
            weights[g].at[pl.ds(pl.multiple_of(side * half, half), half), cols_of(part, to)],
            wide.at[part, half_rows(me), lanes(g)],
            w_sem.at[part, d - 1],
            w_leave.at[leave_at(part, d)],
            sp=to,
        )

    def relay_copy(part, d):
        block = wide.at[part, half_rows(lax.rem(me + spans - d, spans))]
        return remote(block, block, relay_sem.at[part, d - 1], relay_leave.at[part], grp=1 - side)

    def weight_wait(part, d):
        block = wide.at[part, half_rows(lax.rem(me + spans - d, spans))]
        sem = w_sem.at[part, d - 1]
        return remote(block, block, sem, w_leave.at[leave_at(part, d)], sp=span_at(d))

    def when_extra(part, span, step):
        if part == least:
            pl.when(extra(span))(step)
        else:
            step()

    def start_weights(part, d):
        def step():
            for g in range(2):
                weight_copy(part, d, g).start()

        when_extra(part, span_at(d), step)

    def relay_weights(part, d):
        def step():
            weight_wait(part, d).wait_recv()
            relay_copy(part, d).start()

        when_extra(part, me, step)

    def own_weights(part):
        def step():
            for g in range(2):
                own_copy(part, g).start()

        when_extra(part, me, step)

    for part in range(parts):
        own_weights(part)

    with jax.named_scope("states"):
        loads[0].wait()
        low = lax.broadcasted_iota(jnp.int32, (rows, rows), 0)
        high = lax.broadcasted_iota(jnp.int32, (rows, rows), 1)
        rate = rates[...]

        def tall(table):
            return lax.dot_general(
                table.astype(f32),
                rate,
                (((1,), (1,)), ((), ())),
                precision=FULL_PRECISION,
                preferred_element_type=f32,
            )

        until = tall(low >= high)
        single = tall(low == high)
        after = tall(low < high)
        flat = jnp.dot(
            rate, (low <= high).astype(f32), precision=FULL_PRECISION, preferred_element_type=f32
        )
        loads[1].wait()
        loads[2].wait()

        def split(x):
            top = x.astype(bf16)
            return top, (x - top.astype(f32)).astype(bf16)

        for head in range(heads):
            cols = slice(head * HEAD, (head + 1) * HEAD)
            held = value[:, cols]
            for way in range(2):
                line = way * heads + head
                if way == 0:
                    weight = after[:, line : line + 1]
                else:
                    weight = until[:, line : line + 1] - single[:, line : line + 1]
                lifted = key[:, cols].astype(f32) * jnp.exp(jnp.minimum(weight, 0.0))
                state = jnp.zeros((HEAD, HEAD), f32)
                for piece in split(lifted):
                    state += lax.dot_general(
                        piece, held, (((0,), (0,)), ((), ())), preferred_element_type=f32
                    )
                state = state - jnp.mean(state, axis=1, keepdims=True)
                state_send[way, head] = state.astype(bf16)

    with jax.named_scope("barrier"):
        pl.semaphore_wait(barrier, len(peers))
    arrivals = []
    for d in range(1, spans):
        to = span_at(d)
        way = jnp.where(to > me, 0, 1)
        arrivals.append(
            remote(rates, rate_all.at[me], state_sem.at[d - 1, 0], state_leave.at[0], sp=to)
        )
        arrivals.append(
            remote(
                state_send.at[way],
                state_recv.at[me],
                state_sem.at[d - 1, 1],
                state_leave.at[1],
                sp=to,
            )
        )
    for copy in arrivals:
        copy.start()

    with jax.named_scope("inner"):
        loads[3].wait()
        inner = []
        for head in range(heads):
            cols = slice(head * HEAD, (head + 1) * HEAD)
            back = heads + head
            scores = lax.dot_general(
                query[:, cols],
                key[:, cols],
                (((1,), (1,)), ((), ())),
                preferred_element_type=f32,
            ) * (HEAD ** (-0.5))
            ahead_gap = until[:, head : head + 1] - flat[head : head + 1]
            behind_gap = (flat[back : back + 1] - rate[back : back + 1]) - (
                until[:, back : back + 1] - single[:, back : back + 1]
            )
            for gap, keep in ((ahead_gap, low >= high), (behind_gap, low <= high)):
                weighted = jnp.where(keep, jnp.exp(jnp.minimum(gap, 0.0)), 0.0) * scores
                out = jnp.zeros((rows, HEAD), f32)
                for piece in split(weighted):
                    out += jnp.dot(piece, value[:, cols], preferred_element_type=f32)
                inner.append(out)

    with jax.named_scope("state_wait"):
        for copy in arrivals:
            copy.wait_recv()
        loads[4].wait()
        for load in loads[8:]:
            load.wait()
        for part, d in EARLY:
            start_weights(part, d)
    with jax.named_scope("outer"):
        sums = [jnp.sum(rate_all[j], axis=1, keepdims=True) for j in range(spans)]
        mixed = []
        gaps = []
        for j in range(spans):
            ahead_far = jnp.zeros((lines, 1), f32)
            behind_far = jnp.zeros((lines, 1), f32)
            for i in range(spans):
                if i > j:
                    ahead_far += jnp.where(i < me, sums[i], 0.0)
                if i < j:
                    behind_far += jnp.where(i > me, sums[i], 0.0)
            gaps.append((ahead_far, behind_far))
        for head in range(heads):
            cols = slice(head * HEAD, (head + 1) * HEAD)
            back = heads + head
            ahead, behind = inner[2 * head], inner[2 * head + 1]
            for j in range(spans):
                product = jnp.dot(
                    query[:, cols], state_recv[j, head], preferred_element_type=f32
                ) * (HEAD ** (-0.5))
                near = until[:, head : head + 1] + gaps[j][0][head : head + 1]
                far = (
                    after[:, back : back + 1]
                    + single[:, back : back + 1]
                    + gaps[j][1][back : back + 1]
                )
                ahead += jnp.where(j < me, jnp.exp(jnp.minimum(near, 0.0)) * product, 0.0)
                behind += jnp.where(j > me, jnp.exp(jnp.minimum(far, 0.0)) * product, 0.0)
            sides = []
            for row, out in enumerate((ahead, behind)):
                centre = out - jnp.mean(out, axis=1, keepdims=True)
                spread = jnp.mean(centre * centre, axis=1, keepdims=True)
                sides.append(centre * lax.rsqrt(spread + GROUP_EPS) * gains[row : row + 1, cols])
            level = gate[:, cols].astype(f32)
            mixed.append(((level / (1.0 + jnp.exp(-level))) * (sides[0] + sides[1])).astype(bf16))
        mixed = jnp.concatenate(mixed, axis=1)

    def share_rows(index):
        return pl.ds(pl.multiple_of(index * share, share), share)

    with jax.named_scope("attend"):
        loads[5].wait()
        step_cols = math.gcd(model, 512)
        for at in range(0, model, step_cols):
            att_send[:, at : at + step_cols] = jnp.dot(
                mixed, out_w[:, at : at + step_cols], preferred_element_type=f32
            ).astype(bf16)
        pairs = [
            send(att_send.at[share_rows(to)], att_recv.at[i], att_sem.at[i], tp=mate)
            for i, to in enumerate((diag, mate))
        ]
    for part, d in SECOND:
        start_weights(part, d)
    with jax.named_scope("attended_pair"):
        loads[6].wait()
        pairs[0].wait_recv()
        att_mid[...] = (
            att_send[share_rows(cross), :].astype(f32) + att_recv[0].astype(f32)
        ).astype(bf16)
        pairs.append(send(att_mid, att_recv.at[2], att_sem.at[2], tp=cross))
        pairs[1].wait_recv()
    with jax.named_scope("attended_wait"):
        pairs[2].wait_recv()

    def token_rows(span, tp):
        return pl.ds(pl.multiple_of(span * rows + tp * share, share), share)

    with jax.named_scope("normed"):
        attended = att_send[share_rows(lane), :].astype(f32)
        for i in range(1, 3):
            attended = attended + att_recv[i].astype(f32)
        middle = (residual[share_rows(lane), :].astype(f32) + attended).astype(bf16)
        middle_ref[...] = middle
        middle = middle.astype(f32)
        factor = lax.rsqrt(jnp.mean(middle * middle, axis=1, keepdims=True) + NORM_EPS)
        for at in range(0, model, 128):
            gain = norm_gain[at // 128 : at // 128 + 1, :].astype(f32)
            norm_all[token_rows(me, lane), at : at + 128] = (
                middle[:, at : at + 128] * factor * gain
            ).astype(bf16)

    steps = (1, -1)

    def origin(way, hop):
        return me - steps[way] * hop

    def inside(span):
        return (span >= 0) & (span < spans)

    def clamp(span):
        return jnp.clip(span, 0, spans - 1)

    def passes(way, hop):
        return inside(origin(way, hop)) & inside(me + steps[way])

    slab = model // SLABS

    def slab_of(span, tp, c):
        return norm_all.at[token_rows(span, tp), c * slab : (c + 1) * slab]

    def norm_copy(way, hop, c):
        block = slab_of(clamp(origin(way, hop)), lane, c)
        to = clamp(me + steps[way])
        return remote(block, block, norm_sem.at[way, hop, c], norm_leave.at[way, hop], sp=to)

    def mate_copy(span, c):
        block = slab_of(span, lane, c)
        return remote(block, block, gather_sem.at[0], leave_sem.at[0], tp=mate)

    def cross_copy(span, c):
        block = slab_of(span, lane, c)
        return remote(block, block, cross_sem.at[span, c], leave_sem.at[1], tp=cross)

    def diag_copy(span, c):
        block = slab_of(span, cross, c)
        return remote(block, block, gather_sem.at[1], leave_sem.at[2], tp=mate)

    def spread_block(way, hop, c):
        if hop + 1 >= spans:
            return

        @pl.when(passes(way, hop))
        def _():
            norm_copy(way, hop, c).start()

    def norm_hop(hop):
        for c in range(SLABS):
            for way in range(2):

                @pl.when(inside(origin(way, hop)))
                def _():
                    norm_copy(way, hop - 1, c).wait_recv()
                    spread_block(way, hop, c)
                    cross_copy(clamp(origin(way, hop)), c).start()
                    mate_copy(clamp(origin(way, hop)), c).start()

    def cross_hop(hop):
        for way in range(2 if hop else 1):

            @pl.when(inside(origin(way, hop)))
            def _():
                for c in range(SLABS):
                    cross_copy(clamp(origin(way, hop)), c).wait_recv()
                    diag_copy(clamp(origin(way, hop)), c).start()

    with jax.named_scope("norm0"):
        for c in range(SLABS):
            for way in range(2):
                spread_block(way, 0, c)
            cross_copy(me, c).start()
            mate_copy(me, c).start()
    def gather_wait():
        whole = norm_all.at[pl.ds(0, rows)]
        for i in range(2):
            remote(whole, whole, gather_sem.at[i], leave_sem.at[0], tp=mate).wait_recv()

    row_at = lax.broadcasted_iota(jnp.int32, (total, 1), 0)

    def twin_wait(part):
        def step():
            own_wait(part).wait()
            for d in range(1, spans):
                relay_copy(part, d).wait_recv()

        when_extra(part, me, step)

    def compute_hidden(part):
        cols = cols_of(part, me)
        both = jnp.dot(norm_all[...], wide[part], preferred_element_type=f32)
        here = both.astype(bf16).astype(f32)
        earlier, later = pltpu.roll(here, 1, 0), pltpu.roll(here, total - 1, 0)
        earlier = jnp.where(row_at == 0, 0.0, earlier)
        later = jnp.where(row_at == total - 1, 0.0, later)
        weight = jnp.concatenate(
            [gate_taps[:, cols].astype(f32), up_taps[:, cols].astype(f32)], axis=1
        )
        conv = weight[0:1] * earlier + weight[1:2] * here + weight[2:3] * later
        level = conv[:, :128]
        hid_all[:, cols] = ((level / (1.0 + jnp.exp(-level))) * conv[:, 128:]).astype(bf16)

    groups = max(spans // 2, 1)
    depth = spans // groups

    def blocks(part):
        return groups

    def hidden_copy(part, way, hop, b):
        size = total // blocks(part)
        block = hid_all.at[pl.ds(b * size, size), cols_of(part, clamp(origin(way, hop)))]
        return remote(
            block,
            block,
            hid_sem.at[part, way, hop, b],
            hid_leave.at[part, way, hop],
            sp=clamp(me + steps[way]),
        )

    def has(part, span):
        return inside(span) & extra(clamp(span)) if part == least else inside(span)

    def hidden_start(part, way, hop, b):
        if hop + 1 >= spans:
            return

        @pl.when(passes(way, hop) & has(part, origin(way, hop)))
        def _():
            hidden_copy(part, way, hop, b).start()

    def hidden_pass(part, hop, b):
        for way in range(2):

            @pl.when(has(part, origin(way, hop)))
            def _():
                hidden_copy(part, way, hop - 1, b).wait_recv()

            hidden_start(part, way, hop, b)

    def make_hidden(part):
        twin_wait(part)
        if part == least:

            @pl.when(extra(me))
            def _():
                compute_hidden(part)

        else:
            compute_hidden(part)
        for b in range(blocks(part)):
            for way in range(2):
                hidden_start(part, way, 0, b)

    pairs, crossing = {}, {}

    def down(b):
        few = pl.ds(b * depth, depth)
        if b == 0:
            loads[7].wait()
        tp_send[few] = (
            lax.dot_general(
                hid_all[b * depth * rows : (b + 1) * depth * rows, :],
                down_w[...],
                (((1,), (1,)), ((), ())),
                preferred_element_type=f32,
            )
            .astype(bf16)
            .reshape(depth, rows, part_cols)
        )
        pairs[b] = [
            remote(
                tp_send.at[few, share_rows(to)],
                tp_recv.at[i, few],
                tp_sem.at[b, i],
                tp_leave.at[0],
                tp=mate,
            )
            for i, to in enumerate((diag, mate))
        ]
        for copy in pairs[b]:
            copy.start()

    def cross_step(b):
        few = pl.ds(b * depth, depth)
        pairs[b][0].wait_recv()
        tp_mid[few] = (
            tp_send[few, share_rows(cross)].astype(f32) + tp_recv[0, few].astype(f32)
        ).astype(bf16)
        crossing[b] = remote(
            tp_mid.at[few], tp_recv.at[2, few], tp_sem.at[b, 2], tp_leave.at[0], tp=cross
        )
        crossing[b].start()
        pairs[b][1].wait_recv()

    def row_out(b):
        d = lax.rem(b - me + spans, spans)
        return remote(
            row_send.at[b],
            row_recv.at[me],
            row_sem.at[jnp.maximum(d - 1, 0)],
            row_leave.at[0],
            sp=b,
        )

    def row_step(group):
        crossing[group].wait_recv()
        for b in range(group * depth, (group + 1) * depth):
            summed = tp_send[b, share_rows(lane), :].astype(f32)
            for i in range(1, 3):
                summed = summed + tp_recv[i, b].astype(f32)
            row_send[b] = summed.astype(bf16)

            @pl.when(b != me)
            def _():
                row_out(b).start()

            @pl.when(b == me)
            def _():
                row_recv[me] = row_send[b]

    actions = {
        "n": norm_hop,
        "x": cross_hop,
        "w": start_weights,
        "r": relay_weights,
        "m": gather_wait,
        "H": make_hidden,
        "h": hidden_pass,
        "D": down,
        "P": cross_step,
        "R": row_step,
    }
    for name, *numbers in ORDER:
        with jax.named_scope(name + "".join(str(number) for number in numbers)):
            actions[name](*numbers)

    with jax.named_scope("final"):
        for d in range(1, spans):
            row_out(span_at(d)).wait_recv()
        for j in range(spans):
            cols = slice(j * part_cols, (j + 1) * part_cols)
            result[:, cols] = (
                middle_ref[:, cols].astype(f32) + row_recv[j].astype(f32)
            ).astype(bf16)
    with jax.named_scope("drain"):
        for copy in sends:
            copy.wait_send()
        for part in range(parts):
            if part < least:
                block = wide.at[part, pl.ds(0, (spans - 1) * half)]
                remote(
                    block, block, w_sem.at[part, 0], w_leave.at[part], sp=span_at(1)
                ).wait_send()
            for d in range(1, spans if part == least else 1):

                def sent():
                    weight_wait(part, d).wait_send()

                when_extra(part, span_at(d), sent)

            def relayed():
                block = wide.at[part, pl.ds(0, (spans - 1) * half)]
                remote(
                    block, block, relay_sem.at[part, 0], relay_leave.at[part], grp=1 - side
                ).wait_send()

            when_extra(part, me, relayed)
        whole = norm_all.at[pl.ds(0, rows)]
        for i in range(3):
            remote(whole, whole, gather_sem.at[0], leave_sem.at[i], tp=mate).wait_send()
        remote(state_recv.at[pl.ds(0, spans - 1)], state_recv.at[pl.ds(0, spans - 1)],
               state_sem.at[0, 1], state_leave.at[1], sp=span_at(1)).wait_send()
        remote(rate_all.at[pl.ds(0, spans - 1)], rate_all.at[pl.ds(0, spans - 1)],
               state_sem.at[0, 0], state_leave.at[0], sp=span_at(1)).wait_send()
        remote(tp_recv, tp_recv, tp_sem.at[0, 0], tp_leave.at[0], tp=mate).wait_send()
        remote(row_recv.at[pl.ds(0, spans - 1)], row_recv.at[pl.ds(0, spans - 1)],
               row_sem.at[0], row_leave.at[0], sp=span_at(1)).wait_send()
        for way in range(2):
            for hop in range(spans - 1):

                @pl.when(passes(way, hop))
                def _():
                    block = norm_all.at[pl.ds(0, share)]
                    remote(
                        block,
                        block,
                        norm_sem.at[way, hop, 0],
                        norm_leave.at[way, hop],
                        sp=clamp(me + steps[way]),
                    ).wait_send()

                for part in range(parts):

                    @pl.when(passes(way, hop) & has(part, origin(way, hop)))
                    def _():
                        block = hid_all.at[:, pl.ds(0, 128)]
                        remote(
                            block,
                            block,
                            hid_sem.at[part, way, hop, 0],
                            hid_leave.at[part, way, hop],
                            sp=clamp(me + steps[way]),
                        ).wait_send()


def fused_block(
    query_rows,
    key_rows,
    value_rows,
    gate_rows,
    log_decay,
    head_gain,
    out_weight,
    residual,
    norm_gain,
    gate_weight,
    up_weight,
    down_weight,
    gate_taps,
    up_taps,
):
    spans, shares = (lax.axis_size("sp"), lax.axis_size("tp"))
    rows, width = query_rows.shape
    model = residual.shape[1]
    units = gate_weight.shape[1]
    part_cols, share = (model // spans, rows // shares)
    total = spans * rows
    least, rest = tile_split(units // 128, spans)
    parts = least + (rest > 0)
    lines = log_decay.shape[0] * log_decay.shape[1]
    heads = width // HEAD
    rates = log_decay.reshape(lines, rows)
    f32, bf16 = jnp.float32, jnp.bfloat16
    far = pl.BlockSpec(memory_space=pltpu.HBM)
    dma = pltpu.SemaphoreType.DMA
    vmem = pltpu.VMEM
    return pl.pallas_call(
        functools.partial(block_kernel, spans, shares),
        out_shape=jax.ShapeDtypeStruct((share, model), bf16),
        in_specs=[far] * 14,
        out_specs=pl.BlockSpec(memory_space=pltpu.VMEM),
        scratch_shapes=[
            vmem((rows, width), bf16),
            vmem((rows, width), bf16),
            vmem((rows, width), bf16),
            vmem((rows, width), bf16),
            vmem((lines, rows), f32),
            vmem((rows, model), bf16),
            vmem(out_weight.shape, bf16),
            vmem(down_weight.shape, bf16),
            vmem(head_gain.shape, f32),
            vmem((model // 128, 128), bf16),
            vmem(gate_taps.shape, bf16),
            vmem(up_taps.shape, bf16),
            vmem((spans, lines, rows), f32),
            vmem((2, heads, HEAD, HEAD), bf16),
            vmem((spans, heads, HEAD, HEAD), bf16),
            vmem((parts, model, 256), bf16),
            vmem((rows, model), bf16),
            vmem((3, share, model), bf16),
            vmem((share, model), bf16),
            vmem((share, model), bf16),
            vmem((total, model), bf16),
            vmem((total, units), bf16),
            vmem((spans, rows, part_cols), bf16),
            vmem((3, spans, share, part_cols), bf16),
            vmem((spans, share, part_cols), bf16),
            vmem((spans, share, part_cols), bf16),
            vmem((spans, share, part_cols), bf16),
            dma((12,)),
            dma((parts,)),
            dma((spans - 1, 2)),
            dma((2,)),
            dma((parts, spans - 1)),
            dma((parts, spans - 1)),
            dma((least + spans - 1,)),
            dma((parts,)),
            dma((3, 2)),
            dma((2, spans - 1, SLABS)),
            dma((2, spans - 1)),
            dma((spans, SLABS)),
            dma((2,)),
            dma((3,)),
            dma((parts, 2, spans - 1, spans // 2)),
            dma((parts, 2, spans - 1)),
            dma((spans // 2, 3)),
            dma((1,)),
            dma((spans - 1,)),
            dma((1,)),
        ],
        compiler_params=pltpu.CompilerParams(
            collective_id=0, has_side_effects=True, vmem_limit_bytes=GRANT
        ),
    )(
        *(
            pltpu.with_memory_space_constraint(value, pltpu.HBM)
            for value in (
                query_rows,
                key_rows,
                value_rows,
                gate_rows,
                rates,
                head_gain,
                residual,
                norm_gain.reshape(model // 128, 128),
                gate_taps,
                up_taps,
                out_weight,
                gate_weight,
                up_weight,
                down_weight,
            )
        )
    )


def either(*args):
    spans, shares, twins = (lax.axis_size(name) for name in ("sp", "tp", "grp"))
    span_tokens = args[0].shape[0] * spans
    model_width = args[7].shape[1]
    lanes = args[9].shape[1] // 128
    fits = spans == 4 and lanes >= 2 * spans
    if fits and span_tokens < model_width and twins == 2 and shares == 4:
        return fused_block(*args)
    return shards(*args)


def solution(mesh):
    in_specs = (
        P(("grp", "sp"), "tp"),
        P(("grp", "sp"), "tp"),
        P(("grp", "sp"), "tp"),
        P(("grp", "sp"), "tp"),
        P(None, "tp", ("grp", "sp")),
        P(None, "tp"),
        P("tp", None),
        P(("grp", "sp"), None),
        P(),
        P("sp", "tp"),
        P("sp", "tp"),
        P("sp", "tp"),
        P(None, "tp"),
        P(None, "tp"),
    )
    out_specs = P(("grp", "sp", "tp"), None)
    return jax.shard_map(either, mesh=mesh, in_specs=in_specs, out_specs=out_specs, check_vma=False)
```

```python
import functools
import math

import jax
import jax.numpy as jnp
from jax import lax
from jax.experimental import pallas as pl
from jax.experimental.pallas import tpu as pltpu
from jax.sharding import PartitionSpec as P

HEAD = 128
GRANT = 40 << 20
SLABS = 4
PAIRED = False
SPLIT = 'even'
WAYS = (0, 1)
EARLY = ((0, 3), (0, 1), (0, 2))
SECOND = ()
ORDER = (('r', 0, 1), ('n', 1), ('x', 0), ('r', 0, 2), ('n', 2), ('w', 1, 1), ('x', 1), ('r', 0, 3), ('w', 1, 2), ('w', 1, 3), ('n', 3), ('x', 2), ('r', 1, 1), ('x', 3), ('m',), ('H', 0), ('w', 2, 1), ('r', 1, 3), ('w', 2, 2), ('r', 1, 2), ('w', 2, 3), ('h', 0, 1, 0), ('h', 0, 1, 1), ('H', 1), ('r', 2, 1), ('r', 2, 2), ('r', 2, 3), ('h', 0, 2, 0), ('h', 0, 2, 1), ('h', 0, 3, 0), ('h', 0, 3, 1), ('h', 1, 1, 0), ('h', 1, 1, 1), ('H', 2), ('h', 1, 2, 0), ('h', 1, 2, 1), ('h', 1, 3, 0), ('h', 1, 3, 1), ('h', 2, 1, 0), ('h', 2, 2, 0), ('h', 2, 3, 0), ('D', 0), ('h', 2, 1, 1), ('P', 0), ('h', 2, 2, 1), ('h', 2, 3, 1), ('D', 1), ('R', 0), ('P', 1), ('R', 1))


FULL_PRECISION = lax.Precision.HIGHEST
GROUP_EPS = 1e-05
NORM_EPS = 1e-06


def prefix(value, axis, join, neutral, backward):
    count, mine = (lax.axis_size(axis), lax.axis_index(axis))
    pieces = jax.tree.map(lambda part: lax.all_gather(part, axis), value)
    if backward:
        pieces = jax.tree.map(lambda part: part[::-1], pieces)
        mine = count - 1 - mine
    running = jax.tree.map(
        lambda part, zero: jnp.full_like(part, 0) + jnp.asarray(zero, part.dtype), value, neutral
    )

    def lap(position, running):
        longer = join(running, jax.tree.map(lambda part: part[position], pieces))
        return jax.tree.map(lambda new, old: jnp.where(position < mine, new, old), longer, running)

    return lax.fori_loop(0, count - 1, lap, running)


def padded_2(shard, sides, width):
    for axis, dim in sides:
        size, length = (lax.axis_size(axis), shard.shape[dim])
        up = [(i, (i + 1) % size) for i in range(size - 1)]
        down = [(j, i) for i, j in up]
        last = lax.slice_in_dim(shard, length - width, length, axis=dim)
        initial = lax.slice_in_dim(shard, 0, width, axis=dim)
        before = lax.ppermute(last, axis, up)
        after = lax.ppermute(initial, axis, down)
        shard = jnp.concatenate([before, shard, after], axis=dim)
    return shard


def state_combine(earlier, later):
    return (earlier[0] * later[0], earlier[1] * later[0][:, None, None] + later[1])


def group_norm(values):
    length, head_count, head_width = values.shape
    centre = values - jnp.mean(values, axis=2, keepdims=True)
    spread = jnp.mean(centre * centre, axis=2, keepdims=True)
    return (centre * lax.rsqrt(spread + GROUP_EPS)).reshape(length, head_count * head_width)


def rms_scale(middle, gain):
    values = middle.astype(jnp.float32)
    multiplier = lax.rsqrt(jnp.mean(values * values, axis=1, keepdims=True) + NORM_EPS)
    return (values * multiplier * gain.astype(jnp.float32)).astype(jnp.bfloat16)


def local_retention(query_all, key_all, value_all, log_rates):
    length, head_count, head_width = query_all.shape
    block_len = math.gcd(length, 512)
    block_count = length // block_len
    cumul = jnp.cumsum(log_rates, axis=1).T
    query_block = query_all.reshape(block_count, block_len, head_count, head_width)
    key_block = key_all.reshape(block_count, block_len, head_count, head_width)
    value_block = value_all.reshape(block_count, block_len, head_count, head_width)
    cumul_block = cumul.reshape(block_count, block_len, head_count)
    before = jnp.concatenate(
        [jnp.zeros((1, head_count), jnp.float32), cumul_block[:-1, -1]], axis=0
    )
    local_cumul = cumul_block - before[:, None, :]
    gap_logs = local_cumul[:, :, None, :] - local_cumul[:, None, :, :]
    lower_mask = (jnp.arange(block_len)[:, None] >= jnp.arange(block_len)[None, :])[
        None, :, :, None
    ]
    decay_mask = jnp.where(lower_mask, jnp.exp(jnp.minimum(gap_logs, 0.0)), 0.0)
    scores = (
        jnp.einsum("bthd,bshd->btsh", query_block, key_block, precision=FULL_PRECISION) * decay_mask
    )
    inner_part = jnp.einsum("btsh,bshe->bthe", scores, value_block, precision=FULL_PRECISION)
    to_end = jnp.exp(local_cumul[:, -1:, :] - local_cumul)
    block_states = jnp.einsum(
        "bshd,bshe->bhde", key_block * to_end[..., None], value_block, precision=FULL_PRECISION
    )
    block_decay = jnp.exp(local_cumul[:, -1, :])

    def carry_step(carry_state, inputs):
        return (carry_state * inputs[0][:, None, None] + inputs[1], carry_state)

    zero_state = jnp.zeros((head_count, head_width, head_width), jnp.float32)
    end_state, entering = lax.scan(carry_step, zero_state, (block_decay, block_states))
    carried = jnp.einsum(
        "bthd,bhde->bthe",
        query_block * jnp.exp(local_cumul)[..., None],
        entering,
        precision=FULL_PRECISION,
    )
    output = (inner_part + carried).reshape(length, head_count, head_width)
    return (output, end_state, cumul, jnp.exp(cumul[-1]))


def with_incoming(output, query_all, cumul, incoming):
    return output + jnp.einsum(
        "thd,hde->the", query_all * jnp.exp(cumul)[:, :, None], incoming, precision=FULL_PRECISION
    )


def shards(
    query_rows,
    key_rows,
    value_rows,
    gate_rows,
    log_decay,
    head_gain,
    out_weight,
    residual,
    norm_gain,
    gate_weight,
    up_weight,
    down_weight,
    gate_taps,
    up_taps,
):
    pair_local = jnp.concatenate([gate_weight, up_weight], axis=1)
    row_count = query_rows.shape[0]
    head_count = query_rows.shape[1] // HEAD
    key_scale = HEAD ** (-0.5)
    query_all = query_rows.astype(jnp.float32).reshape(row_count, head_count, HEAD)
    key_all = key_rows.astype(jnp.float32).reshape(row_count, head_count, HEAD) * key_scale
    value_all = value_rows.astype(jnp.float32).reshape(row_count, head_count, HEAD)
    identity = (
        jnp.ones((head_count,), jnp.float32),
        jnp.zeros((head_count, HEAD, HEAD), jnp.float32),
    )
    ahead_local, ahead_state, ahead_cumul, ahead_decay = local_retention(
        query_all, key_all, value_all, log_decay[0]
    )
    query_back = query_all[::-1]
    behind_local, behind_state, behind_cumul, behind_decay = local_retention(
        query_back, key_all[::-1], value_all[::-1], log_decay[1][:, ::-1]
    )
    ahead_in = prefix((ahead_decay, ahead_state), "sp", state_combine, identity, False)[1]
    behind_in = prefix((behind_decay, behind_state), "sp", state_combine, identity, True)[1]
    ahead_out = with_incoming(ahead_local, query_all, ahead_cumul, ahead_in)
    behind_out = with_incoming(behind_local, query_back, behind_cumul, behind_in)[::-1]
    combined = group_norm(ahead_out) * head_gain[0] + group_norm(behind_out) * head_gain[1]
    mixed_heads = (jax.nn.silu(gate_rows.astype(jnp.float32)) * combined).astype(jnp.bfloat16)
    gathered = (
        lax.all_gather(pair_local, "sp", axis=0, tiled=True),
        lax.all_gather(down_weight, "sp", axis=0, tiled=True),
    )
    pair_full, down_full = gathered
    share_rows = row_count // lax.axis_size("tp")
    own_start = lax.axis_index("tp") * share_rows
    picked = mixed_heads
    attended = lax.psum_scatter(
        jnp.dot(picked, out_weight, preferred_element_type=jnp.float32).astype(jnp.bfloat16),
        "tp",
        scatter_dimension=0,
        tiled=True,
    ).astype(jnp.float32)
    residual_own = lax.dynamic_slice_in_dim(residual, own_start, share_rows, 0)
    middle_own = lax.optimization_barrier(
        (residual_own.astype(jnp.float32) + attended).astype(jnp.bfloat16)
    )
    normed = rms_scale(middle_own, norm_gain)
    pre_both = jnp.dot(
        lax.all_gather(normed, "tp", axis=0, tiled=True),
        pair_full,
        preferred_element_type=jnp.float32,
    ).astype(jnp.bfloat16)
    padded = padded_2(pre_both, (("sp", 0),), 1)
    half_width = gate_taps.shape[1]
    tap_table = jnp.concatenate([gate_taps, up_taps], axis=1).astype(jnp.float32)
    conv_out = (
        tap_table[0] * padded[:-2].astype(jnp.float32)
        + tap_table[1] * padded[1:-1].astype(jnp.float32)
        + tap_table[2] * padded[2:].astype(jnp.float32)
    )
    hidden = (jax.nn.silu(conv_out[:, :half_width]) * conv_out[:, half_width:]).astype(jnp.bfloat16)
    picked = hidden
    ff_out = lax.psum_scatter(
        lax.dot_general(
            picked, down_full, (((1,), (1,)), ((), ())), preferred_element_type=jnp.float32
        ).astype(jnp.bfloat16),
        "tp",
        scatter_dimension=0,
        tiled=True,
    ).astype(jnp.float32)
    return (middle_own.astype(jnp.float32) + ff_out).astype(jnp.bfloat16)


def tile_counts(lanes, spans):
    if SPLIT == "ends":
        outer = lanes // spans
        near = (lanes - 2 * outer + 1) // 2
        far = lanes - 2 * outer - near
        even, odd = (outer, near, far, outer), (outer, far, near, outer)
    else:
        least, rest = divmod(lanes, spans)
        even = tuple(least + (j < rest) for j in range(spans))
        odd = even[::-1]
        if SPLIT == "middle":
            even, odd = (even[0], even[1], even[3], even[2]), (odd[1], odd[0], odd[2], odd[3])
    return even, odd


def block_kernel(
    spans,
    shares,
    query_hbm,
    key_hbm,
    value_hbm,
    gate_hbm,
    rates_hbm,
    gains_hbm,
    residual_hbm,
    norm_gain_hbm,
    gate_taps_hbm,
    up_taps_hbm,
    out_hbm,
    fg_hbm,
    fu_hbm,
    down_hbm,
    result,
    query,
    key,
    value,
    gate,
    rates,
    residual,
    out_w,
    down_w,
    gains,
    norm_gain,
    gate_taps,
    up_taps,
    rate_all,
    state_send,
    state_recv,
    wide,
    att_send,
    att_recv,
    att_mid,
    middle_ref,
    norm_all,
    hid_all,
    tp_send,
    tp_recv,
    tp_mid,
    row_send,
    row_recv,
    local_sem,
    own_sem,
    state_sem,
    state_leave,
    w_sem,
    relay_sem,
    w_leave,
    relay_leave,
    att_sem,
    norm_sem,
    norm_leave,
    cross_sem,
    gather_sem,
    leave_sem,
    hid_sem,
    hid_leave,
    tp_sem,
    tp_leave,
    row_sem,
    row_leave,
):
    side, me, lane = lax.axis_index("grp"), lax.axis_index("sp"), lax.axis_index("tp")
    rows, width = query.shape
    heads = width // HEAD
    share = rows // shares
    model = residual.shape[1]
    part_cols = model // spans
    half = part_cols // 2
    total = spans * rows
    lines = rates.shape[0]
    units = gate_taps.shape[1]
    counts = tile_counts(units // 128, spans)
    least, parts = min(counts[0]), max(counts[0])
    f32, bf16 = jnp.float32, jnp.bfloat16
    mate = lane + 1 - 2 * lax.rem(lane, 2)
    cross = lax.rem(lane + shares // 2, shares)
    odd = lax.rem(lane, 2)
    diag = cross + 1 - 2 * odd
    sends = []

    def remote(src, dst, sems, leave=None, **place):
        return pltpu.make_async_remote_copy(
            src_ref=src,
            dst_ref=dst,
            send_sem=sems.at[0] if leave is None else leave,
            recv_sem=sems.at[1] if leave is None else sems,
            device_id=place,
            device_id_type=pl.DeviceIdType.MESH,
        )

    def send(src, dst, sems, **place):
        copy = remote(src, dst, sems, **place)
        copy.start()
        sends.append(copy)
        return copy

    def span_at(step):
        return lax.rem(me + step, spans)

    def target(d):
        if not PAIRED:
            return span_at(d)
        if d == 1:
            return me + 1 - 2 * lax.rem(me, 2)
        return lax.rem(me + 2, spans) if d == 2 else spans - 1 - me

    def source(d):
        return target(d) if PAIRED else lax.rem(me + spans - d, spans)

    def share_at(step):
        return lax.rem(lane + step, shares)

    def pick(tables, span):
        value = 0
        for j in range(spans):
            mine = jnp.where(odd == 0, tables[0][j], tables[1][j])
            value = value + jnp.where(span == j, mine, 0)
        return value

    def holds(part, span):
        return pick(counts, span) > part

    starts = [[sum(row[:j]) for j in range(spans)] for row in counts]

    def first_col(span):
        return pick(starts, span) * 128

    def cols_of(part, span):
        begin = jnp.minimum(first_col(span) + part * 128, units - 128)
        return pl.ds(pl.multiple_of(begin, 128), 128)

    barrier = pltpu.get_barrier_semaphore()
    peers = [{"grp": 1 - side}]
    peers += [{"sp": span_at(d)} for d in range(1, spans)]
    peers += [{"tp": share_at(d)} for d in range(1, shares)]
    for place in peers:
        pl.semaphore_signal(
            barrier, inc=1, device_id=place, device_id_type=pl.DeviceIdType.MESH
        )
    loads = [
        pltpu.make_async_copy(src, dst, local_sem.at[i])
        for i, (src, dst) in enumerate(
            (
                (rates_hbm, rates),
                (key_hbm, key),
                (value_hbm, value),
                (query_hbm, query),
                (gate_hbm, gate),
                (out_hbm, out_w),
                (residual_hbm, residual),
                (down_hbm, down_w),
                (gains_hbm, gains),
                (norm_gain_hbm, norm_gain),
                (gate_taps_hbm, gate_taps),
                (up_taps_hbm, up_taps),
            )
        )
    ]
    for load in loads:
        load.start()

    weights = (fg_hbm, fu_hbm)

    def lanes(g):
        return slice(g * 128, (g + 1) * 128)

    def own_copy(part, g):
        return pltpu.make_async_copy(
            weights[g].at[:, cols_of(part, me)],
            wide.at[part, pl.ds(pl.multiple_of(me * part_cols, part_cols), part_cols), lanes(g)],
            own_sem.at[part],
        )

    def own_wait(part):
        block = wide.at[part, pl.ds(pl.multiple_of(me * part_cols, part_cols), part_cols)]
        return pltpu.make_async_copy(block, block, own_sem.at[part])

    def half_rows(span):
        begin = span * part_cols + side * half
        return pl.ds(pl.multiple_of(begin, half), half)

    def leave_at(part, d):
        return part if part < least else least + (part - least) * (spans - 1) + d - 1

    def weight_copy(part, d, g):
        to = target(d)
        return remote(
            weights[g].at[pl.ds(pl.multiple_of(side * half, half), half), cols_of(part, to)],
            wide.at[part, half_rows(me), lanes(g)],
            w_sem.at[part, d - 1],
            w_leave.at[leave_at(part, d)],
            sp=to,
        )

    def relay_copy(part, d):
        block = wide.at[part, half_rows(source(d))]
        return remote(block, block, relay_sem.at[part, d - 1], relay_leave.at[part], grp=1 - side)

    def weight_wait(part, d):
        block = wide.at[part, half_rows(source(d))]
        sem = w_sem.at[part, d - 1]
        return remote(block, block, sem, w_leave.at[leave_at(part, d)], sp=target(d))

    def when_extra(part, span, step):
        if part >= least:
            pl.when(holds(part, span))(step)
        else:
            step()

    def start_weights(part, d):
        def step():
            for g in range(2):
                weight_copy(part, d, g).start()

        when_extra(part, target(d), step)

    def relay_weights(part, d):
        def step():
            weight_wait(part, d).wait_recv()
            relay_copy(part, d).start()

        when_extra(part, me, step)

    def own_weights(part):
        def step():
            for g in range(2):
                own_copy(part, g).start()

        when_extra(part, me, step)

    for part in range(parts):
        own_weights(part)

    with jax.named_scope("states"):
        loads[0].wait()
        low = lax.broadcasted_iota(jnp.int32, (rows, rows), 0)
        high = lax.broadcasted_iota(jnp.int32, (rows, rows), 1)
        rate = rates[...]

        def tall(table):
            return lax.dot_general(
                table.astype(f32),
                rate,
                (((1,), (1,)), ((), ())),
                precision=FULL_PRECISION,
                preferred_element_type=f32,
            )

        until = tall(low >= high)
        single = tall(low == high)
        after = tall(low < high)
        flat = jnp.dot(
            rate, (low <= high).astype(f32), precision=FULL_PRECISION, preferred_element_type=f32
        )
        loads[1].wait()
        loads[2].wait()

        def split(x):
            top = x.astype(bf16)
            return top, (x - top.astype(f32)).astype(bf16)

        for head in range(heads):
            cols = slice(head * HEAD, (head + 1) * HEAD)
            held = value[:, cols]
            for way in range(2):
                line = way * heads + head
                if way == 0:
                    weight = after[:, line : line + 1]
                else:
                    weight = until[:, line : line + 1] - single[:, line : line + 1]
                lifted = key[:, cols].astype(f32) * jnp.exp(jnp.minimum(weight, 0.0))
                state = jnp.zeros((HEAD, HEAD), f32)
                for piece in split(lifted):
                    state += lax.dot_general(
                        piece, held, (((0,), (0,)), ((), ())), preferred_element_type=f32
                    )
                state = state - jnp.mean(state, axis=1, keepdims=True)
                state_send[way, head] = state.astype(bf16)

    with jax.named_scope("barrier"):
        pl.semaphore_wait(barrier, len(peers))
    arrivals = []
    for d in range(1, spans):
        to = span_at(d)
        way = jnp.where(to > me, 0, 1)
        arrivals.append(
            remote(rates, rate_all.at[me], state_sem.at[d - 1, 0], state_leave.at[0], sp=to)
        )
        arrivals.append(
            remote(
                state_send.at[way],
                state_recv.at[me],
                state_sem.at[d - 1, 1],
                state_leave.at[1],
                sp=to,
            )
        )
    for copy in arrivals:
        copy.start()

    with jax.named_scope("inner"):
        loads[3].wait()
        inner = []
        for head in range(heads):
            cols = slice(head * HEAD, (head + 1) * HEAD)
            back = heads + head
            scores = lax.dot_general(
                query[:, cols],
                key[:, cols],
                (((1,), (1,)), ((), ())),
                preferred_element_type=f32,
            ) * (HEAD ** (-0.5))
            ahead_gap = until[:, head : head + 1] - flat[head : head + 1]
            behind_gap = (flat[back : back + 1] - rate[back : back + 1]) - (
                until[:, back : back + 1] - single[:, back : back + 1]
            )
            for gap, keep in ((ahead_gap, low >= high), (behind_gap, low <= high)):
                weighted = jnp.where(keep, jnp.exp(jnp.minimum(gap, 0.0)), 0.0) * scores
                out = jnp.zeros((rows, HEAD), f32)
                for piece in split(weighted):
                    out += jnp.dot(piece, value[:, cols], preferred_element_type=f32)
                inner.append(out)

    with jax.named_scope("state_wait"):
        for copy in arrivals:
            copy.wait_recv()
        loads[4].wait()
        for load in loads[8:]:
            load.wait()
        for part, d in EARLY:
            start_weights(part, d)
    with jax.named_scope("outer"):
        sums = [jnp.sum(rate_all[j], axis=1, keepdims=True) for j in range(spans)]
        mixed = []
        gaps = []
        for j in range(spans):
            ahead_far = jnp.zeros((lines, 1), f32)
            behind_far = jnp.zeros((lines, 1), f32)
            for i in range(spans):
                if i > j:
                    ahead_far += jnp.where(i < me, sums[i], 0.0)
                if i < j:
                    behind_far += jnp.where(i > me, sums[i], 0.0)
            gaps.append((ahead_far, behind_far))
        for head in range(heads):
            cols = slice(head * HEAD, (head + 1) * HEAD)
            back = heads + head
            ahead, behind = inner[2 * head], inner[2 * head + 1]
            for j in range(spans):
                product = jnp.dot(
                    query[:, cols], state_recv[j, head], preferred_element_type=f32
                ) * (HEAD ** (-0.5))
                near = until[:, head : head + 1] + gaps[j][0][head : head + 1]
                far = (
                    after[:, back : back + 1]
                    + single[:, back : back + 1]
                    + gaps[j][1][back : back + 1]
                )
                ahead += jnp.where(j < me, jnp.exp(jnp.minimum(near, 0.0)) * product, 0.0)
                behind += jnp.where(j > me, jnp.exp(jnp.minimum(far, 0.0)) * product, 0.0)
            sides = []
            for row, out in enumerate((ahead, behind)):
                centre = out - jnp.mean(out, axis=1, keepdims=True)
                spread = jnp.mean(centre * centre, axis=1, keepdims=True)
                sides.append(centre * lax.rsqrt(spread + GROUP_EPS) * gains[row : row + 1, cols])
            level = gate[:, cols].astype(f32)
            mixed.append(((level / (1.0 + jnp.exp(-level))) * (sides[0] + sides[1])).astype(bf16))
        mixed = jnp.concatenate(mixed, axis=1)

    def share_rows(index):
        return pl.ds(pl.multiple_of(index * share, share), share)

    with jax.named_scope("attend"):
        loads[5].wait()
        step_cols = math.gcd(model, 512)
        for at in range(0, model, step_cols):
            att_send[:, at : at + step_cols] = jnp.dot(
                mixed, out_w[:, at : at + step_cols], preferred_element_type=f32
            ).astype(bf16)
        pairs = [
            send(att_send.at[share_rows(to)], att_recv.at[i], att_sem.at[i], tp=mate)
            for i, to in enumerate((diag, mate))
        ]
    for part, d in SECOND:
        start_weights(part, d)
    with jax.named_scope("attended_pair"):
        loads[6].wait()
        pairs[0].wait_recv()
        att_mid[...] = (
            att_send[share_rows(cross), :].astype(f32) + att_recv[0].astype(f32)
        ).astype(bf16)
        pairs.append(send(att_mid, att_recv.at[2], att_sem.at[2], tp=cross))
        pairs[1].wait_recv()
    with jax.named_scope("attended_wait"):
        pairs[2].wait_recv()

    def token_rows(span, tp):
        return pl.ds(pl.multiple_of(span * rows + tp * share, share), share)

    with jax.named_scope("normed"):
        attended = att_send[share_rows(lane), :].astype(f32)
        for i in range(1, 3):
            attended = attended + att_recv[i].astype(f32)
        middle = (residual[share_rows(lane), :].astype(f32) + attended).astype(bf16)
        middle_ref[...] = middle
        middle = middle.astype(f32)
        factor = lax.rsqrt(jnp.mean(middle * middle, axis=1, keepdims=True) + NORM_EPS)
        for at in range(0, model, 128):
            gain = norm_gain[at // 128 : at // 128 + 1, :].astype(f32)
            norm_all[token_rows(me, lane), at : at + 128] = (
                middle[:, at : at + 128] * factor * gain
            ).astype(bf16)

    steps = (1, -1)

    def origin(way, hop):
        return me - steps[way] * hop

    def inside(span):
        return (span >= 0) & (span < spans)

    def clamp(span):
        return jnp.clip(span, 0, spans - 1)

    def passes(way, hop):
        return inside(origin(way, hop)) & inside(me + steps[way])

    slab = model // SLABS

    def slab_of(span, tp, c):
        return norm_all.at[token_rows(span, tp), c * slab : (c + 1) * slab]

    def norm_copy(way, hop, c):
        block = slab_of(clamp(origin(way, hop)), lane, c)
        to = clamp(me + steps[way])
        return remote(block, block, norm_sem.at[way, hop, c], norm_leave.at[way, hop], sp=to)

    def mate_copy(span, c):
        block = slab_of(span, lane, c)
        return remote(block, block, gather_sem.at[0], leave_sem.at[0], tp=mate)

    def cross_copy(span, c):
        block = slab_of(span, lane, c)
        return remote(block, block, cross_sem.at[span, c], leave_sem.at[1], tp=cross)

    def diag_copy(span, c):
        block = slab_of(span, cross, c)
        return remote(block, block, gather_sem.at[1], leave_sem.at[2], tp=mate)

    def spread_block(way, hop, c):
        if hop + 1 >= spans:
            return

        @pl.when(passes(way, hop))
        def _():
            norm_copy(way, hop, c).start()

    def norm_hop(hop):
        for c in range(SLABS):
            for way in WAYS:

                @pl.when(inside(origin(way, hop)))
                def _():
                    norm_copy(way, hop - 1, c).wait_recv()
                    spread_block(way, hop, c)
                    cross_copy(clamp(origin(way, hop)), c).start()
                    mate_copy(clamp(origin(way, hop)), c).start()

    def cross_hop(hop):
        for way in range(2 if hop else 1):

            @pl.when(inside(origin(way, hop)))
            def _():
                for c in range(SLABS):
                    cross_copy(clamp(origin(way, hop)), c).wait_recv()
                    diag_copy(clamp(origin(way, hop)), c).start()

    with jax.named_scope("norm0"):
        for c in range(SLABS):
            for way in WAYS:
                spread_block(way, 0, c)
            cross_copy(me, c).start()
            mate_copy(me, c).start()
    def gather_wait():
        whole = norm_all.at[pl.ds(0, rows)]
        for i in range(2):
            remote(whole, whole, gather_sem.at[i], leave_sem.at[0], tp=mate).wait_recv()

    row_at = lax.broadcasted_iota(jnp.int32, (total, 1), 0)

    def twin_wait(part):
        def step():
            own_wait(part).wait()
            for d in range(1, spans):
                relay_copy(part, d).wait_recv()

        when_extra(part, me, step)

    def compute_hidden(part):
        cols = cols_of(part, me)
        both = jnp.dot(norm_all[...], wide[part], preferred_element_type=f32)
        here = both.astype(bf16).astype(f32)
        earlier, later = pltpu.roll(here, 1, 0), pltpu.roll(here, total - 1, 0)
        earlier = jnp.where(row_at == 0, 0.0, earlier)
        later = jnp.where(row_at == total - 1, 0.0, later)
        weight = jnp.concatenate(
            [gate_taps[:, cols].astype(f32), up_taps[:, cols].astype(f32)], axis=1
        )
        conv = weight[0:1] * earlier + weight[1:2] * here + weight[2:3] * later
        level = conv[:, :128]
        hid_all[:, cols] = ((level / (1.0 + jnp.exp(-level))) * conv[:, 128:]).astype(bf16)

    groups = max(spans // 2, 1)
    depth = spans // groups

    def blocks(part):
        return groups

    def hidden_copy(part, way, hop, b):
        size = total // blocks(part)
        block = hid_all.at[pl.ds(b * size, size), cols_of(part, clamp(origin(way, hop)))]
        return remote(
            block,
            block,
            hid_sem.at[part, way, hop, b],
            hid_leave.at[part, way, hop],
            sp=clamp(me + steps[way]),
        )

    def has(part, span):
        return inside(span) & holds(part, clamp(span)) if part >= least else inside(span)

    def hidden_start(part, way, hop, b):
        if hop + 1 >= spans:
            return

        @pl.when(passes(way, hop) & has(part, origin(way, hop)))
        def _():
            hidden_copy(part, way, hop, b).start()

    def hidden_pass(part, hop, b):
        for way in WAYS:

            @pl.when(has(part, origin(way, hop)))
            def _():
                hidden_copy(part, way, hop - 1, b).wait_recv()

            hidden_start(part, way, hop, b)

    def make_hidden(part):
        twin_wait(part)
        if part >= least:

            @pl.when(holds(part, me))
            def _():
                compute_hidden(part)

        else:
            compute_hidden(part)
        for b in range(blocks(part)):
            for way in WAYS:
                hidden_start(part, way, 0, b)

    pairs, crossing = {}, {}

    def down(b):
        few = pl.ds(b * depth, depth)
        if b == 0:
            loads[7].wait()
        tp_send[few] = (
            lax.dot_general(
                hid_all[b * depth * rows : (b + 1) * depth * rows, :],
                down_w[...],
                (((1,), (1,)), ((), ())),
                preferred_element_type=f32,
            )
            .astype(bf16)
            .reshape(depth, rows, part_cols)
        )
        pairs[b] = [
            remote(
                tp_send.at[few, share_rows(to)],
                tp_recv.at[i, few],
                tp_sem.at[b, i],
                tp_leave.at[0],
                tp=mate,
            )
            for i, to in enumerate((diag, mate))
        ]
        for copy in pairs[b]:
            copy.start()

    def cross_step(b):
        few = pl.ds(b * depth, depth)
        pairs[b][0].wait_recv()
        tp_mid[few] = (
            tp_send[few, share_rows(cross)].astype(f32) + tp_recv[0, few].astype(f32)
        ).astype(bf16)
        crossing[b] = remote(
            tp_mid.at[few], tp_recv.at[2, few], tp_sem.at[b, 2], tp_leave.at[0], tp=cross
        )
        crossing[b].start()
        pairs[b][1].wait_recv()

    def row_out(b):
        d = lax.rem(b - me + spans, spans)
        return remote(
            row_send.at[b],
            row_recv.at[me],
            row_sem.at[jnp.maximum(d - 1, 0)],
            row_leave.at[0],
            sp=b,
        )

    def row_step(group):
        crossing[group].wait_recv()
        for b in range(group * depth, (group + 1) * depth):
            summed = tp_send[b, share_rows(lane), :].astype(f32)
            for i in range(1, 3):
                summed = summed + tp_recv[i, b].astype(f32)
            row_send[b] = summed.astype(bf16)

            @pl.when(b != me)
            def _():
                row_out(b).start()

            @pl.when(b == me)
            def _():
                row_recv[me] = row_send[b]

    inner_span = (me > 0) & (me < spans - 1)

    def on_ends(part, d):
        pl.when(jnp.logical_not(inner_span))(lambda: relay_weights(part, d))

    def on_inner(part, d):
        pl.when(inner_span)(lambda: relay_weights(part, d))

    actions = {
        "e": on_ends,
        "i": on_inner,
        "n": norm_hop,
        "x": cross_hop,
        "w": start_weights,
        "r": relay_weights,
        "m": gather_wait,
        "H": make_hidden,
        "h": hidden_pass,
        "D": down,
        "P": cross_step,
        "R": row_step,
    }
    for name, *numbers in ORDER:
        with jax.named_scope(name + "".join(str(number) for number in numbers)):
            actions[name](*numbers)

    with jax.named_scope("final"):
        for d in range(1, spans):
            row_out(span_at(d)).wait_recv()
        for j in range(spans):
            cols = slice(j * part_cols, (j + 1) * part_cols)
            result[:, cols] = (
                middle_ref[:, cols].astype(f32) + row_recv[j].astype(f32)
            ).astype(bf16)
    with jax.named_scope("drain"):
        for copy in sends:
            copy.wait_send()
        for part in range(parts):
            if part < least:
                block = wide.at[part, pl.ds(0, (spans - 1) * half)]
                remote(
                    block, block, w_sem.at[part, 0], w_leave.at[part], sp=span_at(1)
                ).wait_send()
            for d in range(1, spans if part >= least else 1):

                def sent():
                    weight_wait(part, d).wait_send()

                when_extra(part, target(d), sent)

            def relayed():
                block = wide.at[part, pl.ds(0, (spans - 1) * half)]
                remote(
                    block, block, relay_sem.at[part, 0], relay_leave.at[part], grp=1 - side
                ).wait_send()

            when_extra(part, me, relayed)
        whole = norm_all.at[pl.ds(0, rows)]
        for i in range(3):
            remote(whole, whole, gather_sem.at[0], leave_sem.at[i], tp=mate).wait_send()
        remote(state_recv.at[pl.ds(0, spans - 1)], state_recv.at[pl.ds(0, spans - 1)],
               state_sem.at[0, 1], state_leave.at[1], sp=span_at(1)).wait_send()
        remote(rate_all.at[pl.ds(0, spans - 1)], rate_all.at[pl.ds(0, spans - 1)],
               state_sem.at[0, 0], state_leave.at[0], sp=span_at(1)).wait_send()
        remote(tp_recv, tp_recv, tp_sem.at[0, 0], tp_leave.at[0], tp=mate).wait_send()
        remote(row_recv.at[pl.ds(0, spans - 1)], row_recv.at[pl.ds(0, spans - 1)],
               row_sem.at[0], row_leave.at[0], sp=span_at(1)).wait_send()
        for way in range(2):
            for hop in range(spans - 1):

                @pl.when(passes(way, hop))
                def _():
                    block = norm_all.at[pl.ds(0, share)]
                    remote(
                        block,
                        block,
                        norm_sem.at[way, hop, 0],
                        norm_leave.at[way, hop],
                        sp=clamp(me + steps[way]),
                    ).wait_send()

                for part in range(parts):

                    @pl.when(passes(way, hop) & has(part, origin(way, hop)))
                    def _():
                        block = hid_all.at[:, pl.ds(0, 128)]
                        remote(
                            block,
                            block,
                            hid_sem.at[part, way, hop, 0],
                            hid_leave.at[part, way, hop],
                            sp=clamp(me + steps[way]),
                        ).wait_send()


def fused_block(
    query_rows,
    key_rows,
    value_rows,
    gate_rows,
    log_decay,
    head_gain,
    out_weight,
    residual,
    norm_gain,
    gate_weight,
    up_weight,
    down_weight,
    gate_taps,
    up_taps,
):
    spans, shares = (lax.axis_size("sp"), lax.axis_size("tp"))
    rows, width = query_rows.shape
    model = residual.shape[1]
    units = gate_weight.shape[1]
    part_cols, share = (model // spans, rows // shares)
    total = spans * rows
    counts = tile_counts(units // 128, spans)
    least, parts = min(counts[0]), max(counts[0])
    lines = log_decay.shape[0] * log_decay.shape[1]
    heads = width // HEAD
    rates = log_decay.reshape(lines, rows)
    f32, bf16 = jnp.float32, jnp.bfloat16
    far = pl.BlockSpec(memory_space=pltpu.HBM)
    dma = pltpu.SemaphoreType.DMA
    vmem = pltpu.VMEM
    return pl.pallas_call(
        functools.partial(block_kernel, spans, shares),
        out_shape=jax.ShapeDtypeStruct((share, model), bf16),
        in_specs=[far] * 14,
        out_specs=pl.BlockSpec(memory_space=pltpu.VMEM),
        scratch_shapes=[
            vmem((rows, width), bf16),
            vmem((rows, width), bf16),
            vmem((rows, width), bf16),
            vmem((rows, width), bf16),
            vmem((lines, rows), f32),
            vmem((rows, model), bf16),
            vmem(out_weight.shape, bf16),
            vmem(down_weight.shape, bf16),
            vmem(head_gain.shape, f32),
            vmem((model // 128, 128), bf16),
            vmem(gate_taps.shape, bf16),
            vmem(up_taps.shape, bf16),
            vmem((spans, lines, rows), f32),
            vmem((2, heads, HEAD, HEAD), bf16),
            vmem((spans, heads, HEAD, HEAD), bf16),
            vmem((parts, model, 256), bf16),
            vmem((rows, model), bf16),
            vmem((3, share, model), bf16),
            vmem((share, model), bf16),
            vmem((share, model), bf16),
            vmem((total, model), bf16),
            vmem((total, units), bf16),
            vmem((spans, rows, part_cols), bf16),
            vmem((3, spans, share, part_cols), bf16),
            vmem((spans, share, part_cols), bf16),
            vmem((spans, share, part_cols), bf16),
            vmem((spans, share, part_cols), bf16),
            dma((12,)),
            dma((parts,)),
            dma((spans - 1, 2)),
            dma((2,)),
            dma((parts, spans - 1)),
            dma((parts, spans - 1)),
            dma((least + (parts - least) * (spans - 1),)),
            dma((parts,)),
            dma((3, 2)),
            dma((2, spans - 1, SLABS)),
            dma((2, spans - 1)),
            dma((spans, SLABS)),
            dma((2,)),
            dma((3,)),
            dma((parts, 2, spans - 1, spans // 2)),
            dma((parts, 2, spans - 1)),
            dma((spans // 2, 3)),
            dma((1,)),
            dma((spans - 1,)),
            dma((1,)),
        ],
        compiler_params=pltpu.CompilerParams(
            collective_id=0, has_side_effects=True, vmem_limit_bytes=GRANT
        ),
    )(
        *(
            pltpu.with_memory_space_constraint(value, pltpu.HBM)
            for value in (
                query_rows,
                key_rows,
                value_rows,
                gate_rows,
                rates,
                head_gain,
                residual,
                norm_gain.reshape(model // 128, 128),
                gate_taps,
                up_taps,
                out_weight,
                gate_weight,
                up_weight,
                down_weight,
            )
        )
    )


def either(*args):
    spans, shares, twins = (lax.axis_size(name) for name in ("sp", "tp", "grp"))
    span_tokens = args[0].shape[0] * spans
    model_width = args[7].shape[1]
    lanes = args[9].shape[1] // 128
    fits = spans == 4 and lanes >= 2 * spans
    if fits and span_tokens < model_width and twins == 2 and shares == 4:
        return fused_block(*args)
    return shards(*args)


def solution(mesh):
    in_specs = (
        P(("grp", "sp"), "tp"),
        P(("grp", "sp"), "tp"),
        P(("grp", "sp"), "tp"),
        P(("grp", "sp"), "tp"),
        P(None, "tp", ("grp", "sp")),
        P(None, "tp"),
        P("tp", None),
        P(("grp", "sp"), None),
        P(),
        P("sp", "tp"),
        P("sp", "tp"),
        P("sp", "tp"),
        P(None, "tp"),
        P(None, "tp"),
    )
    out_specs = P(("grp", "sp", "tp"), None)
    return jax.shard_map(either, mesh=mesh, in_specs=in_specs, out_specs=out_specs, check_vma=False)
```

```python
import functools
import math

import jax
import jax.numpy as jnp
from jax import lax
from jax.experimental import pallas as pl
from jax.experimental.pallas import tpu as pltpu
from jax.sharding import PartitionSpec as P

HEAD = 128
GRANT = 40 << 20
SLABS = 4
PAIRED = False
SPLIT = 'even'
WAYS = (0, 1)
EARLY = ((0, 3), (0, 1), (0, 2))
SECOND = ()
ORDER = (('r', 0, 1), ('n', 1), ('x', 0), ('r', 0, 2), ('n', 2), ('w', 1, 1), ('x', 1), ('r', 0, 3), ('w', 1, 2), ('w', 1, 3), ('n', 3), ('x', 2), ('r', 1, 1), ('x', 3), ('m',), ('H', 0), ('w', 2, 1), ('r', 1, 3), ('w', 2, 2), ('r', 1, 2), ('w', 2, 3), ('h', 0, 1, 0), ('h', 0, 1, 1), ('H', 1), ('r', 2, 1), ('r', 2, 2), ('r', 2, 3), ('h', 0, 2, 0), ('h', 0, 2, 1), ('h', 1, 1, 0), ('h', 1, 1, 1), ('H', 2), ('h', 0, 3, 0), ('h', 0, 3, 1), ('h', 1, 2, 0), ('h', 1, 3, 0), ('h', 2, 1, 0), ('h', 2, 2, 0), ('h', 2, 3, 0), ('D', 0), ('h', 1, 2, 1), ('h', 1, 3, 1), ('h', 2, 1, 1), ('P', 0), ('h', 2, 2, 1), ('h', 2, 3, 1), ('D', 1), ('P', 1), ('R', 0), ('R', 1))
EDGE = 16


FULL_PRECISION = lax.Precision.HIGHEST
GROUP_EPS = 1e-05
NORM_EPS = 1e-06


def prefix(value, axis, join, neutral, backward):
    count, mine = (lax.axis_size(axis), lax.axis_index(axis))
    pieces = jax.tree.map(lambda part: lax.all_gather(part, axis), value)
    if backward:
        pieces = jax.tree.map(lambda part: part[::-1], pieces)
        mine = count - 1 - mine
    running = jax.tree.map(
        lambda part, zero: jnp.full_like(part, 0) + jnp.asarray(zero, part.dtype), value, neutral
    )

    def lap(position, running):
        longer = join(running, jax.tree.map(lambda part: part[position], pieces))
        return jax.tree.map(lambda new, old: jnp.where(position < mine, new, old), longer, running)

    return lax.fori_loop(0, count - 1, lap, running)


def padded_2(shard, sides, width):
    for axis, dim in sides:
        size, length = (lax.axis_size(axis), shard.shape[dim])
        up = [(i, (i + 1) % size) for i in range(size - 1)]
        down = [(j, i) for i, j in up]
        last = lax.slice_in_dim(shard, length - width, length, axis=dim)
        initial = lax.slice_in_dim(shard, 0, width, axis=dim)
        before = lax.ppermute(last, axis, up)
        after = lax.ppermute(initial, axis, down)
        shard = jnp.concatenate([before, shard, after], axis=dim)
    return shard


def state_combine(earlier, later):
    return (earlier[0] * later[0], earlier[1] * later[0][:, None, None] + later[1])


def group_norm(values):
    length, head_count, head_width = values.shape
    centre = values - jnp.mean(values, axis=2, keepdims=True)
    spread = jnp.mean(centre * centre, axis=2, keepdims=True)
    return (centre * lax.rsqrt(spread + GROUP_EPS)).reshape(length, head_count * head_width)


def rms_scale(middle, gain):
    values = middle.astype(jnp.float32)
    multiplier = lax.rsqrt(jnp.mean(values * values, axis=1, keepdims=True) + NORM_EPS)
    return (values * multiplier * gain.astype(jnp.float32)).astype(jnp.bfloat16)


def local_retention(query_all, key_all, value_all, log_rates):
    length, head_count, head_width = query_all.shape
    block_len = math.gcd(length, 512)
    block_count = length // block_len
    cumul = jnp.cumsum(log_rates, axis=1).T
    query_block = query_all.reshape(block_count, block_len, head_count, head_width)
    key_block = key_all.reshape(block_count, block_len, head_count, head_width)
    value_block = value_all.reshape(block_count, block_len, head_count, head_width)
    cumul_block = cumul.reshape(block_count, block_len, head_count)
    before = jnp.concatenate(
        [jnp.zeros((1, head_count), jnp.float32), cumul_block[:-1, -1]], axis=0
    )
    local_cumul = cumul_block - before[:, None, :]
    gap_logs = local_cumul[:, :, None, :] - local_cumul[:, None, :, :]
    lower_mask = (jnp.arange(block_len)[:, None] >= jnp.arange(block_len)[None, :])[
        None, :, :, None
    ]
    decay_mask = jnp.where(lower_mask, jnp.exp(jnp.minimum(gap_logs, 0.0)), 0.0)
    scores = (
        jnp.einsum("bthd,bshd->btsh", query_block, key_block, precision=FULL_PRECISION) * decay_mask
    )
    inner_part = jnp.einsum("btsh,bshe->bthe", scores, value_block, precision=FULL_PRECISION)
    to_end = jnp.exp(local_cumul[:, -1:, :] - local_cumul)
    block_states = jnp.einsum(
        "bshd,bshe->bhde", key_block * to_end[..., None], value_block, precision=FULL_PRECISION
    )
    block_decay = jnp.exp(local_cumul[:, -1, :])

    def carry_step(carry_state, inputs):
        return (carry_state * inputs[0][:, None, None] + inputs[1], carry_state)

    zero_state = jnp.zeros((head_count, head_width, head_width), jnp.float32)
    end_state, entering = lax.scan(carry_step, zero_state, (block_decay, block_states))
    carried = jnp.einsum(
        "bthd,bhde->bthe",
        query_block * jnp.exp(local_cumul)[..., None],
        entering,
        precision=FULL_PRECISION,
    )
    output = (inner_part + carried).reshape(length, head_count, head_width)
    return (output, end_state, cumul, jnp.exp(cumul[-1]))


def with_incoming(output, query_all, cumul, incoming):
    return output + jnp.einsum(
        "thd,hde->the", query_all * jnp.exp(cumul)[:, :, None], incoming, precision=FULL_PRECISION
    )


def shards(
    query_rows,
    key_rows,
    value_rows,
    gate_rows,
    log_decay,
    head_gain,
    out_weight,
    residual,
    norm_gain,
    gate_weight,
    up_weight,
    down_weight,
    gate_taps,
    up_taps,
):
    pair_local = jnp.concatenate([gate_weight, up_weight], axis=1)
    row_count = query_rows.shape[0]
    head_count = query_rows.shape[1] // HEAD
    key_scale = HEAD ** (-0.5)
    query_all = query_rows.astype(jnp.float32).reshape(row_count, head_count, HEAD)
    key_all = key_rows.astype(jnp.float32).reshape(row_count, head_count, HEAD) * key_scale
    value_all = value_rows.astype(jnp.float32).reshape(row_count, head_count, HEAD)
    identity = (
        jnp.ones((head_count,), jnp.float32),
        jnp.zeros((head_count, HEAD, HEAD), jnp.float32),
    )
    ahead_local, ahead_state, ahead_cumul, ahead_decay = local_retention(
        query_all, key_all, value_all, log_decay[0]
    )
    query_back = query_all[::-1]
    behind_local, behind_state, behind_cumul, behind_decay = local_retention(
        query_back, key_all[::-1], value_all[::-1], log_decay[1][:, ::-1]
    )
    ahead_in = prefix((ahead_decay, ahead_state), "sp", state_combine, identity, False)[1]
    behind_in = prefix((behind_decay, behind_state), "sp", state_combine, identity, True)[1]
    ahead_out = with_incoming(ahead_local, query_all, ahead_cumul, ahead_in)
    behind_out = with_incoming(behind_local, query_back, behind_cumul, behind_in)[::-1]
    combined = group_norm(ahead_out) * head_gain[0] + group_norm(behind_out) * head_gain[1]
    mixed_heads = (jax.nn.silu(gate_rows.astype(jnp.float32)) * combined).astype(jnp.bfloat16)
    gathered = (
        lax.all_gather(pair_local, "sp", axis=0, tiled=True),
        lax.all_gather(down_weight, "sp", axis=0, tiled=True),
    )
    pair_full, down_full = gathered
    share_rows = row_count // lax.axis_size("tp")
    own_start = lax.axis_index("tp") * share_rows
    picked = mixed_heads
    attended = lax.psum_scatter(
        jnp.dot(picked, out_weight, preferred_element_type=jnp.float32).astype(jnp.bfloat16),
        "tp",
        scatter_dimension=0,
        tiled=True,
    ).astype(jnp.float32)
    residual_own = lax.dynamic_slice_in_dim(residual, own_start, share_rows, 0)
    middle_own = lax.optimization_barrier(
        (residual_own.astype(jnp.float32) + attended).astype(jnp.bfloat16)
    )
    normed = rms_scale(middle_own, norm_gain)
    pre_both = jnp.dot(
        lax.all_gather(normed, "tp", axis=0, tiled=True),
        pair_full,
        preferred_element_type=jnp.float32,
    ).astype(jnp.bfloat16)
    padded = padded_2(pre_both, (("sp", 0),), 1)
    half_width = gate_taps.shape[1]
    tap_table = jnp.concatenate([gate_taps, up_taps], axis=1).astype(jnp.float32)
    conv_out = (
        tap_table[0] * padded[:-2].astype(jnp.float32)
        + tap_table[1] * padded[1:-1].astype(jnp.float32)
        + tap_table[2] * padded[2:].astype(jnp.float32)
    )
    hidden = (jax.nn.silu(conv_out[:, :half_width]) * conv_out[:, half_width:]).astype(jnp.bfloat16)
    picked = hidden
    ff_out = lax.psum_scatter(
        lax.dot_general(
            picked, down_full, (((1,), (1,)), ((), ())), preferred_element_type=jnp.float32
        ).astype(jnp.bfloat16),
        "tp",
        scatter_dimension=0,
        tiled=True,
    ).astype(jnp.float32)
    return (middle_own.astype(jnp.float32) + ff_out).astype(jnp.bfloat16)


def tile_counts(lanes, spans):
    if SPLIT == "ends":
        outer = lanes // spans
        near = (lanes - 2 * outer + 1) // 2
        far = lanes - 2 * outer - near
        even, odd = (outer, near, far, outer), (outer, far, near, outer)
    else:
        least, rest = divmod(lanes, spans)
        even = tuple(least + (j < rest) for j in range(spans))
        odd = even[::-1]
        if SPLIT == "middle":
            even, odd = (even[0], even[1], even[3], even[2]), (odd[1], odd[0], odd[2], odd[3])
    return even, odd


def block_kernel(
    spans,
    shares,
    query_hbm,
    key_hbm,
    value_hbm,
    gate_hbm,
    rates_hbm,
    gains_hbm,
    residual_hbm,
    norm_gain_hbm,
    gate_taps_hbm,
    up_taps_hbm,
    out_hbm,
    fg_hbm,
    fu_hbm,
    down_hbm,
    result,
    query,
    key,
    value,
    gate,
    rates,
    residual,
    out_w,
    down_w,
    gains,
    norm_gain,
    gate_taps,
    up_taps,
    rate_all,
    state_send,
    state_recv,
    wide,
    att_send,
    att_recv,
    att_mid,
    middle_ref,
    norm_all,
    hid_all,
    tp_send,
    tp_recv,
    tp_mid,
    row_send,
    row_recv,
    local_sem,
    own_sem,
    state_sem,
    state_leave,
    w_sem,
    relay_sem,
    w_leave,
    relay_leave,
    att_sem,
    norm_sem,
    norm_leave,
    cross_sem,
    gather_sem,
    leave_sem,
    hid_sem,
    hid_leave,
    tp_sem,
    tp_leave,
    row_sem,
    row_leave,
):
    side, me, lane = lax.axis_index("grp"), lax.axis_index("sp"), lax.axis_index("tp")
    rows, width = query.shape
    heads = width // HEAD
    share = rows // shares
    model = residual.shape[1]
    part_cols = model // spans
    half = part_cols // 2
    total = spans * rows
    lines = rates.shape[0]
    units = gate_taps.shape[1]
    counts = tile_counts(units // 128, spans)
    least, parts = min(counts[0]), max(counts[0])
    f32, bf16 = jnp.float32, jnp.bfloat16
    mate = lane + 1 - 2 * lax.rem(lane, 2)
    cross = lax.rem(lane + shares // 2, shares)
    odd = lax.rem(lane, 2)
    diag = cross + 1 - 2 * odd
    sends = []

    def remote(src, dst, sems, leave=None, **place):
        return pltpu.make_async_remote_copy(
            src_ref=src,
            dst_ref=dst,
            send_sem=sems.at[0] if leave is None else leave,
            recv_sem=sems.at[1] if leave is None else sems,
            device_id=place,
            device_id_type=pl.DeviceIdType.MESH,
        )

    def send(src, dst, sems, **place):
        copy = remote(src, dst, sems, **place)
        copy.start()
        sends.append(copy)
        return copy

    def span_at(step):
        return lax.rem(me + step, spans)

    def target(d):
        if not PAIRED:
            return span_at(d)
        if d == 1:
            return me + 1 - 2 * lax.rem(me, 2)
        return lax.rem(me + 2, spans) if d == 2 else spans - 1 - me

    def source(d):
        return target(d) if PAIRED else lax.rem(me + spans - d, spans)

    def share_at(step):
        return lax.rem(lane + step, shares)

    def pick(tables, span):
        value = 0
        for j in range(spans):
            mine = jnp.where(odd == 0, tables[0][j], tables[1][j])
            value = value + jnp.where(span == j, mine, 0)
        return value

    def holds(part, span):
        return pick(counts, span) > part

    starts = [[sum(row[:j]) for j in range(spans)] for row in counts]

    def first_col(span):
        return pick(starts, span) * 128

    def cols_of(part, span):
        begin = jnp.minimum(first_col(span) + part * 128, units - 128)
        return pl.ds(pl.multiple_of(begin, 128), 128)

    barrier = pltpu.get_barrier_semaphore()
    peers = [{"grp": 1 - side}]
    peers += [{"sp": span_at(d)} for d in range(1, spans)]
    peers += [{"tp": share_at(d)} for d in range(1, shares)]
    for place in peers:
        pl.semaphore_signal(
            barrier, inc=1, device_id=place, device_id_type=pl.DeviceIdType.MESH
        )
    loads = [
        pltpu.make_async_copy(src, dst, local_sem.at[i])
        for i, (src, dst) in enumerate(
            (
                (rates_hbm, rates),
                (key_hbm, key),
                (value_hbm, value),
                (query_hbm, query),
                (gate_hbm, gate),
                (out_hbm, out_w),
                (residual_hbm, residual),
                (down_hbm, down_w),
                (gains_hbm, gains),
                (norm_gain_hbm, norm_gain),
                (gate_taps_hbm, gate_taps),
                (up_taps_hbm, up_taps),
            )
        )
    ]
    for load in loads:
        load.start()

    weights = (fg_hbm, fu_hbm)

    def lanes(g):
        return slice(g * 128, (g + 1) * 128)

    def own_copy(part, g):
        return pltpu.make_async_copy(
            weights[g].at[:, cols_of(part, me)],
            wide.at[part, pl.ds(pl.multiple_of(me * part_cols, part_cols), part_cols), lanes(g)],
            own_sem.at[part],
        )

    def own_wait(part):
        block = wide.at[part, pl.ds(pl.multiple_of(me * part_cols, part_cols), part_cols)]
        return pltpu.make_async_copy(block, block, own_sem.at[part])

    def half_rows(span):
        begin = span * part_cols + side * half
        return pl.ds(pl.multiple_of(begin, half), half)

    def leave_at(part, d):
        return part if part < least else least + (part - least) * (spans - 1) + d - 1

    def weight_copy(part, d, g):
        to = target(d)
        return remote(
            weights[g].at[pl.ds(pl.multiple_of(side * half, half), half), cols_of(part, to)],
            wide.at[part, half_rows(me), lanes(g)],
            w_sem.at[part, d - 1],
            w_leave.at[leave_at(part, d)],
            sp=to,
        )

    def relay_copy(part, d):
        block = wide.at[part, half_rows(source(d))]
        return remote(block, block, relay_sem.at[part, d - 1], relay_leave.at[part], grp=1 - side)

    def weight_wait(part, d):
        block = wide.at[part, half_rows(source(d))]
        sem = w_sem.at[part, d - 1]
        return remote(block, block, sem, w_leave.at[leave_at(part, d)], sp=target(d))

    def when_extra(part, span, step):
        if part >= least:
            pl.when(holds(part, span))(step)
        else:
            step()

    def start_weights(part, d):
        def step():
            for g in range(2):
                weight_copy(part, d, g).start()

        when_extra(part, target(d), step)

    def relay_weights(part, d):
        def step():
            weight_wait(part, d).wait_recv()
            relay_copy(part, d).start()

        when_extra(part, me, step)

    def own_weights(part):
        def step():
            for g in range(2):
                own_copy(part, g).start()

        when_extra(part, me, step)

    for part in range(parts):
        own_weights(part)

    with jax.named_scope("states"):
        loads[0].wait()
        low = lax.broadcasted_iota(jnp.int32, (rows, rows), 0)
        high = lax.broadcasted_iota(jnp.int32, (rows, rows), 1)
        rate = rates[...]

        def tall(table):
            return lax.dot_general(
                table.astype(f32),
                rate,
                (((1,), (1,)), ((), ())),
                precision=FULL_PRECISION,
                preferred_element_type=f32,
            )

        until = tall(low >= high)
        single = tall(low == high)
        after = tall(low < high)
        flat = jnp.dot(
            rate, (low <= high).astype(f32), precision=FULL_PRECISION, preferred_element_type=f32
        )
        loads[1].wait()
        loads[2].wait()

        def split(x):
            top = x.astype(bf16)
            return top, (x - top.astype(f32)).astype(bf16)

        for head in range(heads):
            cols = slice(head * HEAD, (head + 1) * HEAD)
            held = value[:, cols]
            for way in range(2):
                line = way * heads + head
                if way == 0:
                    weight = after[:, line : line + 1]
                else:
                    weight = until[:, line : line + 1] - single[:, line : line + 1]
                lifted = key[:, cols].astype(f32) * jnp.exp(jnp.minimum(weight, 0.0))
                state = jnp.zeros((HEAD, HEAD), f32)
                for piece in split(lifted):
                    state += lax.dot_general(
                        piece, held, (((0,), (0,)), ((), ())), preferred_element_type=f32
                    )
                state = state - jnp.mean(state, axis=1, keepdims=True)
                state_send[way, head] = state.astype(bf16)

    with jax.named_scope("barrier"):
        pl.semaphore_wait(barrier, len(peers))
    arrivals = []
    for d in range(1, spans):
        to = span_at(d)
        way = jnp.where(to > me, 0, 1)
        arrivals.append(
            remote(rates, rate_all.at[me], state_sem.at[d - 1, 0], state_leave.at[0], sp=to)
        )
        arrivals.append(
            remote(
                state_send.at[way],
                state_recv.at[me],
                state_sem.at[d - 1, 1],
                state_leave.at[1],
                sp=to,
            )
        )
    for copy in arrivals:
        copy.start()

    with jax.named_scope("inner"):
        loads[3].wait()
        inner = []
        for head in range(heads):
            cols = slice(head * HEAD, (head + 1) * HEAD)
            back = heads + head
            scores = lax.dot_general(
                query[:, cols],
                key[:, cols],
                (((1,), (1,)), ((), ())),
                preferred_element_type=f32,
            ) * (HEAD ** (-0.5))
            ahead_gap = until[:, head : head + 1] - flat[head : head + 1]
            behind_gap = (flat[back : back + 1] - rate[back : back + 1]) - (
                until[:, back : back + 1] - single[:, back : back + 1]
            )
            for gap, keep in ((ahead_gap, low >= high), (behind_gap, low <= high)):
                weighted = jnp.where(keep, jnp.exp(jnp.minimum(gap, 0.0)), 0.0) * scores
                out = jnp.zeros((rows, HEAD), f32)
                for piece in split(weighted):
                    out += jnp.dot(piece, value[:, cols], preferred_element_type=f32)
                inner.append(out)

    with jax.named_scope("state_wait"):
        for copy in arrivals:
            copy.wait_recv()
        loads[4].wait()
        for load in loads[8:]:
            load.wait()
        for part, d in EARLY:
            start_weights(part, d)
    with jax.named_scope("outer"):
        sums = [jnp.sum(rate_all[j], axis=1, keepdims=True) for j in range(spans)]
        mixed = []
        gaps = []
        for j in range(spans):
            ahead_far = jnp.zeros((lines, 1), f32)
            behind_far = jnp.zeros((lines, 1), f32)
            for i in range(spans):
                if i > j:
                    ahead_far += jnp.where(i < me, sums[i], 0.0)
                if i < j:
                    behind_far += jnp.where(i > me, sums[i], 0.0)
            gaps.append((ahead_far, behind_far))
        for head in range(heads):
            cols = slice(head * HEAD, (head + 1) * HEAD)
            back = heads + head
            ahead, behind = inner[2 * head], inner[2 * head + 1]
            for j in range(spans):
                product = jnp.dot(
                    query[:, cols], state_recv[j, head], preferred_element_type=f32
                ) * (HEAD ** (-0.5))
                near = until[:, head : head + 1] + gaps[j][0][head : head + 1]
                far = (
                    after[:, back : back + 1]
                    + single[:, back : back + 1]
                    + gaps[j][1][back : back + 1]
                )
                ahead += jnp.where(j < me, jnp.exp(jnp.minimum(near, 0.0)) * product, 0.0)
                behind += jnp.where(j > me, jnp.exp(jnp.minimum(far, 0.0)) * product, 0.0)
            sides = []
            for row, out in enumerate((ahead, behind)):
                centre = out - jnp.mean(out, axis=1, keepdims=True)
                spread = jnp.mean(centre * centre, axis=1, keepdims=True)
                sides.append(centre * lax.rsqrt(spread + GROUP_EPS) * gains[row : row + 1, cols])
            level = gate[:, cols].astype(f32)
            mixed.append(((level / (1.0 + jnp.exp(-level))) * (sides[0] + sides[1])).astype(bf16))
        mixed = jnp.concatenate(mixed, axis=1)

    def share_rows(index):
        return pl.ds(pl.multiple_of(index * share, share), share)

    with jax.named_scope("attend"):
        loads[5].wait()
        step_cols = math.gcd(model, 512)
        for at in range(0, model, step_cols):
            att_send[:, at : at + step_cols] = jnp.dot(
                mixed, out_w[:, at : at + step_cols], preferred_element_type=f32
            ).astype(bf16)
        pairs = [
            send(att_send.at[share_rows(to)], att_recv.at[i], att_sem.at[i], tp=mate)
            for i, to in enumerate((diag, mate))
        ]
    for part, d in SECOND:
        start_weights(part, d)
    with jax.named_scope("attended_pair"):
        loads[6].wait()
        pairs[0].wait_recv()
        att_mid[...] = (
            att_send[share_rows(cross), :].astype(f32) + att_recv[0].astype(f32)
        ).astype(bf16)
        pairs.append(send(att_mid, att_recv.at[2], att_sem.at[2], tp=cross))
        pairs[1].wait_recv()
    with jax.named_scope("attended_wait"):
        pairs[2].wait_recv()

    def token_rows(span, tp):
        return pl.ds(pl.multiple_of(span * rows + tp * share, share), share)

    with jax.named_scope("normed"):
        attended = att_send[share_rows(lane), :].astype(f32)
        for i in range(1, 3):
            attended = attended + att_recv[i].astype(f32)
        middle = (residual[share_rows(lane), :].astype(f32) + attended).astype(bf16)
        middle_ref[...] = middle
        middle = middle.astype(f32)
        factor = lax.rsqrt(jnp.mean(middle * middle, axis=1, keepdims=True) + NORM_EPS)
        for at in range(0, model, 128):
            gain = norm_gain[at // 128 : at // 128 + 1, :].astype(f32)
            norm_all[token_rows(me, lane), at : at + 128] = (
                middle[:, at : at + 128] * factor * gain
            ).astype(bf16)

    steps = (1, -1)

    def origin(way, hop):
        return me - steps[way] * hop

    def inside(span):
        return (span >= 0) & (span < spans)

    def clamp(span):
        return jnp.clip(span, 0, spans - 1)

    def passes(way, hop):
        return inside(origin(way, hop)) & inside(me + steps[way])

    slab = model // SLABS

    def slab_of(span, tp, c):
        return norm_all.at[token_rows(span, tp), c * slab : (c + 1) * slab]

    def norm_copy(way, hop, c):
        block = slab_of(clamp(origin(way, hop)), lane, c)
        to = clamp(me + steps[way])
        return remote(block, block, norm_sem.at[way, hop, c], norm_leave.at[way, hop], sp=to)

    def mate_copy(span, c):
        block = slab_of(span, lane, c)
        return remote(block, block, gather_sem.at[0], leave_sem.at[0], tp=mate)

    def cross_copy(span, c):
        block = slab_of(span, lane, c)
        return remote(block, block, cross_sem.at[span, c], leave_sem.at[1], tp=cross)

    def diag_copy(span, c):
        block = slab_of(span, cross, c)
        return remote(block, block, gather_sem.at[1], leave_sem.at[2], tp=mate)

    def spread_block(way, hop, c):
        if hop + 1 >= spans:
            return

        @pl.when(passes(way, hop))
        def _():
            norm_copy(way, hop, c).start()

    def norm_hop(hop):
        for c in range(SLABS):
            for way in WAYS:

                @pl.when(inside(origin(way, hop)))
                def _():
                    norm_copy(way, hop - 1, c).wait_recv()
                    spread_block(way, hop, c)
                    cross_copy(clamp(origin(way, hop)), c).start()
                    mate_copy(clamp(origin(way, hop)), c).start()

    def cross_hop(hop):
        for way in range(2 if hop else 1):

            @pl.when(inside(origin(way, hop)))
            def _():
                for c in range(SLABS):
                    cross_copy(clamp(origin(way, hop)), c).wait_recv()
                    diag_copy(clamp(origin(way, hop)), c).start()

    with jax.named_scope("norm0"):
        for c in range(SLABS):
            for way in WAYS:
                spread_block(way, 0, c)
            cross_copy(me, c).start()
            mate_copy(me, c).start()
    def gather_wait():
        whole = norm_all.at[pl.ds(0, rows)]
        for i in range(2):
            remote(whole, whole, gather_sem.at[i], leave_sem.at[0], tp=mate).wait_recv()

    def twin_wait(part):
        def step():
            own_wait(part).wait()
            for d in range(1, spans):
                relay_copy(part, d).wait_recv()

        when_extra(part, me, step)

    groups = max(spans // 2, 1)
    depth = spans // groups

    def blocks(part):
        return groups

    def compute_hidden(part, b):
        cols = cols_of(part, me)
        size = total // groups
        first, stop = b * size, (b + 1) * size
        begin, end = max(first - EDGE, 0), min(stop + EDGE, total)
        both = jnp.dot(norm_all[begin:end, :], wide[part], preferred_element_type=f32)
        here = both.astype(bf16).astype(f32)
        length = end - begin
        row_at = lax.broadcasted_iota(jnp.int32, (length, 1), 0)
        earlier, later = pltpu.roll(here, 1, 0), pltpu.roll(here, length - 1, 0)
        if begin == 0:
            earlier = jnp.where(row_at == 0, 0.0, earlier)
        if end == total:
            later = jnp.where(row_at == length - 1, 0.0, later)
        weight = jnp.concatenate(
            [gate_taps[:, cols].astype(f32), up_taps[:, cols].astype(f32)], axis=1
        )
        conv = weight[0:1] * earlier + weight[1:2] * here + weight[2:3] * later
        conv = conv[first - begin : stop - begin]
        level = conv[:, :128]
        hid_all[first:stop, cols] = ((level / (1.0 + jnp.exp(-level))) * conv[:, 128:]).astype(
            bf16
        )

    def hidden_copy(part, way, hop, b):
        size = total // blocks(part)
        block = hid_all.at[pl.ds(b * size, size), cols_of(part, clamp(origin(way, hop)))]
        return remote(
            block,
            block,
            hid_sem.at[part, way, hop, b],
            hid_leave.at[part, way, hop],
            sp=clamp(me + steps[way]),
        )

    def has(part, span):
        return inside(span) & holds(part, clamp(span)) if part >= least else inside(span)

    def hidden_start(part, way, hop, b):
        if hop + 1 >= spans:
            return

        @pl.when(passes(way, hop) & has(part, origin(way, hop)))
        def _():
            hidden_copy(part, way, hop, b).start()

    def hidden_pass(part, hop, b):
        for way in WAYS:

            @pl.when(has(part, origin(way, hop)))
            def _():
                hidden_copy(part, way, hop - 1, b).wait_recv()

            hidden_start(part, way, hop, b)

    def make_hidden(part):
        twin_wait(part)
        for b in range(blocks(part)):
            if part >= least:

                @pl.when(holds(part, me))
                def _():
                    compute_hidden(part, b)

            else:
                compute_hidden(part, b)
            for way in WAYS:
                hidden_start(part, way, 0, b)

    pairs, crossing = {}, {}

    def down(b):
        few = pl.ds(b * depth, depth)
        if b == 0:
            loads[7].wait()
        tp_send[few] = (
            lax.dot_general(
                hid_all[b * depth * rows : (b + 1) * depth * rows, :],
                down_w[...],
                (((1,), (1,)), ((), ())),
                preferred_element_type=f32,
            )
            .astype(bf16)
            .reshape(depth, rows, part_cols)
        )
        pairs[b] = [
            remote(
                tp_send.at[few, share_rows(to)],
                tp_recv.at[i, few],
                tp_sem.at[b, i],
                tp_leave.at[0],
                tp=mate,
            )
            for i, to in enumerate((diag, mate))
        ]
        for copy in pairs[b]:
            copy.start()

    def cross_step(b):
        few = pl.ds(b * depth, depth)
        pairs[b][0].wait_recv()
        tp_mid[few] = (
            tp_send[few, share_rows(cross)].astype(f32) + tp_recv[0, few].astype(f32)
        ).astype(bf16)
        crossing[b] = remote(
            tp_mid.at[few], tp_recv.at[2, few], tp_sem.at[b, 2], tp_leave.at[0], tp=cross
        )
        crossing[b].start()
        pairs[b][1].wait_recv()

    def row_out(b):
        d = lax.rem(b - me + spans, spans)
        return remote(
            row_send.at[b],
            row_recv.at[me],
            row_sem.at[jnp.maximum(d - 1, 0)],
            row_leave.at[0],
            sp=b,
        )

    def row_step(group):
        crossing[group].wait_recv()
        for b in range(group * depth, (group + 1) * depth):
            summed = tp_send[b, share_rows(lane), :].astype(f32)
            for i in range(1, 3):
                summed = summed + tp_recv[i, b].astype(f32)
            row_send[b] = summed.astype(bf16)

            @pl.when(b != me)
            def _():
                row_out(b).start()

            @pl.when(b == me)
            def _():
                row_recv[me] = row_send[b]

    inner_span = (me > 0) & (me < spans - 1)

    def on_ends(part, d):
        pl.when(jnp.logical_not(inner_span))(lambda: relay_weights(part, d))

    def on_inner(part, d):
        pl.when(inner_span)(lambda: relay_weights(part, d))

    actions = {
        "e": on_ends,
        "i": on_inner,
        "n": norm_hop,
        "x": cross_hop,
        "w": start_weights,
        "r": relay_weights,
        "m": gather_wait,
        "H": make_hidden,
        "h": hidden_pass,
        "D": down,
        "P": cross_step,
        "R": row_step,
    }
    for name, *numbers in ORDER:
        with jax.named_scope(name + "".join(str(number) for number in numbers)):
            actions[name](*numbers)

    with jax.named_scope("final"):
        for d in range(1, spans):
            row_out(span_at(d)).wait_recv()
        for j in range(spans):
            cols = slice(j * part_cols, (j + 1) * part_cols)
            result[:, cols] = (
                middle_ref[:, cols].astype(f32) + row_recv[j].astype(f32)
            ).astype(bf16)
    with jax.named_scope("drain"):
        for copy in sends:
            copy.wait_send()
        for part in range(parts):
            if part < least:
                block = wide.at[part, pl.ds(0, (spans - 1) * half)]
                remote(
                    block, block, w_sem.at[part, 0], w_leave.at[part], sp=span_at(1)
                ).wait_send()
            for d in range(1, spans if part >= least else 1):

                def sent():
                    weight_wait(part, d).wait_send()

                when_extra(part, target(d), sent)

            def relayed():
                block = wide.at[part, pl.ds(0, (spans - 1) * half)]
                remote(
                    block, block, relay_sem.at[part, 0], relay_leave.at[part], grp=1 - side
                ).wait_send()

            when_extra(part, me, relayed)
        whole = norm_all.at[pl.ds(0, rows)]
        for i in range(3):
            remote(whole, whole, gather_sem.at[0], leave_sem.at[i], tp=mate).wait_send()
        remote(state_recv.at[pl.ds(0, spans - 1)], state_recv.at[pl.ds(0, spans - 1)],
               state_sem.at[0, 1], state_leave.at[1], sp=span_at(1)).wait_send()
        remote(rate_all.at[pl.ds(0, spans - 1)], rate_all.at[pl.ds(0, spans - 1)],
               state_sem.at[0, 0], state_leave.at[0], sp=span_at(1)).wait_send()
        remote(tp_recv, tp_recv, tp_sem.at[0, 0], tp_leave.at[0], tp=mate).wait_send()
        remote(row_recv.at[pl.ds(0, spans - 1)], row_recv.at[pl.ds(0, spans - 1)],
               row_sem.at[0], row_leave.at[0], sp=span_at(1)).wait_send()
        for way in range(2):
            for hop in range(spans - 1):

                @pl.when(passes(way, hop))
                def _():
                    block = norm_all.at[pl.ds(0, share)]
                    remote(
                        block,
                        block,
                        norm_sem.at[way, hop, 0],
                        norm_leave.at[way, hop],
                        sp=clamp(me + steps[way]),
                    ).wait_send()

                for part in range(parts):

                    @pl.when(passes(way, hop) & has(part, origin(way, hop)))
                    def _():
                        block = hid_all.at[:, pl.ds(0, 128)]
                        remote(
                            block,
                            block,
                            hid_sem.at[part, way, hop, 0],
                            hid_leave.at[part, way, hop],
                            sp=clamp(me + steps[way]),
                        ).wait_send()


def fused_block(
    query_rows,
    key_rows,
    value_rows,
    gate_rows,
    log_decay,
    head_gain,
    out_weight,
    residual,
    norm_gain,
    gate_weight,
    up_weight,
    down_weight,
    gate_taps,
    up_taps,
):
    spans, shares = (lax.axis_size("sp"), lax.axis_size("tp"))
    rows, width = query_rows.shape
    model = residual.shape[1]
    units = gate_weight.shape[1]
    part_cols, share = (model // spans, rows // shares)
    total = spans * rows
    counts = tile_counts(units // 128, spans)
    least, parts = min(counts[0]), max(counts[0])
    lines = log_decay.shape[0] * log_decay.shape[1]
    heads = width // HEAD
    rates = log_decay.reshape(lines, rows)
    f32, bf16 = jnp.float32, jnp.bfloat16
    far = pl.BlockSpec(memory_space=pltpu.HBM)
    dma = pltpu.SemaphoreType.DMA
    vmem = pltpu.VMEM
    return pl.pallas_call(
        functools.partial(block_kernel, spans, shares),
        out_shape=jax.ShapeDtypeStruct((share, model), bf16),
        in_specs=[far] * 14,
        out_specs=pl.BlockSpec(memory_space=pltpu.VMEM),
        scratch_shapes=[
            vmem((rows, width), bf16),
            vmem((rows, width), bf16),
            vmem((rows, width), bf16),
            vmem((rows, width), bf16),
            vmem((lines, rows), f32),
            vmem((rows, model), bf16),
            vmem(out_weight.shape, bf16),
            vmem(down_weight.shape, bf16),
            vmem(head_gain.shape, f32),
            vmem((model // 128, 128), bf16),
            vmem(gate_taps.shape, bf16),
            vmem(up_taps.shape, bf16),
            vmem((spans, lines, rows), f32),
            vmem((2, heads, HEAD, HEAD), bf16),
            vmem((spans, heads, HEAD, HEAD), bf16),
            vmem((parts, model, 256), bf16),
            vmem((rows, model), bf16),
            vmem((3, share, model), bf16),
            vmem((share, model), bf16),
            vmem((share, model), bf16),
            vmem((total, model), bf16),
            vmem((total, units), bf16),
            vmem((spans, rows, part_cols), bf16),
            vmem((3, spans, share, part_cols), bf16),
            vmem((spans, share, part_cols), bf16),
            vmem((spans, share, part_cols), bf16),
            vmem((spans, share, part_cols), bf16),
            dma((12,)),
            dma((parts,)),
            dma((spans - 1, 2)),
            dma((2,)),
            dma((parts, spans - 1)),
            dma((parts, spans - 1)),
            dma((least + (parts - least) * (spans - 1),)),
            dma((parts,)),
            dma((3, 2)),
            dma((2, spans - 1, SLABS)),
            dma((2, spans - 1)),
            dma((spans, SLABS)),
            dma((2,)),
            dma((3,)),
            dma((parts, 2, spans - 1, spans // 2)),
            dma((parts, 2, spans - 1)),
            dma((spans // 2, 3)),
            dma((1,)),
            dma((spans - 1,)),
            dma((1,)),
        ],
        compiler_params=pltpu.CompilerParams(
            collective_id=0, has_side_effects=True, vmem_limit_bytes=GRANT
        ),
    )(
        *(
            pltpu.with_memory_space_constraint(value, pltpu.HBM)
            for value in (
                query_rows,
                key_rows,
                value_rows,
                gate_rows,
                rates,
                head_gain,
                residual,
                norm_gain.reshape(model // 128, 128),
                gate_taps,
                up_taps,
                out_weight,
                gate_weight,
                up_weight,
                down_weight,
            )
        )
    )


def either(*args):
    spans, shares, twins = (lax.axis_size(name) for name in ("sp", "tp", "grp"))
    span_tokens = args[0].shape[0] * spans
    model_width = args[7].shape[1]
    lanes = args[9].shape[1] // 128
    fits = spans == 4 and lanes >= 2 * spans
    if fits and span_tokens < model_width and twins == 2 and shares == 4:
        return fused_block(*args)
    return shards(*args)


def solution(mesh):
    in_specs = (
        P(("grp", "sp"), "tp"),
        P(("grp", "sp"), "tp"),
        P(("grp", "sp"), "tp"),
        P(("grp", "sp"), "tp"),
        P(None, "tp", ("grp", "sp")),
        P(None, "tp"),
        P("tp", None),
        P(("grp", "sp"), None),
        P(),
        P("sp", "tp"),
        P("sp", "tp"),
        P("sp", "tp"),
        P(None, "tp"),
        P(None, "tp"),
    )
    out_specs = P(("grp", "sp", "tp"), None)
    return jax.shard_map(either, mesh=mesh, in_specs=in_specs, out_specs=out_specs, check_vma=False)
```

```python
import functools
import math

import jax
import jax.numpy as jnp
from jax import lax
from jax.experimental import pallas as pl
from jax.experimental.pallas import tpu as pltpu
from jax.sharding import PartitionSpec as P

HEAD = 128
GRANT = 40 << 20
SLABS = 4
PAIRED = False
SPLIT = 'even'
WAYS = (0, 1)
EARLY = ((0, 3), (0, 1), (0, 2))
SECOND = ()
ORDER = (('r', 0, 1), ('n', 1), ('x', 0), ('r', 0, 2), ('n', 2), ('w', 1, 1), ('x', 1), ('r', 0, 3), ('w', 1, 2), ('w', 1, 3), ('n', 3), ('x', 2), ('r', 1, 1), ('x', 3), ('m',), ('H', 0), ('w', 2, 1), ('r', 1, 3), ('w', 2, 2), ('r', 1, 2), ('w', 2, 3), ('h', 0, 1, 0), ('h', 0, 1, 1), ('H', 1), ('r', 2, 1), ('r', 2, 2), ('r', 2, 3), ('h', 0, 2, 0), ('h', 0, 2, 1), ('h', 1, 1, 0), ('h', 1, 1, 1), ('H', 2), ('h', 0, 3, 0), ('h', 0, 3, 1), ('h', 1, 2, 0), ('h', 1, 3, 0), ('h', 2, 1, 0), ('h', 2, 2, 0), ('h', 2, 3, 0), ('D', 0), ('h', 1, 2, 1), ('h', 1, 3, 1), ('h', 2, 1, 1), ('P', 0), ('h', 2, 2, 1), ('h', 2, 3, 1), ('D', 1), ('P', 1), ('R', 0), ('R', 1))
EDGE = 16


FULL_PRECISION = lax.Precision.HIGHEST
GROUP_EPS = 1e-05
NORM_EPS = 1e-06


def prefix(value, axis, join, neutral, backward):
    count, mine = (lax.axis_size(axis), lax.axis_index(axis))
    pieces = jax.tree.map(lambda part: lax.all_gather(part, axis), value)
    if backward:
        pieces = jax.tree.map(lambda part: part[::-1], pieces)
        mine = count - 1 - mine
    running = jax.tree.map(
        lambda part, zero: jnp.full_like(part, 0) + jnp.asarray(zero, part.dtype), value, neutral
    )

    def lap(position, running):
        longer = join(running, jax.tree.map(lambda part: part[position], pieces))
        return jax.tree.map(lambda new, old: jnp.where(position < mine, new, old), longer, running)

    return lax.fori_loop(0, count - 1, lap, running)


def padded_2(shard, sides, width):
    for axis, dim in sides:
        size, length = (lax.axis_size(axis), shard.shape[dim])
        up = [(i, (i + 1) % size) for i in range(size - 1)]
        down = [(j, i) for i, j in up]
        last = lax.slice_in_dim(shard, length - width, length, axis=dim)
        initial = lax.slice_in_dim(shard, 0, width, axis=dim)
        before = lax.ppermute(last, axis, up)
        after = lax.ppermute(initial, axis, down)
        shard = jnp.concatenate([before, shard, after], axis=dim)
    return shard


def state_combine(earlier, later):
    return (earlier[0] * later[0], earlier[1] * later[0][:, None, None] + later[1])


def group_norm(values):
    length, head_count, head_width = values.shape
    centre = values - jnp.mean(values, axis=2, keepdims=True)
    spread = jnp.mean(centre * centre, axis=2, keepdims=True)
    return (centre * lax.rsqrt(spread + GROUP_EPS)).reshape(length, head_count * head_width)


def rms_scale(middle, gain):
    values = middle.astype(jnp.float32)
    multiplier = lax.rsqrt(jnp.mean(values * values, axis=1, keepdims=True) + NORM_EPS)
    return (values * multiplier * gain.astype(jnp.float32)).astype(jnp.bfloat16)


def local_retention(query_all, key_all, value_all, log_rates):
    length, head_count, head_width = query_all.shape
    block_len = math.gcd(length, 512)
    block_count = length // block_len
    cumul = jnp.cumsum(log_rates, axis=1).T
    query_block = query_all.reshape(block_count, block_len, head_count, head_width)
    key_block = key_all.reshape(block_count, block_len, head_count, head_width)
    value_block = value_all.reshape(block_count, block_len, head_count, head_width)
    cumul_block = cumul.reshape(block_count, block_len, head_count)
    before = jnp.concatenate(
        [jnp.zeros((1, head_count), jnp.float32), cumul_block[:-1, -1]], axis=0
    )
    local_cumul = cumul_block - before[:, None, :]
    gap_logs = local_cumul[:, :, None, :] - local_cumul[:, None, :, :]
    lower_mask = (jnp.arange(block_len)[:, None] >= jnp.arange(block_len)[None, :])[
        None, :, :, None
    ]
    decay_mask = jnp.where(lower_mask, jnp.exp(jnp.minimum(gap_logs, 0.0)), 0.0)
    scores = (
        jnp.einsum("bthd,bshd->btsh", query_block, key_block, precision=FULL_PRECISION) * decay_mask
    )
    inner_part = jnp.einsum("btsh,bshe->bthe", scores, value_block, precision=FULL_PRECISION)
    to_end = jnp.exp(local_cumul[:, -1:, :] - local_cumul)
    block_states = jnp.einsum(
        "bshd,bshe->bhde", key_block * to_end[..., None], value_block, precision=FULL_PRECISION
    )
    block_decay = jnp.exp(local_cumul[:, -1, :])

    def carry_step(carry_state, inputs):
        return (carry_state * inputs[0][:, None, None] + inputs[1], carry_state)

    zero_state = jnp.zeros((head_count, head_width, head_width), jnp.float32)
    end_state, entering = lax.scan(carry_step, zero_state, (block_decay, block_states))
    carried = jnp.einsum(
        "bthd,bhde->bthe",
        query_block * jnp.exp(local_cumul)[..., None],
        entering,
        precision=FULL_PRECISION,
    )
    output = (inner_part + carried).reshape(length, head_count, head_width)
    return (output, end_state, cumul, jnp.exp(cumul[-1]))


def with_incoming(output, query_all, cumul, incoming):
    return output + jnp.einsum(
        "thd,hde->the", query_all * jnp.exp(cumul)[:, :, None], incoming, precision=FULL_PRECISION
    )


def shards(
    query_rows,
    key_rows,
    value_rows,
    gate_rows,
    log_decay,
    head_gain,
    out_weight,
    residual,
    norm_gain,
    gate_weight,
    up_weight,
    down_weight,
    gate_taps,
    up_taps,
):
    pair_local = jnp.concatenate([gate_weight, up_weight], axis=1)
    row_count = query_rows.shape[0]
    head_count = query_rows.shape[1] // HEAD
    key_scale = HEAD ** (-0.5)
    query_all = query_rows.astype(jnp.float32).reshape(row_count, head_count, HEAD)
    key_all = key_rows.astype(jnp.float32).reshape(row_count, head_count, HEAD) * key_scale
    value_all = value_rows.astype(jnp.float32).reshape(row_count, head_count, HEAD)
    identity = (
        jnp.ones((head_count,), jnp.float32),
        jnp.zeros((head_count, HEAD, HEAD), jnp.float32),
    )
    ahead_local, ahead_state, ahead_cumul, ahead_decay = local_retention(
        query_all, key_all, value_all, log_decay[0]
    )
    query_back = query_all[::-1]
    behind_local, behind_state, behind_cumul, behind_decay = local_retention(
        query_back, key_all[::-1], value_all[::-1], log_decay[1][:, ::-1]
    )
    ahead_in = prefix((ahead_decay, ahead_state), "sp", state_combine, identity, False)[1]
    behind_in = prefix((behind_decay, behind_state), "sp", state_combine, identity, True)[1]
    ahead_out = with_incoming(ahead_local, query_all, ahead_cumul, ahead_in)
    behind_out = with_incoming(behind_local, query_back, behind_cumul, behind_in)[::-1]
    combined = group_norm(ahead_out) * head_gain[0] + group_norm(behind_out) * head_gain[1]
    mixed_heads = (jax.nn.silu(gate_rows.astype(jnp.float32)) * combined).astype(jnp.bfloat16)
    gathered = (
        lax.all_gather(pair_local, "sp", axis=0, tiled=True),
        lax.all_gather(down_weight, "sp", axis=0, tiled=True),
    )
    pair_full, down_full = gathered
    share_rows = row_count // lax.axis_size("tp")
    own_start = lax.axis_index("tp") * share_rows
    picked = mixed_heads
    attended = lax.psum_scatter(
        jnp.dot(picked, out_weight, preferred_element_type=jnp.float32).astype(jnp.bfloat16),
        "tp",
        scatter_dimension=0,
        tiled=True,
    ).astype(jnp.float32)
    residual_own = lax.dynamic_slice_in_dim(residual, own_start, share_rows, 0)
    middle_own = lax.optimization_barrier(
        (residual_own.astype(jnp.float32) + attended).astype(jnp.bfloat16)
    )
    normed = rms_scale(middle_own, norm_gain)
    pre_both = jnp.dot(
        lax.all_gather(normed, "tp", axis=0, tiled=True),
        pair_full,
        preferred_element_type=jnp.float32,
    ).astype(jnp.bfloat16)
    padded = padded_2(pre_both, (("sp", 0),), 1)
    half_width = gate_taps.shape[1]
    tap_table = jnp.concatenate([gate_taps, up_taps], axis=1).astype(jnp.float32)
    conv_out = (
        tap_table[0] * padded[:-2].astype(jnp.float32)
        + tap_table[1] * padded[1:-1].astype(jnp.float32)
        + tap_table[2] * padded[2:].astype(jnp.float32)
    )
    hidden = (jax.nn.silu(conv_out[:, :half_width]) * conv_out[:, half_width:]).astype(jnp.bfloat16)
    picked = hidden
    ff_out = lax.psum_scatter(
        lax.dot_general(
            picked, down_full, (((1,), (1,)), ((), ())), preferred_element_type=jnp.float32
        ).astype(jnp.bfloat16),
        "tp",
        scatter_dimension=0,
        tiled=True,
    ).astype(jnp.float32)
    return (middle_own.astype(jnp.float32) + ff_out).astype(jnp.bfloat16)


def tile_counts(lanes, spans):
    if SPLIT == "ends":
        outer = lanes // spans
        near = (lanes - 2 * outer + 1) // 2
        far = lanes - 2 * outer - near
        even, odd = (outer, near, far, outer), (outer, far, near, outer)
    else:
        least, rest = divmod(lanes, spans)
        even = tuple(least + (j < rest) for j in range(spans))
        odd = even[::-1]
        if SPLIT == "middle":
            even, odd = (even[0], even[1], even[3], even[2]), (odd[1], odd[0], odd[2], odd[3])
    return even, odd


def block_kernel(
    spans,
    shares,
    query_hbm,
    key_hbm,
    value_hbm,
    gate_hbm,
    rates_hbm,
    gains_hbm,
    residual_hbm,
    norm_gain_hbm,
    gate_taps_hbm,
    up_taps_hbm,
    out_hbm,
    fg_hbm,
    fu_hbm,
    down_hbm,
    result,
    query,
    key,
    value,
    gate,
    rates,
    residual,
    out_w,
    down_w,
    gains,
    norm_gain,
    gate_taps,
    up_taps,
    rate_all,
    state_send,
    state_recv,
    wide,
    att_send,
    att_recv,
    att_mid,
    middle_ref,
    norm_all,
    hid_all,
    tp_send,
    tp_recv,
    tp_mid,
    row_send,
    row_recv,
    local_sem,
    own_sem,
    state_sem,
    state_leave,
    w_sem,
    relay_sem,
    w_leave,
    relay_leave,
    att_sem,
    norm_sem,
    norm_leave,
    cross_sem,
    gather_sem,
    leave_sem,
    hid_sem,
    hid_leave,
    tp_sem,
    tp_leave,
    row_sem,
    row_leave,
):
    side, me, lane = lax.axis_index("grp"), lax.axis_index("sp"), lax.axis_index("tp")
    rows, width = query.shape
    heads = width // HEAD
    share = rows // shares
    model = residual.shape[1]
    part_cols = model // spans
    half = part_cols // 2
    total = spans * rows
    lines = rates.shape[0]
    units = gate_taps.shape[1]
    counts = tile_counts(units // 128, spans)
    least, parts = min(counts[0]), max(counts[0])
    f32, bf16 = jnp.float32, jnp.bfloat16
    mate = lane + 1 - 2 * lax.rem(lane, 2)
    cross = lax.rem(lane + shares // 2, shares)
    odd = lax.rem(lane, 2)
    diag = cross + 1 - 2 * odd
    sends = []

    def remote(src, dst, sems, leave=None, **place):
        return pltpu.make_async_remote_copy(
            src_ref=src,
            dst_ref=dst,
            send_sem=sems.at[0] if leave is None else leave,
            recv_sem=sems.at[1] if leave is None else sems,
            device_id=place,
            device_id_type=pl.DeviceIdType.MESH,
        )

    def send(src, dst, sems, **place):
        copy = remote(src, dst, sems, **place)
        copy.start()
        sends.append(copy)
        return copy

    def span_at(step):
        return lax.rem(me + step, spans)

    def target(d):
        if not PAIRED:
            return span_at(d)
        if d == 1:
            return me + 1 - 2 * lax.rem(me, 2)
        return lax.rem(me + 2, spans) if d == 2 else spans - 1 - me

    def source(d):
        return target(d) if PAIRED else lax.rem(me + spans - d, spans)

    def share_at(step):
        return lax.rem(lane + step, shares)

    def pick(tables, span):
        value = 0
        for j in range(spans):
            mine = jnp.where(odd == 0, tables[0][j], tables[1][j])
            value = value + jnp.where(span == j, mine, 0)
        return value

    def holds(part, span):
        return pick(counts, span) > part

    starts = [[sum(row[:j]) for j in range(spans)] for row in counts]

    def first_col(span):
        return pick(starts, span) * 128

    def cols_of(part, span):
        begin = jnp.minimum(first_col(span) + part * 128, units - 128)
        return pl.ds(pl.multiple_of(begin, 128), 128)

    barrier = pltpu.get_barrier_semaphore()
    peers = [{"grp": 1 - side}]
    peers += [{"sp": span_at(d)} for d in range(1, spans)]
    peers += [{"tp": share_at(d)} for d in range(1, shares)]
    for place in peers:
        pl.semaphore_signal(
            barrier, inc=1, device_id=place, device_id_type=pl.DeviceIdType.MESH
        )
    loads = [
        pltpu.make_async_copy(src, dst, local_sem.at[i])
        for i, (src, dst) in enumerate(
            (
                (rates_hbm, rates),
                (key_hbm, key),
                (value_hbm, value),
                (query_hbm, query),
                (gate_hbm, gate),
                (out_hbm, out_w),
                (residual_hbm, residual),
                (down_hbm, down_w),
                (gains_hbm, gains),
                (norm_gain_hbm, norm_gain),
                (gate_taps_hbm, gate_taps),
                (up_taps_hbm, up_taps),
            )
        )
    ]
    for load in loads:
        load.start()

    weights = (fg_hbm, fu_hbm)

    def lanes(g):
        return slice(g * 128, (g + 1) * 128)

    def own_copy(part, g):
        return pltpu.make_async_copy(
            weights[g].at[:, cols_of(part, me)],
            wide.at[part, pl.ds(pl.multiple_of(me * part_cols, part_cols), part_cols), lanes(g)],
            own_sem.at[part],
        )

    def own_wait(part):
        block = wide.at[part, pl.ds(pl.multiple_of(me * part_cols, part_cols), part_cols)]
        return pltpu.make_async_copy(block, block, own_sem.at[part])

    def half_rows(span):
        begin = span * part_cols + side * half
        return pl.ds(pl.multiple_of(begin, half), half)

    def leave_at(part, d):
        return part if part < least else least + (part - least) * (spans - 1) + d - 1

    def weight_copy(part, d, g):
        to = target(d)
        return remote(
            weights[g].at[pl.ds(pl.multiple_of(side * half, half), half), cols_of(part, to)],
            wide.at[part, half_rows(me), lanes(g)],
            w_sem.at[part, d - 1],
            w_leave.at[leave_at(part, d)],
            sp=to,
        )

    def relay_copy(part, d):
        block = wide.at[part, half_rows(source(d))]
        return remote(block, block, relay_sem.at[part, d - 1], relay_leave.at[part], grp=1 - side)

    def weight_wait(part, d):
        block = wide.at[part, half_rows(source(d))]
        sem = w_sem.at[part, d - 1]
        return remote(block, block, sem, w_leave.at[leave_at(part, d)], sp=target(d))

    def when_extra(part, span, step):
        if part >= least:
            pl.when(holds(part, span))(step)
        else:
            step()

    def start_weights(part, d):
        def step():
            for g in range(2):
                weight_copy(part, d, g).start()

        when_extra(part, target(d), step)

    def relay_weights(part, d):
        def step():
            weight_wait(part, d).wait_recv()
            relay_copy(part, d).start()

        when_extra(part, me, step)

    def own_weights(part):
        def step():
            for g in range(2):
                own_copy(part, g).start()

        when_extra(part, me, step)

    for part in range(parts):
        own_weights(part)

    with jax.named_scope("states"):
        loads[0].wait()
        low = lax.broadcasted_iota(jnp.int32, (rows, rows), 0)
        high = lax.broadcasted_iota(jnp.int32, (rows, rows), 1)
        rate = rates[...]

        def tall(table):
            return lax.dot_general(
                table.astype(f32),
                rate,
                (((1,), (1,)), ((), ())),
                precision=FULL_PRECISION,
                preferred_element_type=f32,
            )

        until = tall(low >= high)
        single = tall(low == high)
        after = tall(low < high)
        flat = jnp.dot(
            rate, (low <= high).astype(f32), precision=FULL_PRECISION, preferred_element_type=f32
        )
        loads[1].wait()
        loads[2].wait()

        def split(x):
            top = x.astype(bf16)
            return top, (x - top.astype(f32)).astype(bf16)

        for head in range(heads):
            cols = slice(head * HEAD, (head + 1) * HEAD)
            held = value[:, cols]
            for way in range(2):
                line = way * heads + head
                if way == 0:
                    weight = after[:, line : line + 1]
                else:
                    weight = until[:, line : line + 1] - single[:, line : line + 1]
                lifted = key[:, cols].astype(f32) * jnp.exp(jnp.minimum(weight, 0.0))
                state = jnp.zeros((HEAD, HEAD), f32)
                for piece in split(lifted):
                    state += lax.dot_general(
                        piece, held, (((0,), (0,)), ((), ())), preferred_element_type=f32
                    )
                state = state - jnp.mean(state, axis=1, keepdims=True)
                state_send[way, head] = state.astype(bf16)

    with jax.named_scope("barrier"):
        pl.semaphore_wait(barrier, len(peers))
    arrivals = []
    for d in range(1, spans):
        to = span_at(d)
        way = jnp.where(to > me, 0, 1)
        arrivals.append(
            remote(rates, rate_all.at[me], state_sem.at[d - 1, 0], state_leave.at[0], sp=to)
        )
        arrivals.append(
            remote(
                state_send.at[way],
                state_recv.at[me],
                state_sem.at[d - 1, 1],
                state_leave.at[1],
                sp=to,
            )
        )
    for copy in arrivals:
        copy.start()

    with jax.named_scope("inner"):
        loads[3].wait()
        inner = []
        for head in range(heads):
            cols = slice(head * HEAD, (head + 1) * HEAD)
            back = heads + head
            scores = lax.dot_general(
                query[:, cols],
                key[:, cols],
                (((1,), (1,)), ((), ())),
                preferred_element_type=f32,
            ) * (HEAD ** (-0.5))
            ahead_gap = until[:, head : head + 1] - flat[head : head + 1]
            behind_gap = (flat[back : back + 1] - rate[back : back + 1]) - (
                until[:, back : back + 1] - single[:, back : back + 1]
            )
            for gap, keep in ((ahead_gap, low >= high), (behind_gap, low <= high)):
                weighted = jnp.where(keep, jnp.exp(jnp.minimum(gap, 0.0)), 0.0) * scores
                out = jnp.zeros((rows, HEAD), f32)
                for piece in split(weighted):
                    out += jnp.dot(piece, value[:, cols], preferred_element_type=f32)
                inner.append(out)

    with jax.named_scope("state_wait"):
        for copy in arrivals:
            copy.wait_recv()
        loads[4].wait()
        for load in loads[8:]:
            load.wait()
        for part, d in EARLY:
            start_weights(part, d)
    with jax.named_scope("outer"):
        sums = [jnp.sum(rate_all[j], axis=1, keepdims=True) for j in range(spans)]
        mixed = []
        gaps = []
        for j in range(spans):
            ahead_far = jnp.zeros((lines, 1), f32)
            behind_far = jnp.zeros((lines, 1), f32)
            for i in range(spans):
                if i > j:
                    ahead_far += jnp.where(i < me, sums[i], 0.0)
                if i < j:
                    behind_far += jnp.where(i > me, sums[i], 0.0)
            gaps.append((ahead_far, behind_far))
        for head in range(heads):
            cols = slice(head * HEAD, (head + 1) * HEAD)
            back = heads + head
            ahead, behind = inner[2 * head], inner[2 * head + 1]
            for j in range(spans):
                product = jnp.dot(
                    query[:, cols], state_recv[j, head], preferred_element_type=f32
                ) * (HEAD ** (-0.5))
                near = until[:, head : head + 1] + gaps[j][0][head : head + 1]
                far = (
                    after[:, back : back + 1]
                    + single[:, back : back + 1]
                    + gaps[j][1][back : back + 1]
                )
                ahead += jnp.where(j < me, jnp.exp(jnp.minimum(near, 0.0)) * product, 0.0)
                behind += jnp.where(j > me, jnp.exp(jnp.minimum(far, 0.0)) * product, 0.0)
            sides = []
            for row, out in enumerate((ahead, behind)):
                centre = out - jnp.mean(out, axis=1, keepdims=True)
                spread = jnp.mean(centre * centre, axis=1, keepdims=True)
                sides.append(centre * lax.rsqrt(spread + GROUP_EPS) * gains[row : row + 1, cols])
            level = gate[:, cols].astype(f32)
            mixed.append(((level / (1.0 + jnp.exp(-level))) * (sides[0] + sides[1])).astype(bf16))
        mixed = jnp.concatenate(mixed, axis=1)

    def share_rows(index):
        return pl.ds(pl.multiple_of(index * share, share), share)

    with jax.named_scope("attend"):
        loads[5].wait()
        step_cols = math.gcd(model, 512)
        for at in range(0, model, step_cols):
            att_send[:, at : at + step_cols] = jnp.dot(
                mixed, out_w[:, at : at + step_cols], preferred_element_type=f32
            ).astype(bf16)
        pairs = [
            send(att_send.at[share_rows(to)], att_recv.at[i], att_sem.at[i], tp=mate)
            for i, to in enumerate((diag, mate))
        ]
    for part, d in SECOND:
        start_weights(part, d)
    with jax.named_scope("attended_pair"):
        loads[6].wait()
        pairs[0].wait_recv()
        att_mid[...] = (
            att_send[share_rows(cross), :].astype(f32) + att_recv[0].astype(f32)
        ).astype(bf16)
        pairs.append(send(att_mid, att_recv.at[2], att_sem.at[2], tp=cross))
        pairs[1].wait_recv()
    with jax.named_scope("attended_wait"):
        pairs[2].wait_recv()

    def token_rows(span, tp):
        return pl.ds(pl.multiple_of(span * rows + tp * share, share), share)

    with jax.named_scope("normed"):
        attended = att_send[share_rows(lane), :].astype(f32)
        for i in range(1, 3):
            attended = attended + att_recv[i].astype(f32)
        middle = (residual[share_rows(lane), :].astype(f32) + attended).astype(bf16)
        middle_ref[...] = middle
        middle = middle.astype(f32)
        factor = lax.rsqrt(jnp.mean(middle * middle, axis=1, keepdims=True) + NORM_EPS)
        for at in range(0, model, 128):
            gain = norm_gain[at // 128 : at // 128 + 1, :].astype(f32)
            norm_all[token_rows(me, lane), at : at + 128] = (
                middle[:, at : at + 128] * factor * gain
            ).astype(bf16)

    steps = (1, -1)

    def origin(way, hop):
        return me - steps[way] * hop

    def inside(span):
        return (span >= 0) & (span < spans)

    def clamp(span):
        return jnp.clip(span, 0, spans - 1)

    def passes(way, hop):
        return inside(origin(way, hop)) & inside(me + steps[way])

    slab = model // SLABS

    def slab_of(span, tp, c):
        return norm_all.at[token_rows(span, tp), c * slab : (c + 1) * slab]

    def norm_copy(way, hop, c):
        block = slab_of(clamp(origin(way, hop)), lane, c)
        to = clamp(me + steps[way])
        return remote(block, block, norm_sem.at[way, hop, c], norm_leave.at[way, hop], sp=to)

    def mate_copy(span, c):
        block = slab_of(span, lane, c)
        return remote(block, block, gather_sem.at[0], leave_sem.at[0], tp=mate)

    def cross_copy(span, c):
        block = slab_of(span, lane, c)
        return remote(block, block, cross_sem.at[span, c], leave_sem.at[1], tp=cross)

    def diag_copy(span, c):
        block = slab_of(span, cross, c)
        return remote(block, block, gather_sem.at[1], leave_sem.at[2], tp=mate)

    def spread_block(way, hop, c):
        if hop + 1 >= spans:
            return

        @pl.when(passes(way, hop))
        def _():
            norm_copy(way, hop, c).start()

    def norm_hop(hop):
        for c in range(SLABS):
            for way in WAYS:

                @pl.when(inside(origin(way, hop)))
                def _():
                    norm_copy(way, hop - 1, c).wait_recv()
                    spread_block(way, hop, c)
                    cross_copy(clamp(origin(way, hop)), c).start()
                    mate_copy(clamp(origin(way, hop)), c).start()

    def cross_hop(hop):
        for way in range(2 if hop else 1):

            @pl.when(inside(origin(way, hop)))
            def _():
                for c in range(SLABS):
                    cross_copy(clamp(origin(way, hop)), c).wait_recv()
                    diag_copy(clamp(origin(way, hop)), c).start()

    with jax.named_scope("norm0"):
        for c in range(SLABS):
            for way in WAYS:
                spread_block(way, 0, c)
            cross_copy(me, c).start()
            mate_copy(me, c).start()
    def gather_wait():
        whole = norm_all.at[pl.ds(0, rows)]
        for i in range(2):
            remote(whole, whole, gather_sem.at[i], leave_sem.at[0], tp=mate).wait_recv()

    def twin_wait(part):
        def step():
            own_wait(part).wait()
            for d in range(1, spans):
                relay_copy(part, d).wait_recv()

        when_extra(part, me, step)

    groups = max(spans // 2, 1)
    depth = spans // groups

    def blocks(part):
        return groups

    def compute_hidden(part, b):
        cols = cols_of(part, me)
        size = total // groups
        first, stop = b * size, (b + 1) * size
        begin, end = max(first - EDGE, 0), min(stop + EDGE, total)
        both = jnp.dot(norm_all[begin:end, :], wide[part], preferred_element_type=f32)
        here = both.astype(bf16).astype(f32)
        length = end - begin
        row_at = lax.broadcasted_iota(jnp.int32, (length, 1), 0)
        earlier, later = pltpu.roll(here, 1, 0), pltpu.roll(here, length - 1, 0)
        if begin == 0:
            earlier = jnp.where(row_at == 0, 0.0, earlier)
        if end == total:
            later = jnp.where(row_at == length - 1, 0.0, later)
        weight = jnp.concatenate(
            [gate_taps[:, cols].astype(f32), up_taps[:, cols].astype(f32)], axis=1
        )
        conv = weight[0:1] * earlier + weight[1:2] * here + weight[2:3] * later
        conv = conv[first - begin : stop - begin]
        level = conv[:, :128]
        hid_all[first:stop, cols] = ((level / (1.0 + jnp.exp(-level))) * conv[:, 128:]).astype(
            bf16
        )

    def hidden_copy(part, way, hop, b):
        size = total // blocks(part)
        block = hid_all.at[pl.ds(b * size, size), cols_of(part, clamp(origin(way, hop)))]
        return remote(
            block,
            block,
            hid_sem.at[part, way, hop, b],
            hid_leave.at[part, way, hop],
            sp=clamp(me + steps[way]),
        )

    def has(part, span):
        return inside(span) & holds(part, clamp(span)) if part >= least else inside(span)

    def hidden_start(part, way, hop, b):
        if hop + 1 >= spans:
            return

        @pl.when(passes(way, hop) & has(part, origin(way, hop)))
        def _():
            hidden_copy(part, way, hop, b).start()

    def hidden_pass(part, hop, b):
        for way in WAYS:

            @pl.when(has(part, origin(way, hop)))
            def _():
                hidden_copy(part, way, hop - 1, b).wait_recv()

            hidden_start(part, way, hop, b)

    def make_hidden(part):
        twin_wait(part)
        for b in range(blocks(part)):
            if part >= least:

                @pl.when(holds(part, me))
                def _():
                    compute_hidden(part, b)

            else:
                compute_hidden(part, b)
            for way in WAYS:
                hidden_start(part, way, 0, b)

    pairs, crossing = {}, {}

    def down(b):
        few = pl.ds(b * depth, depth)
        if b == 0:
            loads[7].wait()
        tp_send[few] = (
            lax.dot_general(
                hid_all[b * depth * rows : (b + 1) * depth * rows, :],
                down_w[...],
                (((1,), (1,)), ((), ())),
                preferred_element_type=f32,
            )
            .astype(bf16)
            .reshape(depth, rows, part_cols)
        )
        pairs[b] = [
            remote(
                tp_send.at[few, share_rows(to)],
                tp_recv.at[i, few],
                tp_sem.at[b, i],
                tp_leave.at[0],
                tp=mate,
            )
            for i, to in enumerate((diag, mate))
        ]
        for copy in pairs[b]:
            copy.start()

    def cross_step(b):
        few = pl.ds(b * depth, depth)
        pairs[b][0].wait_recv()
        tp_mid[few] = (
            tp_send[few, share_rows(cross)].astype(f32) + tp_recv[0, few].astype(f32)
        ).astype(bf16)
        crossing[b] = remote(
            tp_mid.at[few], tp_recv.at[2, few], tp_sem.at[b, 2], tp_leave.at[0], tp=cross
        )
        crossing[b].start()

    def row_out(b):
        d = lax.rem(b - me + spans, spans)
        return remote(
            row_send.at[b],
            row_recv.at[me],
            row_sem.at[jnp.maximum(d - 1, 0)],
            row_leave.at[0],
            sp=b,
        )

    def row_step(group):
        pairs[group][1].wait_recv()
        crossing[group].wait_recv()
        for b in range(group * depth, (group + 1) * depth):
            summed = tp_send[b, share_rows(lane), :].astype(f32)
            for i in range(1, 3):
                summed = summed + tp_recv[i, b].astype(f32)
            row_send[b] = summed.astype(bf16)

            @pl.when(b != me)
            def _():
                row_out(b).start()

            @pl.when(b == me)
            def _():
                row_recv[me] = row_send[b]

    inner_span = (me > 0) & (me < spans - 1)

    def on_ends(part, d):
        pl.when(jnp.logical_not(inner_span))(lambda: relay_weights(part, d))

    def on_inner(part, d):
        pl.when(inner_span)(lambda: relay_weights(part, d))

    actions = {
        "e": on_ends,
        "i": on_inner,
        "n": norm_hop,
        "x": cross_hop,
        "w": start_weights,
        "r": relay_weights,
        "m": gather_wait,
        "H": make_hidden,
        "h": hidden_pass,
        "D": down,
        "P": cross_step,
        "R": row_step,
    }
    for name, *numbers in ORDER:
        with jax.named_scope(name + "".join(str(number) for number in numbers)):
            actions[name](*numbers)

    with jax.named_scope("final"):
        for d in range(1, spans):
            row_out(span_at(d)).wait_recv()
        for j in range(spans):
            cols = slice(j * part_cols, (j + 1) * part_cols)
            result[:, cols] = (
                middle_ref[:, cols].astype(f32) + row_recv[j].astype(f32)
            ).astype(bf16)
    with jax.named_scope("drain"):
        for copy in sends:
            copy.wait_send()
        for part in range(parts):
            if part < least:
                block = wide.at[part, pl.ds(0, (spans - 1) * half)]
                remote(
                    block, block, w_sem.at[part, 0], w_leave.at[part], sp=span_at(1)
                ).wait_send()
            for d in range(1, spans if part >= least else 1):

                def sent():
                    weight_wait(part, d).wait_send()

                when_extra(part, target(d), sent)

            def relayed():
                block = wide.at[part, pl.ds(0, (spans - 1) * half)]
                remote(
                    block, block, relay_sem.at[part, 0], relay_leave.at[part], grp=1 - side
                ).wait_send()

            when_extra(part, me, relayed)
        whole = norm_all.at[pl.ds(0, rows)]
        for i in range(3):
            remote(whole, whole, gather_sem.at[0], leave_sem.at[i], tp=mate).wait_send()
        remote(state_recv.at[pl.ds(0, spans - 1)], state_recv.at[pl.ds(0, spans - 1)],
               state_sem.at[0, 1], state_leave.at[1], sp=span_at(1)).wait_send()
        remote(rate_all.at[pl.ds(0, spans - 1)], rate_all.at[pl.ds(0, spans - 1)],
               state_sem.at[0, 0], state_leave.at[0], sp=span_at(1)).wait_send()
        remote(tp_recv, tp_recv, tp_sem.at[0, 0], tp_leave.at[0], tp=mate).wait_send()
        remote(row_recv.at[pl.ds(0, spans - 1)], row_recv.at[pl.ds(0, spans - 1)],
               row_sem.at[0], row_leave.at[0], sp=span_at(1)).wait_send()
        for way in range(2):
            for hop in range(spans - 1):

                @pl.when(passes(way, hop))
                def _():
                    block = norm_all.at[pl.ds(0, share)]
                    remote(
                        block,
                        block,
                        norm_sem.at[way, hop, 0],
                        norm_leave.at[way, hop],
                        sp=clamp(me + steps[way]),
                    ).wait_send()

                for part in range(parts):

                    @pl.when(passes(way, hop) & has(part, origin(way, hop)))
                    def _():
                        block = hid_all.at[:, pl.ds(0, 128)]
                        remote(
                            block,
                            block,
                            hid_sem.at[part, way, hop, 0],
                            hid_leave.at[part, way, hop],
                            sp=clamp(me + steps[way]),
                        ).wait_send()


def fused_block(
    query_rows,
    key_rows,
    value_rows,
    gate_rows,
    log_decay,
    head_gain,
    out_weight,
    residual,
    norm_gain,
    gate_weight,
    up_weight,
    down_weight,
    gate_taps,
    up_taps,
):
    spans, shares = (lax.axis_size("sp"), lax.axis_size("tp"))
    rows, width = query_rows.shape
    model = residual.shape[1]
    units = gate_weight.shape[1]
    part_cols, share = (model // spans, rows // shares)
    total = spans * rows
    counts = tile_counts(units // 128, spans)
    least, parts = min(counts[0]), max(counts[0])
    lines = log_decay.shape[0] * log_decay.shape[1]
    heads = width // HEAD
    rates = log_decay.reshape(lines, rows)
    f32, bf16 = jnp.float32, jnp.bfloat16
    far = pl.BlockSpec(memory_space=pltpu.HBM)
    dma = pltpu.SemaphoreType.DMA
    vmem = pltpu.VMEM
    return pl.pallas_call(
        functools.partial(block_kernel, spans, shares),
        out_shape=jax.ShapeDtypeStruct((share, model), bf16),
        in_specs=[far] * 14,
        out_specs=pl.BlockSpec(memory_space=pltpu.VMEM),
        scratch_shapes=[
            vmem((rows, width), bf16),
            vmem((rows, width), bf16),
            vmem((rows, width), bf16),
            vmem((rows, width), bf16),
            vmem((lines, rows), f32),
            vmem((rows, model), bf16),
            vmem(out_weight.shape, bf16),
            vmem(down_weight.shape, bf16),
            vmem(head_gain.shape, f32),
            vmem((model // 128, 128), bf16),
            vmem(gate_taps.shape, bf16),
            vmem(up_taps.shape, bf16),
            vmem((spans, lines, rows), f32),
            vmem((2, heads, HEAD, HEAD), bf16),
            vmem((spans, heads, HEAD, HEAD), bf16),
            vmem((parts, model, 256), bf16),
            vmem((rows, model), bf16),
            vmem((3, share, model), bf16),
            vmem((share, model), bf16),
            vmem((share, model), bf16),
            vmem((total, model), bf16),
            vmem((total, units), bf16),
            vmem((spans, rows, part_cols), bf16),
            vmem((3, spans, share, part_cols), bf16),
            vmem((spans, share, part_cols), bf16),
            vmem((spans, share, part_cols), bf16),
            vmem((spans, share, part_cols), bf16),
            dma((12,)),
            dma((parts,)),
            dma((spans - 1, 2)),
            dma((2,)),
            dma((parts, spans - 1)),
            dma((parts, spans - 1)),
            dma((least + (parts - least) * (spans - 1),)),
            dma((parts,)),
            dma((3, 2)),
            dma((2, spans - 1, SLABS)),
            dma((2, spans - 1)),
            dma((spans, SLABS)),
            dma((2,)),
            dma((3,)),
            dma((parts, 2, spans - 1, spans // 2)),
            dma((parts, 2, spans - 1)),
            dma((spans // 2, 3)),
            dma((1,)),
            dma((spans - 1,)),
            dma((1,)),
        ],
        compiler_params=pltpu.CompilerParams(
            collective_id=0, has_side_effects=True, vmem_limit_bytes=GRANT
        ),
    )(
        *(
            pltpu.with_memory_space_constraint(value, pltpu.HBM)
            for value in (
                query_rows,
                key_rows,
                value_rows,
                gate_rows,
                rates,
                head_gain,
                residual,
                norm_gain.reshape(model // 128, 128),
                gate_taps,
                up_taps,
                out_weight,
                gate_weight,
                up_weight,
                down_weight,
            )
        )
    )


def either(*args):
    spans, shares, twins = (lax.axis_size(name) for name in ("sp", "tp", "grp"))
    span_tokens = args[0].shape[0] * spans
    model_width = args[7].shape[1]
    lanes = args[9].shape[1] // 128
    fits = spans == 4 and lanes >= 2 * spans
    if fits and span_tokens < model_width and twins == 2 and shares == 4:
        return fused_block(*args)
    return shards(*args)


def solution(mesh):
    in_specs = (
        P(("grp", "sp"), "tp"),
        P(("grp", "sp"), "tp"),
        P(("grp", "sp"), "tp"),
        P(("grp", "sp"), "tp"),
        P(None, "tp", ("grp", "sp")),
        P(None, "tp"),
        P("tp", None),
        P(("grp", "sp"), None),
        P(),
        P("sp", "tp"),
        P("sp", "tp"),
        P("sp", "tp"),
        P(None, "tp"),
        P(None, "tp"),
    )
    out_specs = P(("grp", "sp", "tp"), None)
    return jax.shard_map(either, mesh=mesh, in_specs=in_specs, out_specs=out_specs, check_vma=False)
```
